128 devices in a mesh: ep: 64 (over z, y, x), tp: 2 (over core).
Axes of the slice: x: 4, y: 4, z: 4, core: 2. Of those that a mesh axis runs over, the one named last changes fastest.
Arguments:
- stream: bfloat16 [2048, 2048], P('ep'), may hold values from -6 to 6
- mixer_gain: float32 [2048], replicated, may hold values from 0.1 to 1.9
- gate_proj: bfloat16 [2048, 1024], P(None, 'tp'), may hold values from -0.125 to 0.125
- input_proj: bfloat16 [2048, 1024], P(None, 'tp'), may hold values from -0.125 to 0.125
- state_maps: bfloat16 [2, 2048, 256], P(None, None, 'tp'), may hold values from -0.125 to 0.125
- step_proj: bfloat16 [2048, 16], P(None, 'tp'), may hold values from -0.125 to 0.125
- step_bias: float32 [16], P('tp'), may hold values from -3 to 0.5
- decay_rate: float32 [16], P('tp'), may hold values from 0.05 to 4
- input_taps: float32 [4, 1024], P(None, 'tp'), may hold values from -3 to 3
- map_taps: float32 [2, 4, 256], P(None, None, 'tp'), may hold values from -3 to 3
- input_past: bfloat16 [2048, 3, 1024], P('ep', None, 'tp'), may hold values from -6 to 6
- map_past: bfloat16 [2048, 2, 3, 256], P('ep', None, None, 'tp'), may hold values from -6 to 6
- head_state: float32 [2048, 16, 4096], P('ep', 'tp'), may hold values from -1.6 to 1.6
- skip_gain: float32 [16], P('tp'), may hold values from 0 to 2
- inner_gain: float32 [1024], P('tp'), may hold values from 0.1 to 1.9
- mixer_out: bfloat16 [1024, 2048], P('tp'), may hold values from -0.1875 to 0.1875
- channel_gain: float32 [2048], replicated, may hold values from 0.1 to 1.9
- expert_ids: int32 [2048, 2], P('ep'), may hold values from 0 to 7, all different within a row; in each aligned block of 32 rows (0 to 31, 32 to 63, ...) at most 12 rows name the same one
- expert_weight: float32 [2048, 2], P('ep'), may hold values from 0.2 to 1
- expert_gate: bfloat16 [2048, 57344], P(None, ('ep', 'tp')), may hold values from -0.125 to 0.125
- expert_up: bfloat16 [2048, 57344], P(None, ('ep', 'tp')), may hold values from -0.125 to 0.125
- expert_down: bfloat16 [57344, 2048], P(('ep', 'tp')), may hold values from -0.0625 to 0.0625
- dense_gate: bfloat16 [2048, 5632], P('tp', 'ep'), may hold values from -0.125 to 0.125
- dense_up: bfloat16 [2048, 5632], P('tp', 'ep'), may hold values from -0.125 to 0.125
- dense_down: bfloat16 [5632, 2048], P('ep', 'tp'), may hold values from -0.078125 to 0.078125
- dense_mix: float32 [2048], P('tp'), may hold values from -2 to 2
Outputs:
- stream_out: bfloat16 [2048, 2048], P('ep', 'tp')
- state_out: float32 [2048, 16, 4096], P('ep', 'tp')
The draws below stay inside these ranges and needn't reach their ends.
Inputs may be any that keep to these rules, and one draw needn't show every extreme that they name: `expert_ids`: each row names 2 different experts. In each aligned block of 32 rows no expert is named by more than 12 rows, and in some block one expert is named by exactly 12 rows.
All inputs are finite; a program needn't handle non-finite values.
Results may differ from the reference program's by a relative error of at most 0.015.
Values may be sent and summed in bfloat16 or wider, within the bound.
A program may use at most 128 MiB of HBM per device.

```python
import math
import jax
import jax.numpy as jnp
import numpy as np
from jax import lax

D = 2048
INNER = 1024
HEAD = 64
HEADS = 16
GROUPS = 4
NSTATE = 64
CONV = 4
EXPERTS = 8
TOP_K = 2
EXPERT_HIDDEN = 7168
DENSE_HIDDEN = 5632
SEQ_DEV = 32
BATCH = 2048
CAP = 12
N_EP = 64
N_TP = 2


def steps_of(stream_key, dims, shards, low, high):
    level = 1.0
    for dim, blocks in shards:
        heights = jax.random.uniform(jax.random.fold_in(jax.random.fold_in(stream_key, 6), dim), (blocks,), jnp.float32, low / len(shards), high / len(shards))
        level = level * jnp.repeat(jnp.exp(heights), dims[dim] // blocks).reshape((-1,) + (1,) * (len(dims) - 1 - dim))
    return level


def shared_out(stream_key, own, number, rows, amount, top, limit, skew):
    ranking = jax.random.permutation(stream_key, amount)
    packed, common = portions_of(amount, rows * top, limit, skew, True), portions_of(amount, rows * top, limit, skew, False)
    places = jnp.arange(amount)

    def named(sizes, turn):
        used = int((sizes > 0).sum())
        fixed = max(1, used // 4)
        passed = fixed + (places - fixed + turn * (used - fixed)) % max(1, amount - fixed)
        return jnp.zeros((amount,), jnp.int32).at[ranking[jnp.where(places < fixed, places, passed)]].set(jnp.asarray(sizes, jnp.int32))

    sizes = jnp.where(number % 4 == 0, named(packed, number // 4), named(common, number - number // 4 - 1))
    mixed = jax.random.permutation(jax.random.fold_in(own, 3), amount)
    source_of, taker = mixed[0:amount // 2 * 2:2], mixed[1:amount // 2 * 2:2]
    slack = jnp.minimum(sizes[source_of] - 1, limit - sizes[taker]) // 2
    slack = jnp.where((source_of == ranking[0]) | (taker == ranking[0]) | (sizes[taker] == 0), 0, jnp.maximum(slack, 0))
    passed = jax.random.randint(jax.random.fold_in(own, 4), (amount // 2,), 0, 1 << 20) % (slack + 1)
    sizes = sizes.at[source_of].add(-passed).at[taker].add(passed)
    items = jnp.searchsorted(jnp.cumsum(sizes), jnp.arange(rows * top), side="right").astype(jnp.int32)
    table = items.reshape(top, rows).T
    table = table[jax.random.permutation(jax.random.fold_in(own, 1), rows)]
    turn = jax.random.randint(jax.random.fold_in(own, 2), (rows, 1), 0, top)
    return jnp.take_along_axis(table, (jnp.arange(top)[None, :] + turn) % top, axis=1)


def portions_of(amount, total, most, skew, full):
    weights = [(1 << 20) // math.isqrt(rank ** skew) + 1 for rank in range(1, amount + 1)]
    largest = most if full else min(most, max(-(-total // amount), total * weights[0] // sum(weights)))
    least = 1 if total - largest >= amount - 1 else 0
    counts, rest = [largest] + [least] * (amount - 1), total - largest - least * (amount - 1)
    while rest > 0:
        free = [i for i in range(1, amount) if counts[i] < largest] or [i for i in range(1, amount) if counts[i] < most]
        whole, left = sum([weights[i] for i in free]), rest
        for i in free:
            extra = min(most - counts[i], max(1, left * weights[i] // whole), rest)
            counts[i] = counts[i] + extra
            rest = rest - extra
    return np.array(counts)


def noise(rng, shape, width, reach, pieces=(), kind=jnp.bfloat16):
    values = width * jax.random.normal(rng, shape, jnp.float32)
    if pieces:
        values = values * steps_of(rng, shape, pieces, -0.22, 0.18)
    return jnp.clip(values, -reach, reach).astype(kind)


def setup_inputs(seed: int = 0) -> dict:
    key_list = jax.random.split(jax.random.key(seed), 27)
    stream = noise(key_list[0], (BATCH, D), 1.0, 6.0, ((0, 64),))
    mixer_gain = jnp.clip(1.0 + 0.18 * jax.random.normal(key_list[1], (D,), jnp.float32), 0.1, 1.9)
    gate_proj = noise(key_list[2], (D, INNER), D ** -0.5, 0.125, ((1, 2),))
    input_proj = noise(key_list[3], (D, INNER), D ** -0.5, 0.125, ((1, 2),))
    state_maps = noise(key_list[4], (2, D, GROUPS * NSTATE), D ** -0.5, 0.125, ((2, 2),))
    step_proj = noise(key_list[5], (D, HEADS), D ** -0.5, 0.125, ((1, 2),))
    step_bias = jnp.clip(-3.0 + 3.5 * jax.random.uniform(key_list[6], (HEADS,), jnp.float32) ** steps_of(key_list[6], (HEADS,), ((0, 2),), -0.2, 0.2), -3.0, 0.5)
    decay_rate = jnp.clip(jnp.exp(math.log(4.0) - 4.3820266 * jax.random.uniform(key_list[7], (HEADS,), jnp.float32) ** steps_of(key_list[7], (HEADS,), ((0, 2),), -0.2, 0.2)), 0.05, 4.0)
    input_taps = noise(key_list[8], (CONV, INNER), 0.5, 3.0, ((1, 2),), jnp.float32)
    map_taps = noise(key_list[9], (2, CONV, GROUPS * NSTATE), 0.5, 3.0, ((2, 2),), jnp.float32)
    input_past = noise(key_list[10], (BATCH, CONV - 1, INNER), 1.0, 6.0, ((0, 64), (2, 2)))
    map_past = noise(key_list[11], (BATCH, 2, CONV - 1, GROUPS * NSTATE), 1.0, 6.0, ((0, 64), (3, 2)))
    head_state = noise(key_list[12], (BATCH, HEADS, HEAD * NSTATE), 0.2, 1.6, ((0, 64), (1, 2)), jnp.float32)
    skip_gain = jnp.clip(2.0 * jax.random.uniform(key_list[13], (HEADS,), jnp.float32) ** steps_of(key_list[13], (HEADS,), ((0, 2),), -0.2, 0.2), 0.0, 2.0)
    inner_gain = jnp.clip(1.0 + 0.18 * jax.random.normal(key_list[14], (INNER,), jnp.float32), 0.1, 1.9)
    mixer_out = noise(key_list[15], (INNER, D), INNER ** -0.5, 0.1875, ((0, 2),))
    channel_gain = jnp.clip(1.0 + 0.18 * jax.random.normal(key_list[16], (D,), jnp.float32), 0.1, 1.9)
    expert_ids_keys = jax.random.split(jax.random.fold_in(key_list[17], 1), BATCH // SEQ_DEV)
    expert_ids_turns = jax.random.permutation(jax.random.fold_in(key_list[17], 3), BATCH // SEQ_DEV)
    expert_ids = jax.vmap(lambda own, number: shared_out(jax.random.fold_in(key_list[17], 2), own, number, SEQ_DEV, EXPERTS, TOP_K, CAP, 2))(expert_ids_keys, expert_ids_turns).reshape((BATCH, TOP_K))
    expert_weight = jnp.clip(0.2 + 0.8 * jax.random.uniform(key_list[18], (BATCH, TOP_K), jnp.float32) ** steps_of(key_list[18], (BATCH, TOP_K), ((0, 64),), -0.2, 0.2), 0.2, 1.0)
    expert_gate = noise(key_list[19], (D, EXPERTS * EXPERT_HIDDEN), D ** -0.5, 0.125, ((1, 128),))
    expert_up = noise(key_list[20], (D, EXPERTS * EXPERT_HIDDEN), D ** -0.5, 0.125, ((1, 128),))
    expert_down = noise(key_list[21], (EXPERTS * EXPERT_HIDDEN, D), EXPERT_HIDDEN ** -0.5, 0.0625, ((0, 128),))
    dense_gate = noise(key_list[22], (D, DENSE_HIDDEN), D ** -0.5, 0.125, ((0, 2), (1, 64)))
    dense_up = noise(key_list[23], (D, DENSE_HIDDEN), D ** -0.5, 0.125, ((0, 2), (1, 64)))
    dense_down = noise(key_list[24], (DENSE_HIDDEN, D), DENSE_HIDDEN ** -0.5, 0.078125, ((0, 64), (1, 2)))
    dense_mix = jnp.clip(jax.random.uniform(key_list[25], (D,), jnp.float32, -2.0, 2.0) * steps_of(key_list[25], (D,), ((0, 2),), -0.4, 0.0), -2.0, 2.0)
    return {"stream": stream, "mixer_gain": mixer_gain, "gate_proj": gate_proj, "input_proj": input_proj, "state_maps": state_maps, "step_proj": step_proj, "step_bias": step_bias, "decay_rate": decay_rate, "input_taps": input_taps, "map_taps": map_taps, "input_past": input_past, "map_past": map_past, "head_state": head_state, "skip_gain": skip_gain, "inner_gain": inner_gain, "mixer_out": mixer_out, "channel_gain": channel_gain, "expert_ids": expert_ids, "expert_weight": expert_weight, "expert_gate": expert_gate, "expert_up": expert_up, "expert_down": expert_down, "dense_gate": dense_gate, "dense_up": dense_up, "dense_down": dense_down, "dense_mix": dense_mix}


EPS = 1e-06

def rms_scale(values):
    return values * lax.rsqrt(lax.optimization_barrier(jnp.mean(values * values, axis=-1, keepdims=True)) + EPS)

def short_conv(past_rows, newest, tap_weights, along):
    window = jnp.concatenate([past_rows, jnp.expand_dims(newest, along)], axis=along).astype(jnp.float32)
    return jax.nn.silu(lax.optimization_barrier(jnp.sum(window * tap_weights, axis=along)))

def mix_heads(stream, mixer_gain, gate_proj, input_proj, state_maps, step_proj, step_bias, decay_rate, input_taps, map_taps, input_past, map_past, head_state, skip_gain, inner_gain):
    row_count = stream.shape[0]
    normed = (rms_scale(stream.astype(jnp.float32)) * mixer_gain).astype(jnp.bfloat16)
    gate_in = jnp.dot(normed, gate_proj, preferred_element_type=jnp.float32).astype(jnp.bfloat16)
    input_new = jnp.dot(normed, input_proj, preferred_element_type=jnp.float32).astype(jnp.bfloat16)
    map_new = jnp.stack([jnp.dot(normed, state_maps[0], preferred_element_type=jnp.float32), jnp.dot(normed, state_maps[1], preferred_element_type=jnp.float32)], axis=1).astype(jnp.bfloat16)
    step_size = jax.nn.softplus(jnp.dot(normed, step_proj, preferred_element_type=jnp.float32) + step_bias)
    conv_in = short_conv(input_past, input_new, input_taps, 1)
    conv_map = short_conv(map_past, map_new, map_taps, 2)
    head_count = step_size.shape[1]
    per_group = HEADS // GROUPS
    group_count = head_count // per_group
    write_map = jnp.repeat(conv_map[:, 0].reshape(row_count, group_count, NSTATE), per_group, axis=1)
    read_map = jnp.repeat(conv_map[:, 1].reshape(row_count, group_count, NSTATE), per_group, axis=1)
    values = conv_in.reshape(row_count, head_count, HEAD)
    decay_now = jnp.exp(-decay_rate * step_size)
    state_old = head_state.reshape(row_count, head_count, HEAD, NSTATE)
    state_new = decay_now[:, :, None, None] * state_old + (step_size[:, :, None] * values)[:, :, :, None] * write_map[:, :, None, :]
    gated = lax.optimization_barrier(jnp.sum(state_new * read_map[:, :, None, :], axis=3)) + skip_gain[:, None] * values
    gated = gated.reshape(row_count, head_count * HEAD) * jax.nn.silu(gate_in.astype(jnp.float32))
    inner_out = rms_scale(gated.reshape(row_count, group_count, -1)).reshape(row_count, -1) * inner_gain
    return (inner_out.astype(jnp.bfloat16), state_new.reshape(row_count, head_count, HEAD * NSTATE))

def expert_sum(ffn_in, expert_ids, expert_weight, expert_gate, expert_up, expert_down):
    total_rows, feature_count = ffn_in.shape
    hidden = expert_gate.shape[1] // EXPERTS
    row_limit = min(total_rows, N_EP * CAP)

    def visit(running, expert_index):
        matched = expert_ids == expert_index
        chosen = jnp.any(matched, axis=1)
        weight = lax.optimization_barrier(jnp.sum(jnp.where(matched, expert_weight, jnp.zeros_like(expert_weight)), axis=1))
        picked = jnp.nonzero(chosen, size=row_limit, fill_value=0)[0].astype(jnp.int32)
        is_live = jnp.arange(row_limit, dtype=jnp.int32) < jnp.sum(chosen.astype(jnp.int32))
        taken_rows = ffn_in[picked]
        first_col = (expert_index * hidden).astype(jnp.int32)
        w_gate = lax.dynamic_slice_in_dim(expert_gate, first_col, hidden, 1)
        w_up = lax.dynamic_slice_in_dim(expert_up, first_col, hidden, 1)
        w_down = lax.dynamic_slice_in_dim(expert_down, first_col, hidden, 0)
        act = (jax.nn.silu(jnp.dot(taken_rows, w_gate, preferred_element_type=jnp.float32)) * jnp.dot(taken_rows, w_up, preferred_element_type=jnp.float32)).astype(jnp.bfloat16)
        result = jnp.dot(act, w_down, preferred_element_type=jnp.float32)
        scale = jnp.where(is_live, weight[picked], jnp.zeros_like(weight[picked]))
        return (running.at[picked].add(result * scale[:, None]), None)
    start_sum = jnp.zeros((total_rows, feature_count), jnp.float32)
    total, _ = lax.scan(visit, start_sum, jnp.arange(EXPERTS, dtype=jnp.int32))
    return total

def reference(stream, mixer_gain, gate_proj, input_proj, state_maps, step_proj, step_bias, decay_rate, input_taps, map_taps, input_past, map_past, head_state, skip_gain, inner_gain, mixer_out, channel_gain, expert_ids, expert_weight, expert_gate, expert_up, expert_down, dense_gate, dense_up, dense_down, dense_mix):
    inner_out, state_out = mix_heads(stream, mixer_gain, gate_proj, input_proj, state_maps, step_proj, step_bias, decay_rate, input_taps, map_taps, input_past, map_past, head_state, skip_gain, inner_gain)
    block_cols = inner_out.shape[1] // N_TP
    mixed = jnp.zeros((stream.shape[0], mixer_out.shape[1]), jnp.float32)
    for portion in range(N_TP):
        partial_out = jnp.dot(inner_out[:, portion * block_cols:(portion + 1) * block_cols], mixer_out[portion * block_cols:(portion + 1) * block_cols], preferred_element_type=jnp.float32)
        mixed = mixed + lax.optimization_barrier(partial_out.astype(jnp.bfloat16)).astype(jnp.float32)
    hidden_mid = stream.astype(jnp.float32) + mixed
    ffn_in = (rms_scale(hidden_mid) * channel_gain).astype(jnp.bfloat16)
    routed = expert_sum(ffn_in, expert_ids, expert_weight, expert_gate, expert_up, expert_down)
    dense_act = (jax.nn.silu(jnp.dot(ffn_in, dense_gate, preferred_element_type=jnp.float32)) * jnp.dot(ffn_in, dense_up, preferred_element_type=jnp.float32)).astype(jnp.bfloat16)
    dense_res = jnp.dot(dense_act, dense_down, preferred_element_type=jnp.float32)
    stream_out = (hidden_mid + routed + jax.nn.sigmoid(dense_mix) * dense_res).astype(jnp.bfloat16)
    return (stream_out, state_out)
```

```python
import functools

import jax
import jax.numpy as jnp
from jax import lax
from jax.experimental import pallas as pl
from jax.experimental.pallas import tpu as pltpu
from jax.sharding import PartitionSpec as P

EPS = 1e-06
MESH = pl.DeviceIdType.MESH
F32 = jnp.float32
BF16 = jnp.bfloat16
VMEM = pltpu.VMEM
ANY = pl.ANY

HEADS = 8
ROWS = 32
EXPERTS = 8
CAP = 12
CHUNKS = 8
CHUNK = 512
GROUPS = 8
GROUP_ROWS = 256
SLOTS = 96
HALF = 1024
HIDDEN = 448
HPAD = 512
DENSE = 88

WIDTHS = (384, 384, 256)
STARTS = (0, 384, 768)
BLOCK_ROWS = (32, 32, 48)
ORDERS = ((2, 1, 0), (1, 0, 2), (0, 2, 1))


def dot(a, b):
    return jnp.dot(a, b, preferred_element_type=F32)


def dot_nt(a, b):
    return lax.dot_general(a, b, (((1,), (1,)), ((), ())), preferred_element_type=F32)


def dot_tn(a, b):
    return lax.dot_general(a, b, (((0,), (0,)), ((), ())), preferred_element_type=F32)


def silu(v):
    return v / (1.0 + jnp.exp(-v))


def rms(v):
    return v * lax.rsqrt(jnp.mean(v * v, axis=-1, keepdims=True) + EPS)


def split(v):
    high = v.astype(BF16)
    return high, (v - high.astype(F32)).astype(BF16)


def mixer_kernel(
    stream,
    mixer_gain,
    step_t,
    bias,
    decay,
    skip,
    input_taps,
    map_taps,
    input_past,
    map_past,
    inner_gain,
    ids,
    weights,
    gate_hbm,
    input_hbm,
    maps_hbm,
    out_hbm,
    state_hbm,
    state_out,
    partial,
    meta,
    gate_w,
    input_w,
    maps_w,
    out_w,
    old,
    new,
    dec,
    write,
    read,
    xs_high,
    xs_low,
    tmp,
    y,
    sems,
):
    loads = [
        pltpu.make_async_copy(input_hbm, input_w, sems.at[0]),
        pltpu.make_async_copy(maps_hbm, maps_w, sems.at[1]),
        pltpu.make_async_copy(gate_hbm, gate_w, sems.at[2]),
        pltpu.make_async_copy(out_hbm, out_w, sems.at[3]),
    ]

    def load_state(t):
        cols = pl.ds(pl.multiple_of(t * CHUNK, CHUNK), CHUNK)
        return pltpu.make_async_copy(state_hbm.at[:, cols], old.at[t], sems.at[4 + t])

    def store_state(t):
        cols = pl.ds(pl.multiple_of(t * CHUNK, CHUNK), CHUNK)
        return pltpu.make_async_copy(
            new.at[t], state_out.at[:, cols], sems.at[4 + CHUNKS + t]
        )

    loads[0].start()
    loads[1].start()
    for t in range(CHUNKS):
        load_state(t).start()
    loads[2].start()
    loads[3].start()

    normed = (rms(stream[...].astype(F32)) * mixer_gain[...]).astype(BF16)
    steps = dot_nt(normed, step_t[...])

    expert_of = lax.broadcasted_iota(jnp.int32, (EXPERTS, ROWS), 0)
    hit0 = (ids[0:1, :] == expert_of).astype(F32)
    hit1 = (ids[1:2, :] == expert_of).astype(F32)
    member = hit0 + hit1
    upper = (
        lax.broadcasted_iota(jnp.int32, (ROWS, ROWS), 0)
        <= lax.broadcasted_iota(jnp.int32, (ROWS, ROWS), 1)
    ).astype(BF16)
    rank = dot(member.astype(BF16), upper) * member
    weight = hit0 * weights[0:1, :] + hit1 * weights[1:2, :]
    w_high = weight.astype(BF16).astype(F32)
    w_low = weight - w_high
    table = jnp.concatenate(
        [rank, w_high, w_low, jnp.zeros((104, ROWS), F32)], axis=0
    ).astype(BF16)
    eye = (
        lax.broadcasted_iota(jnp.int32, (ROWS, ROWS), 0)
        == lax.broadcasted_iota(jnp.int32, (ROWS, ROWS), 1)
    ).astype(BF16)
    by_row = dot_nt(eye, table)
    meta[...] = jnp.concatenate([by_row[0:16], by_row[16:32]], axis=1).astype(BF16)

    loads[0].wait()
    newest = dot(normed, input_w[...]).astype(BF16).astype(F32)
    conv = newest * input_taps[3:4, :]
    for t in range(3):
        conv = conv + input_past[t].astype(F32) * input_taps[t : t + 1, :]
    conv = silu(conv)

    loads[1].wait()
    conv_maps = []
    for m in range(2):
        new_map = dot(normed, maps_w[m]).astype(BF16).astype(F32)
        acc = new_map * map_taps[m, 3:4, :]
        for t in range(3):
            acc = acc + map_past[3 * m + t].astype(F32) * map_taps[m, t : t + 1, :]
        conv_maps.append(silu(acc))

    lane = lax.broadcasted_iota(jnp.int32, (ROWS, 128), 1)
    low_half = lane < 64

    def both_halves(v):
        turned = pltpu.roll(v, 64, 1)
        return jnp.where(low_half, v, turned), jnp.where(low_half, turned, v)

    write_by_group = both_halves(conv_maps[0])
    read_by_group = both_halves(conv_maps[1])
    for h in range(HEADS):
        rows = pl.ds(h, ROWS, stride=HEADS)
        v = jnp.broadcast_to(steps[:, h : h + 1], (ROWS, 128)) + bias[h]
        step = jnp.maximum(v, 0.0) + jnp.log1p(jnp.exp(-jnp.abs(v)))
        dec[rows, :] = jnp.exp(-decay[h] * step)
        pair = conv[:, 128 * (h // 2) : 128 * (h // 2) + 128]
        mine = low_half if h % 2 == 0 else jnp.logical_not(low_half)
        tmp[rows, :] = jnp.where(mine, step * pair, 0.0)
        write[rows, :] = write_by_group[h // 4]
        read[rows, :] = read_by_group[h // 4]
    high, low = split(tmp[...])
    xs_high[...] = high
    xs_low[...] = low
    y[...] = jnp.zeros_like(y)

    slot = lax.broadcasted_iota(jnp.int32, (128, CHUNK), 0) % 64
    place = lax.broadcasted_iota(jnp.int32, (128, CHUNK), 1) // 64

    def chunk_step(t, carry):
        spread = (slot == place + 8 * t).astype(F32).astype(BF16)
        load_state(t).wait()
        values = dot(xs_high[...], spread) + dot(xs_low[...], spread)
        wide = lambda ref: jnp.concatenate([ref[...]] * (CHUNK // 128), axis=1)
        fresh = wide(dec) * old[t] + values * wide(write)
        new[t] = fresh
        store_state(t).start()
        high, low = split(fresh * wide(read))
        y[...] += dot_nt(high, spread) + dot_nt(low, spread)
        return carry

    lax.fori_loop(0, CHUNKS, chunk_step, 0)

    loads[2].wait()
    gate = silu(dot(normed, gate_w[...]).astype(BF16).astype(F32))
    pieces = []
    for j in range(HEADS // 2):
        even = y[pl.ds(2 * j, ROWS, stride=HEADS), :]
        odd = y[pl.ds(2 * j + 1, ROWS, stride=HEADS), :]
        gain = jnp.where(low_half, skip[2 * j], skip[2 * j + 1])
        cols = slice(128 * j, 128 * j + 128)
        pieces.append(
            (jnp.where(low_half, even, odd) + gain * conv[:, cols]) * gate[:, cols]
        )
    groups = [jnp.concatenate(pieces[2 * g : 2 * g + 2], axis=1) for g in range(2)]
    inner = jnp.concatenate([rms(g) for g in groups], axis=1) * inner_gain[...]
    loads[3].wait()
    partial[...] = dot(inner.astype(BF16), out_w[...]).astype(BF16)
    for t in range(CHUNKS):
        store_state(t).wait()


def run_mixer(
    stream,
    mixer_gain,
    step_t,
    bias,
    decay,
    skip,
    input_taps,
    map_taps,
    input_past,
    map_past,
    inner_gain,
    ids,
    weights,
    gate_proj,
    input_proj,
    state_maps,
    mixer_out,
    state,
):
    vmem = pl.BlockSpec(memory_space=VMEM)
    smem = pl.BlockSpec(memory_space=pltpu.SMEM)
    hbm = pl.BlockSpec(memory_space=ANY)
    lanes = lambda: VMEM((256, 128), F32)
    return pl.pallas_call(
        mixer_kernel,
        out_shape=(
            jax.ShapeDtypeStruct((256, 4096), F32),
            jax.ShapeDtypeStruct((ROWS, 2 * HALF), BF16),
            jax.ShapeDtypeStruct((16, 256), BF16),
        ),
        in_specs=[vmem] * 3 + [smem] * 3 + [vmem] * 7 + [hbm] * 5,
        out_specs=(hbm, vmem, vmem),
        scratch_shapes=[
            VMEM((2048, 512), BF16),
            VMEM((2048, 512), BF16),
            VMEM((2, 2048, 128), BF16),
            VMEM((512, 2048), BF16),
            VMEM((CHUNKS, 256, CHUNK), F32),
            VMEM((CHUNKS, 256, CHUNK), F32),
            lanes(),
            lanes(),
            lanes(),
            VMEM((256, 128), BF16),
            VMEM((256, 128), BF16),
            lanes(),
            lanes(),
            pltpu.SemaphoreType.DMA((4 + 2 * CHUNKS,)),
        ],
        compiler_params=pltpu.CompilerParams(vmem_limit_bytes=40 * 2**20),
        name="mixer",
    )(
        stream,
        mixer_gain,
        step_t,
        bias,
        decay,
        skip,
        input_taps,
        map_taps,
        input_past,
        map_past,
        inner_gain,
        ids,
        weights,
        gate_proj,
        input_proj,
        state_maps,
        mixer_out,
        state,
    )


def ffn_kernel(
    partial,
    stream,
    gain,
    meta,
    mix,
    eg_hbm,
    eu_hbm,
    ed_hbm,
    dg_hbm,
    du_hbm,
    dd_hbm,
    out,
    x0,
    x1,
    x2,
    y0,
    y1,
    y2,
    s0,
    s1,
    s2,
    ra0,
    ra1,
    ra2,
    rb0,
    rb1,
    rb2,
    rc0,
    rc1,
    rc2,
    other_partial,
    wide,
    mid,
    eg,
    eu,
    ed,
    ed_other,
    dgu,
    dgu_other,
    dd,
    dd_scaled,
    packed,
    slot_weight,
    act,
    act_other,
    left_side,
    result,
    local_sem,
    ag_send,
    ag_recv,
    dd_send,
    dd_recv,
    rs_send,
    rs_recv,
    mi_send,
    mi_recv,
):
    ep = lax.axis_index("ep")
    core = lax.axis_index("tp")
    coords = (ep // 16, (ep // 4) % 4, ep % 4)
    other = 1 - core
    own_cols = pl.multiple_of(core * HALF, HALF)
    other_cols = pl.multiple_of(other * HALF, HALF)
    expert = ep // 8
    mine = (x0, x1, x2)
    theirs = (y0, y1, y2)
    sums = (s0, s1, s2)
    arrivals = ((rc0, rc1, rc2), (rb0, rb1, rb2), (ra0, ra1, ra2))

    def neighbour(dim, shift):
        moved = list(coords)
        moved[dim] = lax.rem(coords[dim] + shift, 4)
        return (moved[0] * 16 + moved[1] * 4 + moved[2], core)

    partner = (ep, other)

    barrier = pltpu.get_barrier_semaphore()
    for dim in range(3):
        for shift in (1, 3):
            pl.semaphore_signal(
                barrier, inc=1, device_id=neighbour(dim, shift), device_id_type=MESH
            )
    pl.semaphore_signal(barrier, inc=1, device_id=partner, device_id_type=MESH)
    pl.semaphore_wait(barrier, 7)

    def to_partner(src, dst, n):
        return pltpu.make_async_remote_copy(
            src_ref=src,
            dst_ref=dst,
            send_sem=mi_send.at[n],
            recv_sem=mi_recv.at[n],
            device_id=partner,
            device_id_type=MESH,
        )

    swap_partial = to_partner(partial, other_partial, 0)
    swap_partial.start()
    loads = [
        pltpu.make_async_copy(eg_hbm, eg.at[pl.ds(0, HIDDEN)], local_sem.at[0]),
        pltpu.make_async_copy(eu_hbm, eu.at[pl.ds(0, HIDDEN)], local_sem.at[1]),
        pltpu.make_async_copy(
            ed_hbm.at[:, pl.ds(own_cols, HALF)], ed.at[pl.ds(0, HIDDEN)], local_sem.at[2]
        ),
        pltpu.make_async_copy(dg_hbm, dgu.at[pl.ds(0, DENSE)], local_sem.at[3]),
        pltpu.make_async_copy(du_hbm, dgu.at[pl.ds(128, DENSE)], local_sem.at[4]),
        pltpu.make_async_copy(dd_hbm, dd, local_sem.at[5]),
    ]
    for load in loads:
        load.start()

    swap_partial.wait()
    mixed = partial[...].astype(F32) + other_partial[...].astype(F32)
    hidden = stream[...].astype(F32) + mixed
    mid[...] = hidden
    wide[...] = (rms(hidden) * gain[...]).astype(BF16)
    here = coords
    for p in range(3):
        cols = pl.ds(pl.multiple_of(own_cols + STARTS[p], 128), WIDTHS[p])
        mine[p][here[0], here[1], here[2], 0:ROWS, :] = wide[:, cols]
    x2[here[0], here[1], here[2], ROWS : ROWS + 16, :] = meta[...]

    def view(buf, p, k, j, half, rows=None):
        index = [None, None, None]
        free = sorted(ORDERS[p][:k])
        for q in range(3):
            dim = ORDERS[p][q]
            if q < k:
                index[dim] = pl.ds(0, 4)
            elif q == k:
                index[dim] = j
            else:
                index[dim] = coords[dim]
        if half is not None:
            if free:
                index[free[0]] = pl.ds(2 * half, 2)
            else:
                index.append(pl.ds(16 * half, 16) if rows is None or half == 0 else rows)
        elif rows is not None:
            index.append(rows)
        return buf.at[tuple(index)]

    def turn(p, k, shift):
        return lax.rem(coords[ORDERS[p][k]] + shift, 4)

    def gather_copy(p, k, n, j, half, shift):
        rows = pl.ds(16, BLOCK_ROWS[p] - 16) if k == 0 else None
        where = view(mine[p], p, k, j, half, rows)
        at = 6 * (3 * k + p) + n
        return pltpu.make_async_remote_copy(
            src_ref=where,
            dst_ref=where,
            send_sem=ag_send.at[at],
            recv_sem=ag_recv.at[at],
            device_id=neighbour(ORDERS[p][k], shift),
            device_id_type=MESH,
        )

    hand_overs = []

    def hand_over(p, j, half, n):
        free = sorted(ORDERS[p][:2])
        rows = pl.ds(0, ROWS)

        def cut(buf):
            index = [None, None, None, rows]
            index[ORDERS[p][2]] = j
            for dim in free:
                index[dim] = pl.ds(0, 4)
            if half is not None:
                index[free[0]] = pl.ds(2 * half, 2)
            return buf.at[tuple(index)]

        copy = pltpu.make_async_remote_copy(
            src_ref=cut(mine[p]),
            dst_ref=cut(theirs[p]),
            send_sem=dd_send.at[7 * p + n],
            recv_sem=dd_recv.at[7 * p + n],
            device_id=partner,
            device_id_type=MESH,
        )
        copy.start()
        hand_overs.append(copy)

    for k in range(3):
        copies = []
        for p in range(3):
            me, right, left = turn(p, k, 0), turn(p, k, 1), turn(p, k, 3)
            table = [
                gather_copy(p, k, 0, me, 0, 1),
                gather_copy(p, k, 1, me, 1, 1),
                gather_copy(p, k, 2, me, 1, 3),
                gather_copy(p, k, 3, me, 0, 3),
                gather_copy(p, k, 4, left, 0, 1),
                gather_copy(p, k, 5, right, 1, 3),
            ]
            copies.append(table)
            table[0].start()
            table[2].start()
            table[1].start()
            table[3].start()
            if k == 2:
                hand_over(p, me, None, 0)
        if k == 0:
            early = [
                to_partner(
                    ed_hbm.at[:, pl.ds(other_cols, HALF)], ed_other.at[pl.ds(0, HIDDEN)], 1
                ),
                to_partner(dg_hbm, dgu_other.at[pl.ds(0, DENSE)], 2),
                to_partner(du_hbm, dgu_other.at[pl.ds(128, DENSE)], 3),
            ]
            for copy in early:
                copy.start()
            for ref in (eg, eu, ed, ed_other):
                ref[HIDDEN:HPAD, :] = jnp.zeros((HPAD - HIDDEN, ref.shape[1]), BF16)
            for ref in (dgu, dgu_other):
                ref[DENSE:128, :] = jnp.zeros((128 - DENSE, HALF), BF16)
                ref[128 + DENSE : 256, :] = jnp.zeros((128 - DENSE, HALF), BF16)
            dd_scaled[DENSE:128, :] = jnp.zeros((128 - DENSE, HALF), BF16)
            for g in range(GROUPS):
                result[g, SLOTS:128, :] = jnp.zeros((128 - SLOTS, HALF), BF16)
        for p in range(3):
            left, right = turn(p, k, 3), turn(p, k, 1)
            copies[p][0].wait_recv()
            copies[p][4].start()
            copies[p][2].wait_recv()
            copies[p][5].start()
            if k == 2:
                hand_over(p, left, 0, 1)
                hand_over(p, right, 1, 2)
        for p in range(3):
            left, right, far = turn(p, k, 3), turn(p, k, 1), turn(p, k, 2)
            copies[p][1].wait_recv()
            copies[p][3].wait_recv()
            if k == 2:
                hand_over(p, left, 1, 3)
                hand_over(p, right, 0, 4)
        for p in range(3):
            far = turn(p, k, 2)
            copies[p][4].wait_recv()
            copies[p][5].wait_recv()
            if k == 2:
                hand_over(p, far, 0, 5)
                hand_over(p, far, 1, 6)
        for p in range(3):
            for copy in copies[p]:
                copy.wait_send()
    for copy in hand_overs:
        copy.wait()
    for load in loads:
        load.wait()
    for copy in early:
        copy.wait()

    pick_row = lax.broadcasted_iota(jnp.int32, (128, 128), 0)
    pick_rank = (pick_row == expert).astype(F32).astype(BF16)
    pick_weight = (
        jnp.logical_or(pick_row == expert + 8, pick_row == expert + 16)
    ).astype(F32).astype(BF16)
    lane = lax.broadcasted_iota(jnp.int32, (GROUP_ROWS, 128), 1)
    source = lax.broadcasted_iota(jnp.int32, (GROUP_ROWS, 128), 0) // ROWS

    def group_of(bufs, g):
        z, y = g // 2, 2 * lax.rem(g, 2)
        return jnp.concatenate(
            [
                bufs[p][z, pl.ds(y, 2), :, 0:ROWS, :].reshape(GROUP_ROWS, WIDTHS[p])
                for p in range(3)
            ],
            axis=1,
        )

    def pack_group(g, carry):
        z, y = g // 2, 2 * lax.rem(g, 2)
        tags = x2[z, pl.ds(y, 2), :, ROWS : ROWS + 16, :].reshape(8, 16, 256)
        tags = jnp.concatenate([tags[:, :, 0:128], tags[:, :, 128:256]], axis=1)
        tags = tags.reshape(GROUP_ROWS, 128)
        rank = dot(tags, pick_rank).astype(jnp.int32)
        hit = jnp.logical_and(rank > 0, rank + (CAP * source - 1) == lane)
        table = hit.astype(F32).astype(BF16)
        left_side[g, :, 0:128] = table
        used = table[:, 0:SLOTS]
        slots = pl.ds(pl.multiple_of(g * SLOTS, SLOTS), SLOTS)
        packed[slots, pl.ds(own_cols, HALF)] = dot_tn(used, group_of(mine, g)).astype(BF16)
        packed[slots, pl.ds(other_cols, HALF)] = dot_tn(used, group_of(theirs, g)).astype(
            BF16
        )
        slot_tags = dot_tn(used, tags).astype(BF16)
        slot_weight[slots, :] = dot(slot_tags, pick_weight)
        return carry

    lax.fori_loop(0, GROUPS, pack_group, 0)

    sends = []
    for i in range(2):
        rows = pl.ds(i * 384, 384)
        taken = packed[rows, :]
        gate = dot_nt(taken, eg[...])
        up = dot_nt(taken, eu[...])
        act[rows, :] = (silu(gate) * up * slot_weight[rows, 0:1]).astype(BF16)
        copy = to_partner(act.at[rows], act_other.at[rows], 4 + i)
        copy.start()
        sends.append(copy)

    def dense_group(g, carry):
        both = dot_nt(group_of(mine, g), dgu[...]) + dot_nt(group_of(theirs, g), dgu_other[...])
        left_side[g, :, 128:256] = (silu(both[:, 0:128]) * both[:, 128:256]).astype(BF16)
        return carry

    lax.fori_loop(0, GROUPS, dense_group, 0)
    share = 1.0 / (1.0 + jnp.exp(-mix[...]))
    dd_scaled[0:DENSE, :] = (dd[...].astype(F32) * share).astype(BF16)

    for i in range(2):
        rows = pl.ds(i * 384, 384)
        sends[i].wait()
        back = dot(act[rows, :], ed[...]) + dot(act_other[rows, :], ed_other[...])
        result[pl.ds(4 * i, 4), 0:SLOTS, :] = back.astype(BF16).reshape(4, SLOTS, HALF)

    def spread_group(g, carry):
        z, y = g // 2, 2 * lax.rem(g, 2)
        total = dot(left_side[g], jnp.concatenate([result[g], dd_scaled[...]], axis=0))
        for p in range(3):
            cut = total[:, STARTS[p] : STARTS[p] + WIDTHS[p]].astype(BF16)
            sums[p][z, pl.ds(y, 2)] = cut.reshape(2, 4, ROWS, WIDTHS[p])
        return carry

    lax.fori_loop(0, GROUPS, spread_group, 0)

    def scatter_copy(p, k, n, j, half, shift):
        at = 6 * (3 * k + p) + n
        return pltpu.make_async_remote_copy(
            src_ref=view(sums[p], p, k, j, half),
            dst_ref=arrivals[k][p].at[n],
            send_sem=rs_send.at[at],
            recv_sem=rs_recv.at[at],
            device_id=neighbour(ORDERS[p][k], shift),
            device_id_type=MESH,
        )

    def add_in(p, k, j, half, slots):
        got = arrivals[k][p]
        if k == 0:
            rows = pl.ds(16 * half, 16)
            ref = sums[p].at[
                tuple(j if d == ORDERS[p][0] else coords[d] for d in range(3)) + (rows,)
            ]
            total = ref[...].astype(F32)
            for n in slots:
                total = total + got[n].astype(F32)
            ref[...] = total.astype(BF16)
            return
        free = sorted(ORDERS[p][:k])

        def block(t, carry):
            place = [coords[0], coords[1], coords[2]]
            place[ORDERS[p][k]] = j
            if k == 2:
                a, b = t // 4, lax.rem(t, 4)
                place[free[0]], place[free[1]] = 2 * half + a, b
                inner = (a, b)
            else:
                place[free[0]] = 2 * half + t
                inner = (t,)
            place = tuple(place)
            total = sums[p][place].astype(F32)
            for n in slots:
                total = total + got[(n,) + inner].astype(F32)
            sums[p][place] = total.astype(BF16)
            return carry

        lax.fori_loop(0, 8 if k == 2 else 2, block, 0)

    for k in (2, 1, 0):
        copies = []
        for p in range(3):
            right, far, left = turn(p, k, 1), turn(p, k, 2), turn(p, k, 3)
            table = [
                scatter_copy(p, k, 0, far, 0, 1),
                scatter_copy(p, k, 1, right, 1, 1),
                scatter_copy(p, k, 2, far, 1, 3),
                scatter_copy(p, k, 3, left, 0, 3),
                scatter_copy(p, k, 4, right, 0, 1),
                scatter_copy(p, k, 5, left, 1, 3),
            ]
            copies.append(table)
            table[0].start()
            table[2].start()
            table[1].start()
            table[3].start()
        for p in range(3):
            copies[p][0].wait_recv()
            add_in(p, k, turn(p, k, 1), 0, (0,))
            copies[p][4].start()
            copies[p][2].wait_recv()
            add_in(p, k, turn(p, k, 3), 1, (2,))
            copies[p][5].start()
        for p in range(3):
            copies[p][3].wait_recv()
            copies[p][4].wait_recv()
            if k > 0:
                add_in(p, k, turn(p, k, 0), 0, (3, 4))
            copies[p][1].wait_recv()
            copies[p][5].wait_recv()
            if k > 0:
                add_in(p, k, turn(p, k, 0), 1, (1, 5))
        for p in range(3):
            for copy in copies[p]:
                copy.wait_send()

    for p in range(3):
        got = arrivals[0][p]
        for half, slots in ((0, (3, 4)), (1, (1, 5))):
            rows = pl.ds(16 * half, 16)
            total = sums[p][here[0], here[1], here[2], rows, :].astype(F32)
            for n in slots:
                total = total + got[n].astype(F32)
            cols = pl.ds(pl.multiple_of(own_cols + STARTS[p], 128), WIDTHS[p])
            kept = mid[rows, cols]
            out[rows, STARTS[p] : STARTS[p] + WIDTHS[p]] = (kept + total).astype(BF16)


def run_ffn(partial, stream, gain, meta, mix, eg, eu, ed, dg, du, dd):
    vmem = pl.BlockSpec(memory_space=VMEM)
    hbm = pl.BlockSpec(memory_space=ANY)
    blocks = lambda *lead: [VMEM((*lead, WIDTHS[p]), BF16) for p in range(3)]
    sem = pltpu.SemaphoreType.DMA
    return pl.pallas_call(
        ffn_kernel,
        out_shape=jax.ShapeDtypeStruct((ROWS, HALF), BF16),
        in_specs=[vmem] * 5 + [hbm] * 6,
        out_specs=vmem,
        scratch_shapes=[
            *[VMEM((4, 4, 4, BLOCK_ROWS[p], WIDTHS[p]), BF16) for p in range(3)],
            *blocks(4, 4, 4, ROWS),
            *blocks(4, 4, 4, ROWS),
            *blocks(6, 2, 4, ROWS),
            *blocks(6, 2, ROWS),
            *blocks(6, 16),
            VMEM((ROWS, 2 * HALF), BF16),
            VMEM((ROWS, 2 * HALF), BF16),
            VMEM((ROWS, 2 * HALF), F32),
            VMEM((HPAD, 2 * HALF), BF16),
            VMEM((HPAD, 2 * HALF), BF16),
            VMEM((HPAD, HALF), BF16),
            VMEM((HPAD, HALF), BF16),
            VMEM((256, HALF), BF16),
            VMEM((256, HALF), BF16),
            VMEM((DENSE, HALF), BF16),
            VMEM((128, HALF), BF16),
            VMEM((GROUPS * SLOTS, 2 * HALF), BF16),
            VMEM((GROUPS * SLOTS, 128), F32),
            VMEM((GROUPS * SLOTS, HPAD), BF16),
            VMEM((GROUPS * SLOTS, HPAD), BF16),
            VMEM((GROUPS, GROUP_ROWS, 256), BF16),
            VMEM((GROUPS, 128, HALF), BF16),
            sem((6,)),
            sem((54,)),
            sem((54,)),
            sem((21,)),
            sem((21,)),
            sem((54,)),
            sem((54,)),
            sem((6,)),
            sem((6,)),
        ],
        compiler_params=pltpu.CompilerParams(
            collective_id=0, has_side_effects=True, vmem_limit_bytes=60 * 2**20
        ),
        name="ffn",
    )(partial, stream, gain, meta, mix, eg, eu, ed, dg, du, dd)


def local(
    stream,
    mixer_gain,
    gate_proj,
    input_proj,
    state_maps,
    step_proj,
    step_bias,
    decay_rate,
    input_taps,
    map_taps,
    input_past,
    map_past,
    head_state,
    skip_gain,
    inner_gain,
    mixer_out,
    channel_gain,
    expert_ids,
    expert_weight,
    expert_gate,
    expert_up,
    expert_down,
    dense_gate,
    dense_up,
    dense_down,
    dense_mix,
):
    state_out, partial, meta = run_mixer(
        stream,
        mixer_gain.reshape(1, -1),
        step_proj.T,
        step_bias,
        decay_rate,
        skip_gain,
        input_taps,
        map_taps,
        jnp.transpose(input_past, (1, 0, 2)),
        jnp.transpose(map_past, (1, 2, 0, 3)).reshape(6, ROWS, 128),
        inner_gain.reshape(1, -1),
        expert_ids.T,
        expert_weight.T,
        gate_proj,
        input_proj,
        state_maps,
        mixer_out,
        head_state.reshape(256, 4096),
    )
    out = run_ffn(
        partial,
        stream,
        channel_gain.reshape(1, -1),
        meta,
        dense_mix.reshape(1, -1),
        expert_gate.T,
        expert_up.T,
        expert_down,
        dense_gate.T,
        dense_up.T,
        dense_down,
    )
    return out, state_out.reshape(head_state.shape)


def solution(mesh):
    placed = (
        P("ep", None),
        P(),
        P(None, "tp"),
        P(None, "tp"),
        P(None, None, "tp"),
        P(None, "tp"),
        P("tp"),
        P("tp"),
        P(None, "tp"),
        P(None, None, "tp"),
        P("ep", None, "tp"),
        P("ep", None, None, "tp"),
        P("ep", "tp", None),
        P("tp"),
        P("tp"),
        P("tp", None),
        P(),
        P("ep", None),
        P("ep", None),
        P(None, ("ep", "tp")),
        P(None, ("ep", "tp")),
        P(("ep", "tp"), None),
        P("tp", "ep"),
        P("tp", "ep"),
        P("ep", "tp"),
        P("tp"),
    )
    return jax.shard_map(
        local,
        mesh=mesh,
        in_specs=placed,
        out_specs=(P("ep", "tp"), P("ep", "tp", None)),
        check_vma=False,
    )
```

```python
import functools

import jax
import jax.numpy as jnp
from jax import lax
from jax.experimental import pallas as pl
from jax.experimental.pallas import tpu as pltpu
from jax.sharding import PartitionSpec as P

EPS = 1e-06
MESH = pl.DeviceIdType.MESH
F32 = jnp.float32
BF16 = jnp.bfloat16
VMEM = pltpu.VMEM
ANY = pl.ANY

HEADS = 8
ROWS = 32
EXPERTS = 8
CAP = 12
CHUNKS = 8
CHUNK = 512
GROUPS = 8
GROUP_ROWS = 256
SLOTS = 96
HALF = 1024
HIDDEN = 448
HPAD = 512
DENSE = 88

WIDTHS = (384, 384, 256)
STARTS = (0, 384, 768)
BLOCK_ROWS = (32, 32, 48)
ORDERS = ((2, 1, 0), (1, 0, 2), (0, 2, 1))


def dot(a, b):
    return jnp.dot(a, b, preferred_element_type=F32)


def dot_nt(a, b):
    return lax.dot_general(a, b, (((1,), (1,)), ((), ())), preferred_element_type=F32)


def dot_tn(a, b):
    return lax.dot_general(a, b, (((0,), (0,)), ((), ())), preferred_element_type=F32)


def silu(v):
    return v / (1.0 + jnp.exp(-v))


def rms(v):
    return v * lax.rsqrt(jnp.mean(v * v, axis=-1, keepdims=True) + EPS)


def split(v):
    high = v.astype(BF16)
    return high, (v - high.astype(F32)).astype(BF16)


def mixer_kernel(*refs):
    given, refs = refs[:18], refs[18:]
    state_hbm = given[17]
    state_out, partial, meta = refs[:3]
    held, refs = refs[3:20], refs[20:]
    (
        stream,
        mixer_gain,
        step_t,
        ids,
        weights,
        bias,
        decay,
        skip,
        input_w,
        input_taps,
        input_past,
        maps_w,
        map_taps,
        map_past,
        inner_gain,
        gate_w,
        out_w,
    ) = held
    old, new, dec, write, read, xs_high, xs_low, tmp, y, past, in_sems, sems = refs
    loads = [
        pltpu.make_async_copy(src, dst, in_sems.at[n])
        for n, (src, dst) in enumerate(zip(given, held))
    ]

    def load_state(t):
        cols = pl.ds(pl.multiple_of(t * CHUNK, CHUNK), CHUNK)
        return pltpu.make_async_copy(state_hbm.at[:, cols], old.at[t], sems.at[t])

    def store_state(t):
        cols = pl.ds(pl.multiple_of(t * CHUNK, CHUNK), CHUNK)
        return pltpu.make_async_copy(
            new.at[t], state_out.at[:, cols], sems.at[CHUNKS + t]
        )

    for load in loads[:15]:
        load.start()
    for t in range(CHUNKS):
        load_state(t).start()
    loads[15].start()
    loads[16].start()

    for load in loads[:8]:
        load.wait()
    normed = (rms(stream[...].astype(F32)) * mixer_gain[...]).astype(BF16)
    steps = dot_nt(normed, step_t[...])

    expert_of = lax.broadcasted_iota(jnp.int32, (EXPERTS, ROWS), 0)
    hit0 = (ids[0:1, :] == expert_of).astype(F32)
    hit1 = (ids[1:2, :] == expert_of).astype(F32)
    member = hit0 + hit1
    upper = (
        lax.broadcasted_iota(jnp.int32, (ROWS, ROWS), 0)
        <= lax.broadcasted_iota(jnp.int32, (ROWS, ROWS), 1)
    ).astype(BF16)
    rank = dot(member.astype(BF16), upper) * member
    weight = hit0 * weights[0:1, :] + hit1 * weights[1:2, :]
    w_high = weight.astype(BF16).astype(F32)
    w_low = weight - w_high
    table = jnp.concatenate(
        [rank, w_high, w_low, jnp.zeros((104, ROWS), F32)], axis=0
    ).astype(BF16)
    eye = (
        lax.broadcasted_iota(jnp.int32, (ROWS, ROWS), 0)
        == lax.broadcasted_iota(jnp.int32, (ROWS, ROWS), 1)
    ).astype(BF16)
    by_row = dot_nt(eye, table)
    meta[...] = jnp.concatenate([by_row[0:16], by_row[16:32]], axis=1).astype(BF16)

    for load in loads[8:11]:
        load.wait()
    newest = dot(normed, input_w[...]).astype(BF16).astype(F32)
    conv = newest * input_taps[3:4, :]
    for t in range(3):
        conv = conv + input_past[t].astype(F32) * input_taps[t : t + 1, :]
    conv = silu(conv)

    for load in loads[11:14]:
        load.wait()
    past[...] = map_past[...].astype(F32)
    conv_maps = []
    for m in range(2):
        new_map = dot(normed, maps_w[m]).astype(BF16).astype(F32)
        acc = new_map * map_taps[m, 3:4, :]
        for t in range(3):
            acc = acc + past[pl.ds(2 * t + m, ROWS, stride=6), :] * map_taps[m, t : t + 1, :]
        conv_maps.append(silu(acc))

    lane = lax.broadcasted_iota(jnp.int32, (ROWS, 128), 1)
    low_half = lane < 64

    def both_halves(v):
        turned = pltpu.roll(v, 64, 1)
        return jnp.where(low_half, v, turned), jnp.where(low_half, turned, v)

    write_by_group = both_halves(conv_maps[0])
    read_by_group = both_halves(conv_maps[1])
    for h in range(HEADS):
        rows = pl.ds(h, ROWS, stride=HEADS)
        v = jnp.broadcast_to(steps[:, h : h + 1], (ROWS, 128)) + bias[h]
        step = jnp.maximum(v, 0.0) + jnp.log1p(jnp.exp(-jnp.abs(v)))
        dec[rows, :] = jnp.exp(-decay[h] * step)
        pair = conv[:, 128 * (h // 2) : 128 * (h // 2) + 128]
        mine = low_half if h % 2 == 0 else jnp.logical_not(low_half)
        tmp[rows, :] = jnp.where(mine, step * pair, 0.0)
        write[rows, :] = write_by_group[h // 4]
        read[rows, :] = read_by_group[h // 4]
    high, low = split(tmp[...])
    xs_high[...] = high
    xs_low[...] = low
    y[...] = jnp.zeros_like(y)

    slot = lax.broadcasted_iota(jnp.int32, (128, CHUNK), 0) % 64
    place = lax.broadcasted_iota(jnp.int32, (128, CHUNK), 1) // 64

    def chunk_step(t, carry):
        spread = (slot == place + 8 * t).astype(F32).astype(BF16)
        load_state(t).wait()
        values = dot(xs_high[...], spread) + dot(xs_low[...], spread)
        wide = lambda ref: jnp.concatenate([ref[...]] * (CHUNK // 128), axis=1)
        fresh = wide(dec) * old[t] + values * wide(write)
        new[t] = fresh
        store_state(t).start()
        high, low = split(fresh * wide(read))
        y[...] += dot_nt(high, spread) + dot_nt(low, spread)
        return carry

    lax.fori_loop(0, CHUNKS, chunk_step, 0)

    loads[14].wait()
    loads[15].wait()
    gate = silu(dot(normed, gate_w[...]).astype(BF16).astype(F32))
    pieces = []
    for j in range(HEADS // 2):
        even = y[pl.ds(2 * j, ROWS, stride=HEADS), :]
        odd = y[pl.ds(2 * j + 1, ROWS, stride=HEADS), :]
        gain = jnp.where(low_half, skip[2 * j], skip[2 * j + 1])
        cols = slice(128 * j, 128 * j + 128)
        pieces.append(
            (jnp.where(low_half, even, odd) + gain * conv[:, cols]) * gate[:, cols]
        )
    groups = [jnp.concatenate(pieces[2 * g : 2 * g + 2], axis=1) for g in range(2)]
    inner = jnp.concatenate([rms(g) for g in groups], axis=1) * inner_gain[...]
    loads[16].wait()
    partial[...] = dot(inner.astype(BF16), out_w[...]).astype(BF16)
    for t in range(CHUNKS):
        store_state(t).wait()


def run_mixer(*given):
    vmem = pl.BlockSpec(memory_space=VMEM)
    hbm = pl.BlockSpec(memory_space=pltpu.HBM)
    lanes = lambda: VMEM((256, 128), F32)
    held = [
        (pltpu.SMEM if 5 <= n < 8 else VMEM)(v.shape, v.dtype)
        for n, v in enumerate(given[:17])
    ]
    return pl.pallas_call(
        mixer_kernel,
        out_shape=(
            jax.ShapeDtypeStruct((256, 4096), F32),
            jax.ShapeDtypeStruct((ROWS, 2 * HALF), BF16),
            jax.ShapeDtypeStruct((16, 256), BF16),
        ),
        in_specs=[hbm] * 18,
        out_specs=(hbm, vmem, vmem),
        scratch_shapes=[
            *held,
            VMEM((CHUNKS, 256, CHUNK), F32),
            VMEM((CHUNKS, 256, CHUNK), F32),
            lanes(),
            lanes(),
            lanes(),
            VMEM((256, 128), BF16),
            VMEM((256, 128), BF16),
            lanes(),
            lanes(),
            VMEM((192, 128), F32),
            pltpu.SemaphoreType.DMA((17,)),
            pltpu.SemaphoreType.DMA((2 * CHUNKS,)),
        ],
        compiler_params=pltpu.CompilerParams(vmem_limit_bytes=67043328),
        name="mixer",
    )(*given)


def ffn_kernel(
    partial,
    meta,
    stream_hbm,
    gain_hbm,
    mix_hbm,
    eg_hbm,
    eu_hbm,
    ed_hbm,
    dg_hbm,
    du_hbm,
    dd_hbm,
    out,
    x0,
    x1,
    x2,
    y0,
    y1,
    y2,
    s0,
    s1,
    s2,
    *rest,
):
    landed, rest = rest[:18], rest[18:]
    landing = [(landed[6 * k : 6 * k + 3], landed[6 * k + 3 : 6 * k + 6]) for k in range(3)]
    (
    other_partial,
    wide,
    mid,
    eg,
    eu,
    ed,
    ed_other,
    dgu,
    dgu_other,
    dd,
    dd_scaled,
    packed,
    slot_weight,
    act,
    act_other,
    left_side,
    result,
    local_sem,
    ag_send,
    ag_recv,
    dd_send,
    dd_recv,
    rs_send,
    rs_recv,
    mi_send,
    mi_recv,
    stream,
    gain,
    mix,
    small_sem,
    ) = rest
    ep = lax.axis_index("ep")
    core = lax.axis_index("tp")
    coords = (ep // 16, (ep // 4) % 4, ep % 4)
    other = 1 - core
    own_cols = pl.multiple_of(core * HALF, HALF)
    other_cols = pl.multiple_of(other * HALF, HALF)
    expert = ep // 8
    mine = (x0, x1, x2)
    theirs = (y0, y1, y2)
    sums = (s0, s1, s2)

    def neighbour(dim, shift):
        moved = list(coords)
        moved[dim] = lax.rem(coords[dim] + shift, 4)
        return (moved[0] * 16 + moved[1] * 4 + moved[2], core)

    partner = (ep, other)

    small = [
        pltpu.make_async_copy(stream_hbm, stream, small_sem.at[0]),
        pltpu.make_async_copy(gain_hbm, gain, small_sem.at[1]),
        pltpu.make_async_copy(mix_hbm, mix, small_sem.at[2]),
    ]
    for load in small:
        load.start()
    barrier = pltpu.get_barrier_semaphore()
    for dim in range(3):
        for shift in (1, 3):
            pl.semaphore_signal(
                barrier, inc=1, device_id=neighbour(dim, shift), device_id_type=MESH
            )
    pl.semaphore_signal(barrier, inc=1, device_id=partner, device_id_type=MESH)
    pl.semaphore_wait(barrier, 7)

    def to_partner(src, dst, n):
        return pltpu.make_async_remote_copy(
            src_ref=src,
            dst_ref=dst,
            send_sem=mi_send.at[n],
            recv_sem=mi_recv.at[n],
            device_id=partner,
            device_id_type=MESH,
        )

    swap_partial = to_partner(partial, other_partial, 0)
    swap_partial.start()
    loads = [
        pltpu.make_async_copy(eg_hbm, eg.at[pl.ds(0, HIDDEN)], local_sem.at[0]),
        pltpu.make_async_copy(eu_hbm, eu.at[pl.ds(0, HIDDEN)], local_sem.at[1]),
        pltpu.make_async_copy(
            ed_hbm.at[:, pl.ds(own_cols, HALF)], ed.at[pl.ds(0, HIDDEN)], local_sem.at[2]
        ),
        pltpu.make_async_copy(dg_hbm, dgu.at[pl.ds(0, DENSE)], local_sem.at[3]),
        pltpu.make_async_copy(du_hbm, dgu.at[pl.ds(128, DENSE)], local_sem.at[4]),
        pltpu.make_async_copy(dd_hbm, dd, local_sem.at[5]),
    ]
    for load in loads:
        load.start()

    for load in small:
        load.wait()
    swap_partial.wait()
    mixed = partial[...].astype(F32) + other_partial[...].astype(F32)
    hidden = stream[...].astype(F32) + mixed
    mid[...] = hidden
    wide[...] = (rms(hidden) * gain[...]).astype(BF16)
    here = coords
    for p in range(3):
        cols = pl.ds(pl.multiple_of(own_cols + STARTS[p], 128), WIDTHS[p])
        mine[p][here[0], here[1], here[2], 0:ROWS, :] = wide[:, cols]
    x2[here[0], here[1], here[2], ROWS : ROWS + 16, :] = meta[...]

    def cut(buf, p, where, half=None, rows=None):
        index = [None, None, None]
        for q in range(3):
            index[ORDERS[p][q]] = pl.ds(0, 4) if where[q] is None else where[q]
        if half is not None:
            free = sorted(ORDERS[p][q] for q in range(3) if where[q] is None)
            if free:
                index[free[0]] = pl.ds(2 * half, 2)
            else:
                rows = pl.ds(0, 16) if half == 0 else pl.ds(16, rows - 16)
        elif rows is not None:
            rows = pl.ds(0, rows)
        if rows is not None and not (half is not None and free):
            index.append(rows)
        return buf.at[tuple(index)]

    def turn(p, k, shift):
        return lax.rem(coords[ORDERS[p][k]] + shift, 4)

    ME, RIGHT, FAR, LEFT = 0, 1, 2, 3
    spots = [[[turn(p, k, shift) for shift in range(4)] for k in range(3)] for p in range(3)]

    class Ring:
        def __init__(self, p, k, at, place):
            self.p, self.k, self.place = p, k, place
            self.copies = [
                self.copy(at, ME, None, 1),
                self.copy(at + 1, ME, None, 3),
                self.copy(at + 2, LEFT, 0, 1),
                self.copy(at + 3, RIGHT, 1, 3),
            ]

        def copy(self, at, shift, half, to):
            p = self.p
            where = list(self.place)
            where[self.k] = spots[p][self.k][shift]
            rows = BLOCK_ROWS[p] if half is not None else None
            ref = cut(mine[p], p, where, half, rows)
            return pltpu.make_async_remote_copy(
                src_ref=ref,
                dst_ref=ref,
                send_sem=ag_send.at[at],
                recv_sem=ag_recv.at[at],
                device_id=neighbour(ORDERS[p][self.k], to),
                device_id_type=MESH,
            )

        def start(self):
            self.copies[0].start()
            self.copies[1].start()

        def on(self):
            self.copies[0].wait_recv()
            self.copies[2].start()
            self.copies[1].wait_recv()
            self.copies[3].start()

        def end(self):
            self.copies[2].wait_recv()
            self.copies[3].wait_recv()

    first, second, blocks, lines = [], [], [], []
    for p in range(3):
        at = 48 * p
        own = [spots[p][k][ME] for k in range(3)]
        first.append(Ring(p, 0, at, own))
        second.append(
            [Ring(p, 1, at + 4 + 4 * u, [spots[p][0][u], None, own[2]]) for u in range(4)]
        )
        blocks.append(
            [Ring(p, 2, at + 20 + 4 * u, [spots[p][0][u], own[1], None]) for u in range(4)]
        )
        lines.append(
            [Ring(p, 2, at + 36 + 4 * (u - 1), [None, spots[p][1][u], None]) for u in (1, 2, 3)]
        )
    rings = [first] + second + blocks + lines
    hand_overs = []

    def hand_over(p, n, second_at, third_at):
        where = [None, second_at, third_at]
        copy = pltpu.make_async_remote_copy(
            src_ref=cut(mine[p], p, where, None, ROWS),
            dst_ref=cut(theirs[p], p, where, None, ROWS),
            send_sem=dd_send.at[13 * p + n],
            recv_sem=dd_recv.at[13 * p + n],
            device_id=partner,
            device_id_type=MESH,
        )
        copy.start()
        hand_overs.append(copy)

    parts = range(3)
    for p in parts:
        first[p].start()
    for p in parts:
        second[p][ME].start()
    for p in parts:
        blocks[p][ME].start()

    early = [
        to_partner(
            ed_hbm.at[:, pl.ds(other_cols, HALF)], ed_other.at[pl.ds(0, HIDDEN)], 1
        ),
        to_partner(dg_hbm, dgu_other.at[pl.ds(0, DENSE)], 2),
        to_partner(du_hbm, dgu_other.at[pl.ds(128, DENSE)], 3),
    ]
    for copy in early:
        copy.start()

    for p in parts:
        first[p].on()
        for u in (LEFT, RIGHT):
            second[p][u].start()
            blocks[p][u].start()
    for p in parts:
        second[p][ME].on()
    for p in parts:
        blocks[p][ME].on()
    for p in parts:
        first[p].end()
        second[p][FAR].start()
        blocks[p][FAR].start()
    for p in parts:
        second[p][LEFT].on()
        second[p][RIGHT].on()
    for p in parts:
        blocks[p][LEFT].on()
        blocks[p][RIGHT].on()
    for p in parts:
        second[p][FAR].on()
        lines[p][RIGHT - 1].start()
        lines[p][LEFT - 1].start()
    for ref in (eg, eu, ed, ed_other):
        ref[HIDDEN:HPAD, :] = jnp.zeros((HPAD - HIDDEN, ref.shape[1]), BF16)
    for ref in (dgu, dgu_other):
        ref[DENSE:128, :] = jnp.zeros((128 - DENSE, HALF), BF16)
        ref[128 + DENSE : 256, :] = jnp.zeros((128 - DENSE, HALF), BF16)
    dd_scaled[DENSE:128, :] = jnp.zeros((128 - DENSE, HALF), BF16)
    for g in range(GROUPS):
        result[g, SLOTS:128, :] = jnp.zeros((128 - SLOTS, HALF), BF16)
    for p in parts:
        for u in range(4):
            second[p][u].end()
        lines[p][FAR - 1].start()
        hand_over(p, 0, None, spots[p][2][ME])
    for p in parts:
        blocks[p][FAR].on()
        hand_over(p, 1, spots[p][1][ME], spots[p][2][LEFT])
        hand_over(p, 2, spots[p][1][ME], spots[p][2][RIGHT])
    for n, u in ((3, RIGHT), (6, LEFT), (9, FAR)):
        for p in parts:
            lines[p][u - 1].on()
            hand_over(p, n, spots[p][1][u], spots[p][2][LEFT])
            hand_over(p, n + 1, spots[p][1][u], spots[p][2][RIGHT])
        for p in parts:
            if u == RIGHT:
                for v in range(4):
                    blocks[p][v].end()
                hand_over(p, n + 2, spots[p][1][ME], spots[p][2][FAR])
            else:
                done = RIGHT if u == LEFT else LEFT
                lines[p][done - 1].end()
                hand_over(p, n + 2, spots[p][1][done], spots[p][2][FAR])
    for p in parts:
        lines[p][FAR - 1].end()
        hand_over(p, 12, spots[p][1][FAR], spots[p][2][FAR])
    for load in loads:
        load.wait()
    for copy in early:
        copy.wait()
    for group in rings:
        for ring in group:
            for copy in ring.copies:
                copy.wait_send()
    for copy in hand_overs:
        copy.wait()

    pick_row = lax.broadcasted_iota(jnp.int32, (128, 128), 0)
    pick_rank = (pick_row == expert).astype(F32).astype(BF16)
    pick_weight = (
        jnp.logical_or(pick_row == expert + 8, pick_row == expert + 16)
    ).astype(F32).astype(BF16)
    lane = lax.broadcasted_iota(jnp.int32, (GROUP_ROWS, 128), 1)
    source = lax.broadcasted_iota(jnp.int32, (GROUP_ROWS, 128), 0) // ROWS

    def group_of(bufs, g):
        z, y = g // 2, 2 * lax.rem(g, 2)
        return jnp.concatenate(
            [
                bufs[p][z, pl.ds(y, 2), :, 0:ROWS, :].reshape(GROUP_ROWS, WIDTHS[p])
                for p in range(3)
            ],
            axis=1,
        )

    def pack_group(g, carry):
        z, y = g // 2, 2 * lax.rem(g, 2)
        tags = x2[z, pl.ds(y, 2), :, ROWS : ROWS + 16, :].reshape(8, 16, 256)
        tags = jnp.concatenate([tags[:, :, 0:128], tags[:, :, 128:256]], axis=1)
        tags = tags.reshape(GROUP_ROWS, 128)
        rank = dot(tags, pick_rank).astype(jnp.int32)
        hit = jnp.logical_and(rank > 0, rank + (CAP * source - 1) == lane)
        table = hit.astype(F32).astype(BF16)
        left_side[g, :, 0:128] = table
        used = table[:, 0:SLOTS]
        slots = pl.ds(pl.multiple_of(g * SLOTS, SLOTS), SLOTS)
        packed[slots, pl.ds(own_cols, HALF)] = dot_tn(used, group_of(mine, g)).astype(BF16)
        packed[slots, pl.ds(other_cols, HALF)] = dot_tn(used, group_of(theirs, g)).astype(
            BF16
        )
        slot_tags = dot_tn(used, tags).astype(BF16)
        slot_weight[slots, :] = dot(slot_tags, pick_weight)
        return carry

    lax.fori_loop(0, GROUPS, pack_group, 0)

    sends = []
    for i in range(2):
        rows = pl.ds(i * 384, 384)
        taken = packed[rows, :]
        gate = dot_nt(taken, eg[...])
        up = dot_nt(taken, eu[...])
        act[rows, :] = (silu(gate) * up * slot_weight[rows, 0:1]).astype(BF16)
        copy = to_partner(act.at[rows], act_other.at[rows], 4 + i)
        copy.start()
        sends.append(copy)

    def dense_group(g, carry):
        both = dot_nt(group_of(mine, g), dgu[...]) + dot_nt(group_of(theirs, g), dgu_other[...])
        left_side[g, :, 128:256] = (silu(both[:, 0:128]) * both[:, 128:256]).astype(BF16)
        return carry

    lax.fori_loop(0, GROUPS, dense_group, 0)
    share = 1.0 / (1.0 + jnp.exp(-mix[...]))
    dd_scaled[0:DENSE, :] = (dd[...].astype(F32) * share).astype(BF16)

    for i in range(2):
        rows = pl.ds(i * 384, 384)
        sends[i].wait()
        back = dot(act[rows, :], ed[...]) + dot(act_other[rows, :], ed_other[...])
        result[pl.ds(4 * i, 4), 0:SLOTS, :] = back.astype(BF16).reshape(4, SLOTS, HALF)

    def spread_group(g, carry):
        z, y = g // 2, 2 * lax.rem(g, 2)
        total = dot(left_side[g], jnp.concatenate([result[g], dd_scaled[...]], axis=0))
        for p in range(3):
            cut = total[:, STARTS[p] : STARTS[p] + WIDTHS[p]].astype(BF16)
            sums[p][z, pl.ds(y, 2)] = cut.reshape(2, 4, ROWS, WIDTHS[p])
        return carry

    lax.fori_loop(0, GROUPS, spread_group, 0)

    class Back:
        def __init__(self, p, k, at, place, slot):
            self.p, self.k, self.place, self.slot = p, k, place, slot
            self.halves, self.wholes = landing[k][0][p], landing[k][1][p]
            self.copies = [
                self.copy(at, FAR, 0, 1, self.halves.at[slot, 0]),
                self.copy(at + 1, FAR, 1, 3, self.halves.at[slot, 1]),
                self.copy(at + 2, RIGHT, None, 1, self.wholes.at[slot, 0]),
                self.copy(at + 3, LEFT, None, 3, self.wholes.at[slot, 1]),
            ]

        def spot(self, shift):
            where = list(self.place)
            where[self.k] = spots[self.p][self.k][shift]
            return where

        def copy(self, at, shift, half, to, target):
            p = self.p
            rows = ROWS if half is not None else None
            return pltpu.make_async_remote_copy(
                src_ref=cut(sums[p], p, self.spot(shift), half, rows),
                dst_ref=target,
                send_sem=rs_send.at[at],
                recv_sem=rs_recv.at[at],
                device_id=neighbour(ORDERS[p][self.k], to),
                device_id_type=MESH,
            )

        def start(self):
            self.copies[0].start()
            self.copies[1].start()

        def add_half(self, shift, half):
            p, got = self.p, self.halves
            where = self.spot(shift)
            place = [None, None, None]
            for q in range(3):
                place[ORDERS[p][q]] = where[q]
            free = [d for d in range(3) if place[d] is None]
            if not free:
                rows = pl.ds(16 * half, 16)
                ref = sums[p].at[tuple(place) + (rows,)]
                ref[...] = ref[...] + got[self.slot, half]
                return
            for t in range(2):
                place[free[0]] = 2 * half + t
                ref = sums[p].at[tuple(place)]
                ref[...] = ref[...] + got[self.slot, half, t]

        def on(self):
            self.copies[0].wait_recv()
            self.add_half(RIGHT, 0)
            self.copies[2].start()
            self.copies[1].wait_recv()
            self.add_half(LEFT, 1)
            self.copies[3].start()

        def arrive(self):
            self.copies[2].wait_recv()
            self.copies[3].wait_recv()

        def end(self):
            p, got = self.p, self.wholes
            self.arrive()
            where = self.spot(ME)
            place = [None, None, None]
            for q in range(3):
                place[ORDERS[p][q]] = where[q]
            free = [d for d in range(3) if place[d] is None]
            for t in range(4):
                place[free[0]] = t
                ref = sums[p].at[tuple(place)]
                total = ref[...].astype(F32) + got[self.slot, 0, t].astype(F32)
                ref[...] = (total + got[self.slot, 1, t].astype(F32)).astype(BF16)

    third, middle, last = [], [], []
    for p in parts:
        at = 24 * p
        own = [spots[p][k][ME] for k in range(3)]
        third.append(
            [Back(p, 2, at + 4 * u, [None, spots[p][1][u], None], u) for u in range(4)]
        )
        middle.append(Back(p, 1, at + 16, [None, None, own[2]], 0))
        last.append(Back(p, 0, at + 20, own, 0))
    order = (FAR, LEFT, RIGHT, ME)
    for u in order:
        for p in parts:
            third[p][u].start()
    for u in order:
        for p in parts:
            third[p][u].on()
    for u in order:
        for p in parts:
            third[p][u].end()
            if u == FAR:
                middle[p].start()
        if u == RIGHT:
            for p in parts:
                middle[p].on()
    for p in parts:
        middle[p].end()
        last[p].start()
    for p in parts:
        last[p].on()
    for p in parts:
        last[p].arrive()
        got = last[p].wholes
        total = mid[:, pl.ds(pl.multiple_of(own_cols + STARTS[p], 128), WIDTHS[p])]
        total = total + sums[p][here[0], here[1], here[2]].astype(F32)
        total = total + got[0, 0].astype(F32) + got[0, 1].astype(F32)
        out[:, STARTS[p] : STARTS[p] + WIDTHS[p]] = total.astype(BF16)
    for group in third + [middle, last]:
        for back in group:
            for copy in back.copies:
                copy.wait_send()


def run_ffn(partial, meta, stream, gain, mix, eg, eu, ed, dg, du, dd):
    vmem = pl.BlockSpec(memory_space=VMEM)
    hbm = pl.BlockSpec(memory_space=pltpu.HBM)
    blocks = lambda *lead: [VMEM((*lead, WIDTHS[p]), BF16) for p in range(3)]
    sem = pltpu.SemaphoreType.DMA
    return pl.pallas_call(
        ffn_kernel,
        out_shape=jax.ShapeDtypeStruct((ROWS, HALF), BF16),
        in_specs=[vmem] * 2 + [hbm] * 9,
        out_specs=vmem,
        scratch_shapes=[
            *[VMEM((4, 4, 4, BLOCK_ROWS[p], WIDTHS[p]), BF16) for p in range(3)],
            *blocks(4, 4, 4, ROWS),
            *blocks(4, 4, 4, ROWS),
            *blocks(1, 2, 16),
            *blocks(1, 2, ROWS),
            *blocks(1, 2, 2, ROWS),
            *blocks(1, 2, 4, ROWS),
            *blocks(4, 2, 2, ROWS),
            *blocks(4, 2, 4, ROWS),
            VMEM((ROWS, 2 * HALF), BF16),
            VMEM((ROWS, 2 * HALF), BF16),
            VMEM((ROWS, 2 * HALF), F32),
            VMEM((HPAD, 2 * HALF), BF16),
            VMEM((HPAD, 2 * HALF), BF16),
            VMEM((HPAD, HALF), BF16),
            VMEM((HPAD, HALF), BF16),
            VMEM((256, HALF), BF16),
            VMEM((256, HALF), BF16),
            VMEM((DENSE, HALF), BF16),
            VMEM((128, HALF), BF16),
            VMEM((GROUPS * SLOTS, 2 * HALF), BF16),
            VMEM((GROUPS * SLOTS, 128), F32),
            VMEM((GROUPS * SLOTS, HPAD), BF16),
            VMEM((GROUPS * SLOTS, HPAD), BF16),
            VMEM((GROUPS, GROUP_ROWS, 256), BF16),
            VMEM((GROUPS, 128, HALF), BF16),
            sem((6,)),
            sem((144,)),
            sem((144,)),
            sem((39,)),
            sem((39,)),
            sem((72,)),
            sem((72,)),
            sem((6,)),
            sem((6,)),
            VMEM((ROWS, 2 * HALF), BF16),
            VMEM((1, 2 * HALF), F32),
            VMEM((1, HALF), F32),
            sem((3,)),
        ],
        compiler_params=pltpu.CompilerParams(
            collective_id=0, has_side_effects=True, vmem_limit_bytes=67043328
        ),
        name="ffn",
    )(partial, meta, stream, gain, mix, eg, eu, ed, dg, du, dd)


def local(
    stream,
    mixer_gain,
    gate_proj,
    input_proj,
    state_maps,
    step_proj,
    step_bias,
    decay_rate,
    input_taps,
    map_taps,
    input_past,
    map_past,
    head_state,
    skip_gain,
    inner_gain,
    mixer_out,
    channel_gain,
    expert_ids,
    expert_weight,
    expert_gate,
    expert_up,
    expert_down,
    dense_gate,
    dense_up,
    dense_down,
    dense_mix,
):
    state_out, partial, meta = run_mixer(
        stream,
        mixer_gain.reshape(1, -1),
        step_proj.T,
        expert_ids.T,
        expert_weight.T,
        step_bias,
        decay_rate,
        skip_gain,
        input_proj,
        input_taps,
        jnp.transpose(input_past, (1, 0, 2)),
        state_maps,
        map_taps,
        jnp.transpose(map_past, (0, 2, 1, 3)).reshape(192, 128),
        inner_gain.reshape(1, -1),
        gate_proj,
        mixer_out,
        head_state.reshape(256, 4096),
    )
    out = run_ffn(
        partial,
        meta,
        stream,
        channel_gain.reshape(1, -1),
        dense_mix.reshape(1, -1),
        expert_gate.T,
        expert_up.T,
        expert_down,
        dense_gate.T,
        dense_up.T,
        dense_down,
    )
    return out, state_out.reshape(head_state.shape)


def solution(mesh):
    placed = (
        P("ep", None),
        P(),
        P(None, "tp"),
        P(None, "tp"),
        P(None, None, "tp"),
        P(None, "tp"),
        P("tp"),
        P("tp"),
        P(None, "tp"),
        P(None, None, "tp"),
        P("ep", None, "tp"),
        P("ep", None, None, "tp"),
        P("ep", "tp", None),
        P("tp"),
        P("tp"),
        P("tp", None),
        P(),
        P("ep", None),
        P("ep", None),
        P(None, ("ep", "tp")),
        P(None, ("ep", "tp")),
        P(("ep", "tp"), None),
        P("tp", "ep"),
        P("tp", "ep"),
        P("ep", "tp"),
        P("tp"),
    )
    return jax.shard_map(
        local,
        mesh=mesh,
        in_specs=placed,
        out_specs=(P("ep", "tp"), P("ep", "tp", None)),
        check_vma=False,
    )
```

```python
import functools

import jax
import jax.numpy as jnp
from jax import lax
from jax.experimental import pallas as pl
from jax.experimental.pallas import tpu as pltpu
from jax.sharding import PartitionSpec as P

EPS = 1e-06
MESH = pl.DeviceIdType.MESH
F32 = jnp.float32
BF16 = jnp.bfloat16
VMEM = pltpu.VMEM
ANY = pl.ANY

HEADS = 8
ROWS = 32
EXPERTS = 8
CAP = 12
CHUNKS = 8
CHUNK = 512
GROUPS = 8
GROUP_ROWS = 256
SLOTS = 96
HALF = 1024
HIDDEN = 448
HPAD = 512
DENSE = 88

WIDTHS = (384, 384, 256)
STARTS = (0, 384, 768)
BLOCK_ROWS = (32, 32, 48)
ORDERS = ((2, 1, 0), (1, 0, 2), (0, 2, 1))


def dot(a, b):
    return jnp.dot(a, b, preferred_element_type=F32)


def dot_nt(a, b):
    return lax.dot_general(a, b, (((1,), (1,)), ((), ())), preferred_element_type=F32)


def dot_tn(a, b):
    return lax.dot_general(a, b, (((0,), (0,)), ((), ())), preferred_element_type=F32)


def silu(v):
    return v / (1.0 + jnp.exp(-v))


def rms(v):
    return v * lax.rsqrt(jnp.mean(v * v, axis=-1, keepdims=True) + EPS)


def split(v):
    high = v.astype(BF16)
    return high, (v - high.astype(F32)).astype(BF16)


def mixer_kernel(*refs):
    given, refs = refs[:18], refs[18:]
    state_hbm = given[17]
    state_out, partial, meta = refs[:3]
    held, refs = refs[3:20], refs[20:]
    (
        stream,
        mixer_gain,
        step_t,
        ids,
        weights,
        bias,
        decay,
        skip,
        input_w,
        input_taps,
        input_past,
        maps_w,
        map_taps,
        map_past,
        inner_gain,
        gate_w,
        out_w,
    ) = held
    old, new, dec, write, read, xs_high, xs_low, tmp, y, past, in_sems, sems = refs
    loads = [
        pltpu.make_async_copy(src, dst, in_sems.at[n])
        for n, (src, dst) in enumerate(zip(given, held))
    ]

    def load_state(t):
        cols = pl.ds(pl.multiple_of(t * CHUNK, CHUNK), CHUNK)
        return pltpu.make_async_copy(state_hbm.at[:, cols], old.at[t], sems.at[t])

    def store_state(t):
        cols = pl.ds(pl.multiple_of(t * CHUNK, CHUNK), CHUNK)
        return pltpu.make_async_copy(
            new.at[t], state_out.at[:, cols], sems.at[CHUNKS + t]
        )

    for load in loads[:15]:
        load.start()
    for t in range(CHUNKS):
        load_state(t).start()
    loads[15].start()
    loads[16].start()

    for load in loads[:8]:
        load.wait()
    normed = (rms(stream[...].astype(F32)) * mixer_gain[...]).astype(BF16)
    steps = dot_nt(normed, step_t[...])

    expert_of = lax.broadcasted_iota(jnp.int32, (EXPERTS, ROWS), 0)
    hit0 = (ids[0:1, :] == expert_of).astype(F32)
    hit1 = (ids[1:2, :] == expert_of).astype(F32)
    member = hit0 + hit1
    upper = (
        lax.broadcasted_iota(jnp.int32, (ROWS, ROWS), 0)
        <= lax.broadcasted_iota(jnp.int32, (ROWS, ROWS), 1)
    ).astype(BF16)
    rank = dot(member.astype(BF16), upper) * member
    weight = hit0 * weights[0:1, :] + hit1 * weights[1:2, :]
    w_high = weight.astype(BF16).astype(F32)
    w_low = weight - w_high
    table = jnp.concatenate(
        [rank, w_high, w_low, jnp.zeros((104, ROWS), F32)], axis=0
    ).astype(BF16)
    eye = (
        lax.broadcasted_iota(jnp.int32, (ROWS, ROWS), 0)
        == lax.broadcasted_iota(jnp.int32, (ROWS, ROWS), 1)
    ).astype(BF16)
    by_row = dot_nt(eye, table)
    meta[...] = jnp.concatenate([by_row[0:16], by_row[16:32]], axis=1).astype(BF16)

    for load in loads[8:11]:
        load.wait()
    newest = dot(normed, input_w[...]).astype(BF16).astype(F32)
    conv = newest * input_taps[3:4, :]
    for t in range(3):
        conv = conv + input_past[t].astype(F32) * input_taps[t : t + 1, :]
    conv = silu(conv)

    for load in loads[11:14]:
        load.wait()
    past[...] = map_past[...].astype(F32)
    conv_maps = []
    for m in range(2):
        new_map = dot(normed, maps_w[m]).astype(BF16).astype(F32)
        acc = new_map * map_taps[m, 3:4, :]
        for t in range(3):
            acc = acc + past[pl.ds(2 * t + m, ROWS, stride=6), :] * map_taps[m, t : t + 1, :]
        conv_maps.append(silu(acc))

    lane = lax.broadcasted_iota(jnp.int32, (ROWS, 128), 1)
    low_half = lane < 64

    def both_halves(v):
        turned = pltpu.roll(v, 64, 1)
        return jnp.where(low_half, v, turned), jnp.where(low_half, turned, v)

    write_by_group = both_halves(conv_maps[0])
    read_by_group = both_halves(conv_maps[1])
    for h in range(HEADS):
        rows = pl.ds(h, ROWS, stride=HEADS)
        v = jnp.broadcast_to(steps[:, h : h + 1], (ROWS, 128)) + bias[h]
        step = jnp.maximum(v, 0.0) + jnp.log1p(jnp.exp(-jnp.abs(v)))
        dec[rows, :] = jnp.exp(-decay[h] * step)
        pair = conv[:, 128 * (h // 2) : 128 * (h // 2) + 128]
        mine = low_half if h % 2 == 0 else jnp.logical_not(low_half)
        tmp[rows, :] = jnp.where(mine, step * pair, 0.0)
        write[rows, :] = write_by_group[h // 4]
        read[rows, :] = read_by_group[h // 4]
    high, low = split(tmp[...])
    xs_high[...] = high
    xs_low[...] = low
    y[...] = jnp.zeros_like(y)

    slot = lax.broadcasted_iota(jnp.int32, (128, CHUNK), 0) % 64
    place = lax.broadcasted_iota(jnp.int32, (128, CHUNK), 1) // 64

    def chunk_step(t, carry):
        spread = (slot == place + 8 * t).astype(F32).astype(BF16)
        load_state(t).wait()
        values = dot(xs_high[...], spread) + dot(xs_low[...], spread)
        wide = lambda ref: jnp.concatenate([ref[...]] * (CHUNK // 128), axis=1)
        fresh = wide(dec) * old[t] + values * wide(write)
        new[t] = fresh
        store_state(t).start()
        high, low = split(fresh * wide(read))
        y[...] += dot_nt(high, spread) + dot_nt(low, spread)
        return carry

    lax.fori_loop(0, CHUNKS, chunk_step, 0)

    loads[14].wait()
    loads[15].wait()
    gate = silu(dot(normed, gate_w[...]).astype(BF16).astype(F32))
    pieces = []
    for j in range(HEADS // 2):
        even = y[pl.ds(2 * j, ROWS, stride=HEADS), :]
        odd = y[pl.ds(2 * j + 1, ROWS, stride=HEADS), :]
        gain = jnp.where(low_half, skip[2 * j], skip[2 * j + 1])
        cols = slice(128 * j, 128 * j + 128)
        pieces.append(
            (jnp.where(low_half, even, odd) + gain * conv[:, cols]) * gate[:, cols]
        )
    groups = [jnp.concatenate(pieces[2 * g : 2 * g + 2], axis=1) for g in range(2)]
    inner = jnp.concatenate([rms(g) for g in groups], axis=1) * inner_gain[...]
    loads[16].wait()
    partial[...] = dot(inner.astype(BF16), out_w[...]).astype(BF16)
    for t in range(CHUNKS):
        store_state(t).wait()


def run_mixer(*given):
    vmem = pl.BlockSpec(memory_space=VMEM)
    hbm = pl.BlockSpec(memory_space=pltpu.HBM)
    lanes = lambda: VMEM((256, 128), F32)
    held = [
        (pltpu.SMEM if 5 <= n < 8 else VMEM)(v.shape, v.dtype)
        for n, v in enumerate(given[:17])
    ]
    return pl.pallas_call(
        mixer_kernel,
        out_shape=(
            jax.ShapeDtypeStruct((256, 4096), F32),
            jax.ShapeDtypeStruct((ROWS, 2 * HALF), BF16),
            jax.ShapeDtypeStruct((16, 256), BF16),
        ),
        in_specs=[hbm] * 18,
        out_specs=(hbm, vmem, vmem),
        scratch_shapes=[
            *held,
            VMEM((CHUNKS, 256, CHUNK), F32),
            VMEM((CHUNKS, 256, CHUNK), F32),
            lanes(),
            lanes(),
            lanes(),
            VMEM((256, 128), BF16),
            VMEM((256, 128), BF16),
            lanes(),
            lanes(),
            VMEM((192, 128), F32),
            pltpu.SemaphoreType.DMA((17,)),
            pltpu.SemaphoreType.DMA((2 * CHUNKS,)),
        ],
        compiler_params=pltpu.CompilerParams(vmem_limit_bytes=67043328),
        name="mixer",
    )(*given)


def ffn_kernel(
    partial,
    meta,
    stream_hbm,
    gain_hbm,
    mix_hbm,
    eg_hbm,
    eu_hbm,
    ed_hbm,
    dg_hbm,
    du_hbm,
    dd_hbm,
    out,
    x0,
    x1,
    x2,
    y0,
    y1,
    y2,
    s0,
    s1,
    s2,
    *rest,
):
    landed, rest = rest[:12], rest[12:]
    landing = [landed[3 * k : 3 * k + 3] for k in range(4)]
    (
    other_partial,
    wide,
    mid,
    eg,
    eu,
    ed,
    ed_other,
    dgu,
    dgu_other,
    dd,
    dd_scaled,
    packed,
    slot_weight,
    act,
    act_other,
    left_side,
    result,
    local_sem,
    ag_send,
    ag_recv,
    dd_send,
    dd_recv,
    rs_send,
    rs_recv,
    mi_send,
    mi_recv,
    stream,
    gain,
    mix,
    small_sem,
    ) = rest
    ep = lax.axis_index("ep")
    core = lax.axis_index("tp")
    coords = (ep // 16, (ep // 4) % 4, ep % 4)
    other = 1 - core
    own_cols = pl.multiple_of(core * HALF, HALF)
    other_cols = pl.multiple_of(other * HALF, HALF)
    expert = ep // 8
    mine = (x0, x1, x2)
    theirs = (y0, y1, y2)
    sums = (s0, s1, s2)

    def neighbour(dim, shift):
        moved = list(coords)
        moved[dim] = lax.rem(coords[dim] + shift, 4)
        return (moved[0] * 16 + moved[1] * 4 + moved[2], core)

    partner = (ep, other)

    small = [
        pltpu.make_async_copy(stream_hbm, stream, small_sem.at[0]),
        pltpu.make_async_copy(gain_hbm, gain, small_sem.at[1]),
        pltpu.make_async_copy(mix_hbm, mix, small_sem.at[2]),
    ]
    for load in small:
        load.start()
    barrier = pltpu.get_barrier_semaphore()
    for dim in range(3):
        for shift in (1, 2, 3):
            pl.semaphore_signal(
                barrier, inc=1, device_id=neighbour(dim, shift), device_id_type=MESH
            )
    pl.semaphore_signal(barrier, inc=1, device_id=partner, device_id_type=MESH)
    pl.semaphore_wait(barrier, 10)

    def to_partner(src, dst, n):
        return pltpu.make_async_remote_copy(
            src_ref=src,
            dst_ref=dst,
            send_sem=mi_send.at[n],
            recv_sem=mi_recv.at[n],
            device_id=partner,
            device_id_type=MESH,
        )

    swap_partial = to_partner(partial, other_partial, 0)
    swap_partial.start()
    loads = [
        pltpu.make_async_copy(eg_hbm, eg.at[pl.ds(0, HIDDEN)], local_sem.at[0]),
        pltpu.make_async_copy(eu_hbm, eu.at[pl.ds(0, HIDDEN)], local_sem.at[1]),
        pltpu.make_async_copy(
            ed_hbm.at[:, pl.ds(own_cols, HALF)], ed.at[pl.ds(0, HIDDEN)], local_sem.at[2]
        ),
        pltpu.make_async_copy(dg_hbm, dgu.at[pl.ds(0, DENSE)], local_sem.at[3]),
        pltpu.make_async_copy(du_hbm, dgu.at[pl.ds(128, DENSE)], local_sem.at[4]),
        pltpu.make_async_copy(dd_hbm, dd, local_sem.at[5]),
    ]
    for load in loads:
        load.start()

    for load in small:
        load.wait()
    swap_partial.wait()
    mixed = partial[...].astype(F32) + other_partial[...].astype(F32)
    hidden = stream[...].astype(F32) + mixed
    mid[...] = hidden
    wide[...] = (rms(hidden) * gain[...]).astype(BF16)
    here = coords
    for p in range(3):
        cols = pl.ds(pl.multiple_of(own_cols + STARTS[p], 128), WIDTHS[p])
        mine[p][here[0], here[1], here[2], 0:ROWS, :] = wide[:, cols]
    x2[here[0], here[1], here[2], ROWS : ROWS + 16, :] = meta[...]

    def cut(buf, p, where, half=None, rows=None):
        index = [None, None, None]
        for q in range(3):
            index[ORDERS[p][q]] = pl.ds(0, 4) if where[q] is None else where[q]
        if half is not None:
            free = sorted(ORDERS[p][q] for q in range(3) if where[q] is None)
            if free:
                index[free[0]] = pl.ds(2 * half, 2)
            else:
                rows = pl.ds(0, 16) if half == 0 else pl.ds(16, rows - 16)
        elif rows is not None:
            rows = pl.ds(0, rows)
        if rows is not None and not (half is not None and free):
            index.append(rows)
        return buf.at[tuple(index)]

    def turn(p, k, shift):
        return lax.rem(coords[ORDERS[p][k]] + shift, 4)

    ME, RIGHT, FAR, LEFT = 0, 1, 2, 3
    spots = [[[turn(p, k, shift) for shift in range(4)] for k in range(3)] for p in range(3)]

    class Ring:
        def __init__(self, p, k, at, place, direct=False):
            self.p, self.k, self.place, self.direct = p, k, place, direct
            self.copies = [self.copy(at, ME, None, 1), self.copy(at + 1, ME, None, 3)]
            if direct:
                self.copies.append(self.copy(at + 2, ME, None, 2))
            else:
                self.copies.append(self.copy(at + 2, LEFT, 0, 1))
                self.copies.append(self.copy(at + 3, RIGHT, 1, 3))

        def copy(self, at, shift, half, to):
            p = self.p
            where = list(self.place)
            where[self.k] = spots[p][self.k][shift]
            rows = BLOCK_ROWS[p] if half is not None else None
            ref = cut(mine[p], p, where, half, rows)
            return pltpu.make_async_remote_copy(
                src_ref=ref,
                dst_ref=ref,
                send_sem=ag_send.at[at],
                recv_sem=ag_recv.at[at],
                device_id=neighbour(ORDERS[p][self.k], to),
                device_id_type=MESH,
            )

        def start(self):
            if self.direct:
                self.copies[2].start()
            self.copies[0].start()
            self.copies[1].start()

        def on(self):
            self.copies[0].wait_recv()
            if not self.direct:
                self.copies[2].start()
            self.copies[1].wait_recv()
            if not self.direct:
                self.copies[3].start()

        def end(self):
            for copy in self.copies[2:]:
                copy.wait_recv()

    first, second, blocks, lines = [], [], [], []
    for p in range(3):
        at = 48 * p
        own = [spots[p][k][ME] for k in range(3)]
        first.append(Ring(p, 0, at, own, True))
        second.append(
            [
                Ring(p, 1, at + 4 + 4 * u, [spots[p][0][u], None, own[2]], u != ME)
                for u in range(4)
            ]
        )
        blocks.append(
            [Ring(p, 2, at + 20 + 4 * u, [spots[p][0][u], own[1], None]) for u in range(4)]
        )
        lines.append(
            [Ring(p, 2, at + 36 + 4 * (u - 1), [None, spots[p][1][u], None]) for u in (1, 2, 3)]
        )
    rings = [first] + second + blocks + lines
    hand_overs = []

    def hand_over(p, n, second_at, third_at):
        where = [None, second_at, third_at]
        copy = pltpu.make_async_remote_copy(
            src_ref=cut(mine[p], p, where, None, ROWS),
            dst_ref=cut(theirs[p], p, where, None, ROWS),
            send_sem=dd_send.at[13 * p + n],
            recv_sem=dd_recv.at[13 * p + n],
            device_id=partner,
            device_id_type=MESH,
        )
        copy.start()
        hand_overs.append(copy)

    parts = range(3)
    for p in parts:
        first[p].start()
    for p in parts:
        second[p][ME].start()
    for p in parts:
        blocks[p][ME].start()

    early = [
        to_partner(
            ed_hbm.at[:, pl.ds(other_cols, HALF)], ed_other.at[pl.ds(0, HIDDEN)], 1
        ),
        to_partner(dg_hbm, dgu_other.at[pl.ds(0, DENSE)], 2),
        to_partner(du_hbm, dgu_other.at[pl.ds(128, DENSE)], 3),
    ]
    for copy in early:
        copy.start()

    for p in parts:
        first[p].on()
        for u in (LEFT, RIGHT):
            second[p][u].start()
            blocks[p][u].start()
    for p in parts:
        second[p][ME].on()
    for p in parts:
        blocks[p][ME].on()
    for p in parts:
        first[p].end()
        second[p][FAR].start()
        blocks[p][FAR].start()
    for p in parts:
        second[p][LEFT].on()
        second[p][RIGHT].on()
    for p in parts:
        blocks[p][LEFT].on()
        blocks[p][RIGHT].on()
    for p in parts:
        second[p][FAR].on()
        lines[p][RIGHT - 1].start()
        lines[p][LEFT - 1].start()
    for ref in (eg, eu, ed, ed_other):
        ref[HIDDEN:HPAD, :] = jnp.zeros((HPAD - HIDDEN, ref.shape[1]), BF16)
    for ref in (dgu, dgu_other):
        ref[DENSE:128, :] = jnp.zeros((128 - DENSE, HALF), BF16)
        ref[128 + DENSE : 256, :] = jnp.zeros((128 - DENSE, HALF), BF16)
    dd_scaled[DENSE:128, :] = jnp.zeros((128 - DENSE, HALF), BF16)
    for g in range(GROUPS):
        result[g, SLOTS:128, :] = jnp.zeros((128 - SLOTS, HALF), BF16)
    for p in parts:
        for u in range(4):
            second[p][u].end()
        lines[p][FAR - 1].start()
        hand_over(p, 0, None, spots[p][2][ME])
    for p in parts:
        blocks[p][FAR].on()
        hand_over(p, 1, spots[p][1][ME], spots[p][2][LEFT])
        hand_over(p, 2, spots[p][1][ME], spots[p][2][RIGHT])
    for n, u in ((3, RIGHT), (6, LEFT), (9, FAR)):
        for p in parts:
            lines[p][u - 1].on()
            hand_over(p, n, spots[p][1][u], spots[p][2][LEFT])
            hand_over(p, n + 1, spots[p][1][u], spots[p][2][RIGHT])
        for p in parts:
            if u == RIGHT:
                for v in range(4):
                    blocks[p][v].end()
                hand_over(p, n + 2, spots[p][1][ME], spots[p][2][FAR])
            else:
                done = RIGHT if u == LEFT else LEFT
                lines[p][done - 1].end()
                hand_over(p, n + 2, spots[p][1][done], spots[p][2][FAR])
    for p in parts:
        lines[p][FAR - 1].end()
        hand_over(p, 12, spots[p][1][FAR], spots[p][2][FAR])
    for load in loads:
        load.wait()
    for copy in early:
        copy.wait()
    for group in rings:
        for ring in group:
            for copy in ring.copies:
                copy.wait_send()
    for copy in hand_overs:
        copy.wait()

    pick_row = lax.broadcasted_iota(jnp.int32, (128, 128), 0)
    pick_rank = (pick_row == expert).astype(F32).astype(BF16)
    pick_weight = (
        jnp.logical_or(pick_row == expert + 8, pick_row == expert + 16)
    ).astype(F32).astype(BF16)
    lane = lax.broadcasted_iota(jnp.int32, (GROUP_ROWS, 128), 1)
    source = lax.broadcasted_iota(jnp.int32, (GROUP_ROWS, 128), 0) // ROWS

    def group_of(bufs, g):
        z, y = g // 2, 2 * lax.rem(g, 2)
        return jnp.concatenate(
            [
                bufs[p][z, pl.ds(y, 2), :, 0:ROWS, :].reshape(GROUP_ROWS, WIDTHS[p])
                for p in range(3)
            ],
            axis=1,
        )

    def pack_group(g, carry):
        z, y = g // 2, 2 * lax.rem(g, 2)
        tags = x2[z, pl.ds(y, 2), :, ROWS : ROWS + 16, :].reshape(8, 16, 256)
        tags = jnp.concatenate([tags[:, :, 0:128], tags[:, :, 128:256]], axis=1)
        tags = tags.reshape(GROUP_ROWS, 128)
        rank = dot(tags, pick_rank).astype(jnp.int32)
        hit = jnp.logical_and(rank > 0, rank + (CAP * source - 1) == lane)
        table = hit.astype(F32).astype(BF16)
        left_side[g, :, 0:128] = table
        used = table[:, 0:SLOTS]
        slots = pl.ds(pl.multiple_of(g * SLOTS, SLOTS), SLOTS)
        packed[slots, pl.ds(own_cols, HALF)] = dot_tn(used, group_of(mine, g)).astype(BF16)
        packed[slots, pl.ds(other_cols, HALF)] = dot_tn(used, group_of(theirs, g)).astype(
            BF16
        )
        slot_tags = dot_tn(used, tags).astype(BF16)
        slot_weight[slots, :] = dot(slot_tags, pick_weight)
        return carry

    lax.fori_loop(0, GROUPS, pack_group, 0, unroll=2)

    sends = []
    for i in range(2):
        rows = pl.ds(i * 384, 384)
        taken = packed[rows, :]
        gate = dot_nt(taken, eg[...])
        up = dot_nt(taken, eu[...])
        act[rows, :] = (silu(gate) * up * slot_weight[rows, 0:1]).astype(BF16)
        copy = to_partner(act.at[rows], act_other.at[rows], 4 + i)
        copy.start()
        sends.append(copy)

    def dense_group(g, carry):
        both = dot_nt(group_of(mine, g), dgu[...]) + dot_nt(group_of(theirs, g), dgu_other[...])
        left_side[g, :, 128:256] = (silu(both[:, 0:128]) * both[:, 128:256]).astype(BF16)
        return carry

    lax.fori_loop(0, GROUPS, dense_group, 0, unroll=2)
    share = 1.0 / (1.0 + jnp.exp(-mix[...]))
    dd_scaled[0:DENSE, :] = (dd[...].astype(F32) * share).astype(BF16)

    class Back:
        def __init__(self, p, k, at, place, slot):
            self.p, self.k, self.place, self.slot = p, k, place, slot
            self.halves, self.wholes = landing[0][p], landing[1][p]
            self.copies = [
                self.copy(at, FAR, 0, 1, self.halves.at[slot, 0]),
                self.copy(at + 1, FAR, 1, 3, self.halves.at[slot, 1]),
                self.copy(at + 2, RIGHT, None, 1, self.wholes.at[slot, 0]),
                self.copy(at + 3, LEFT, None, 3, self.wholes.at[slot, 1]),
            ]

        def spot(self, shift):
            where = list(self.place)
            where[self.k] = spots[self.p][self.k][shift]
            return where

        def copy(self, at, shift, half, to, target):
            p = self.p
            rows = ROWS if half is not None else None
            return pltpu.make_async_remote_copy(
                src_ref=cut(sums[p], p, self.spot(shift), half, rows),
                dst_ref=target,
                send_sem=rs_send.at[at],
                recv_sem=rs_recv.at[at],
                device_id=neighbour(ORDERS[p][self.k], to),
                device_id_type=MESH,
            )

        def start(self):
            self.copies[0].start()
            self.copies[1].start()

        def add_half(self, shift, half):
            p, got = self.p, self.halves
            where = self.spot(shift)
            place = [None, None, None]
            for q in range(3):
                place[ORDERS[p][q]] = where[q]
            free = [d for d in range(3) if place[d] is None]
            for t in range(2):
                place[free[0]] = 2 * half + t
                ref = sums[p].at[tuple(place)]
                ref[...] = ref[...] + got[self.slot, half, t]

        def on(self):
            self.copies[0].wait_recv()
            self.add_half(RIGHT, 0)
            self.copies[2].start()
            self.copies[1].wait_recv()
            self.add_half(LEFT, 1)
            self.copies[3].start()

        def end(self):
            p, got = self.p, self.wholes
            self.copies[2].wait_recv()
            self.copies[3].wait_recv()
            where = self.spot(ME)
            place = [None, None, None]
            for q in range(3):
                place[ORDERS[p][q]] = where[q]
            free = [d for d in range(3) if place[d] is None]
            for t in range(4):
                place[free[0]] = t
                ref = sums[p].at[tuple(place)]
                total = ref[...].astype(F32) + got[self.slot, 0, t].astype(F32)
                ref[...] = (total + got[self.slot, 1, t].astype(F32)).astype(BF16)

    class Straight:
        def __init__(self, p, k, at, place):
            self.p, self.k, self.place, self.wholes = p, k, place, landing[2 + k][p]
            self.copies = [self.copy(at + u - 1, u) for u in (RIGHT, FAR, LEFT)]

        def copy(self, at, u):
            p = self.p
            where = list(self.place)
            where[self.k] = spots[p][self.k][u]
            return pltpu.make_async_remote_copy(
                src_ref=cut(sums[p], p, where),
                dst_ref=self.wholes.at[u - 1],
                send_sem=rs_send.at[at],
                recv_sem=rs_recv.at[at],
                device_id=neighbour(ORDERS[p][self.k], u),
                device_id_type=MESH,
            )

        def send(self, u):
            self.copies[u - 1].start()

        def arrive(self):
            for copy in self.copies:
                copy.wait_recv()

        def add(self, first_at):
            p, got = self.p, self.wholes
            place = [None, None, None]
            for q in range(3):
                place[ORDERS[p][q]] = spots[p][q][ME]
            place[ORDERS[p][0]] = first_at
            ref = sums[p].at[tuple(place)]
            total = ref[...].astype(F32)
            for n in range(3):
                total = total + got[n, first_at].astype(F32)
            ref[...] = total.astype(BF16)

    third, middle, last = [], [], []
    for p in parts:
        at = 24 * p
        own = [spots[p][k][ME] for k in range(3)]
        third.append(
            [Back(p, 2, at + 4 * u, [None, spots[p][1][u], None], u) for u in range(4)]
        )
        middle.append(Straight(p, 1, at + 16, [None, None, own[2]]))
        last.append(Straight(p, 0, at + 20, own))
    order = (FAR, LEFT, RIGHT, ME)
    for send in sends:
        send.wait()
    for p in parts:
        cols = slice(STARTS[p], STARTS[p] + WIDTHS[p])
        for i in range(2):
            rows = pl.ds(i * 384, 384)
            back = dot(act[rows, :], ed[:, cols]) + dot(act_other[rows, :], ed_other[:, cols])
            result[pl.ds(4 * i, 4), 0:SLOTS, cols] = back.astype(BF16).reshape(
                4, SLOTS, WIDTHS[p]
            )

        def spread_group(g, carry):
            z, y = g // 2, 2 * lax.rem(g, 2)
            right_side = jnp.concatenate([result[g, :, cols], dd_scaled[:, cols]], axis=0)
            total = dot(left_side[g], right_side).astype(BF16)
            sums[p][z, pl.ds(y, 2)] = total.reshape(2, 4, ROWS, WIDTHS[p])
            return carry

        lax.fori_loop(0, GROUPS, spread_group, 0, unroll=2)
        for u in order:
            third[p][u].start()
    for u in order:
        for p in parts:
            third[p][u].on()
    for u in order:
        for p in parts:
            third[p][u].end()
            if u != ME:
                middle[p].send(u)
    for p in parts:
        middle[p].arrive()
        for u in order:
            middle[p].add(spots[p][0][u])
            if u != ME:
                last[p].send(u)
    for p in parts:
        last[p].arrive()
        got = last[p].wholes
        total = mid[:, pl.ds(pl.multiple_of(own_cols + STARTS[p], 128), WIDTHS[p])]
        total = total + sums[p][here[0], here[1], here[2]].astype(F32)
        for n in range(3):
            total = total + got[n].astype(F32)
        out[:, STARTS[p] : STARTS[p] + WIDTHS[p]] = total.astype(BF16)
    for group in third + [middle, last]:
        for back in group:
            for copy in back.copies:
                copy.wait_send()


def run_ffn(partial, meta, stream, gain, mix, eg, eu, ed, dg, du, dd):
    vmem = pl.BlockSpec(memory_space=VMEM)
    hbm = pl.BlockSpec(memory_space=pltpu.HBM)
    blocks = lambda *lead: [VMEM((*lead, WIDTHS[p]), BF16) for p in range(3)]
    sem = pltpu.SemaphoreType.DMA
    return pl.pallas_call(
        ffn_kernel,
        out_shape=jax.ShapeDtypeStruct((ROWS, HALF), BF16),
        in_specs=[vmem] * 2 + [hbm] * 9,
        out_specs=vmem,
        scratch_shapes=[
            *[VMEM((4, 4, 4, BLOCK_ROWS[p], WIDTHS[p]), BF16) for p in range(3)],
            *blocks(4, 4, 4, ROWS),
            *blocks(4, 4, 4, ROWS),
            *blocks(4, 2, 2, ROWS),
            *blocks(4, 2, 4, ROWS),
            *blocks(3, ROWS),
            *blocks(3, 4, ROWS),
            VMEM((ROWS, 2 * HALF), BF16),
            VMEM((ROWS, 2 * HALF), BF16),
            VMEM((ROWS, 2 * HALF), F32),
            VMEM((HPAD, 2 * HALF), BF16),
            VMEM((HPAD, 2 * HALF), BF16),
            VMEM((HPAD, HALF), BF16),
            VMEM((HPAD, HALF), BF16),
            VMEM((256, HALF), BF16),
            VMEM((256, HALF), BF16),
            VMEM((DENSE, HALF), BF16),
            VMEM((128, HALF), BF16),
            VMEM((GROUPS * SLOTS, 2 * HALF), BF16),
            VMEM((GROUPS * SLOTS, 128), F32),
            VMEM((GROUPS * SLOTS, HPAD), BF16),
            VMEM((GROUPS * SLOTS, HPAD), BF16),
            VMEM((GROUPS, GROUP_ROWS, 256), BF16),
            VMEM((GROUPS, 128, HALF), BF16),
            sem((6,)),
            sem((144,)),
            sem((144,)),
            sem((39,)),
            sem((39,)),
            sem((72,)),
            sem((72,)),
            sem((6,)),
            sem((6,)),
            VMEM((ROWS, 2 * HALF), BF16),
            VMEM((1, 2 * HALF), F32),
            VMEM((1, HALF), F32),
            sem((3,)),
        ],
        compiler_params=pltpu.CompilerParams(
            collective_id=0, has_side_effects=True, vmem_limit_bytes=67043328
        ),
        name="ffn",
    )(partial, meta, stream, gain, mix, eg, eu, ed, dg, du, dd)


def local(
    stream,
    mixer_gain,
    gate_proj,
    input_proj,
    state_maps,
    step_proj,
    step_bias,
    decay_rate,
    input_taps,
    map_taps,
    input_past,
    map_past,
    head_state,
    skip_gain,
    inner_gain,
    mixer_out,
    channel_gain,
    expert_ids,
    expert_weight,
    expert_gate,
    expert_up,
    expert_down,
    dense_gate,
    dense_up,
    dense_down,
    dense_mix,
):
    state_out, partial, meta = run_mixer(
        stream,
        mixer_gain.reshape(1, -1),
        step_proj.T,
        expert_ids.T,
        expert_weight.T,
        step_bias,
        decay_rate,
        skip_gain,
        input_proj,
        input_taps,
        jnp.transpose(input_past, (1, 0, 2)),
        state_maps,
        map_taps,
        jnp.transpose(map_past, (0, 2, 1, 3)).reshape(192, 128),
        inner_gain.reshape(1, -1),
        gate_proj,
        mixer_out,
        head_state.reshape(256, 4096),
    )
    out = run_ffn(
        partial,
        meta,
        stream,
        channel_gain.reshape(1, -1),
        dense_mix.reshape(1, -1),
        expert_gate.T,
        expert_up.T,
        expert_down,
        dense_gate.T,
        dense_up.T,
        dense_down,
    )
    return out, state_out.reshape(head_state.shape)


def solution(mesh):
    placed = (
        P("ep", None),
        P(),
        P(None, "tp"),
        P(None, "tp"),
        P(None, None, "tp"),
        P(None, "tp"),
        P("tp"),
        P("tp"),
        P(None, "tp"),
        P(None, None, "tp"),
        P("ep", None, "tp"),
        P("ep", None, None, "tp"),
        P("ep", "tp", None),
        P("tp"),
        P("tp"),
        P("tp", None),
        P(),
        P("ep", None),
        P("ep", None),
        P(None, ("ep", "tp")),
        P(None, ("ep", "tp")),
        P(("ep", "tp"), None),
        P("tp", "ep"),
        P("tp", "ep"),
        P("ep", "tp"),
        P("tp"),
    )
    return jax.shard_map(
        local,
        mesh=mesh,
        in_specs=placed,
        out_specs=(P("ep", "tp"), P("ep", "tp", None)),
        check_vma=False,
    )
```

```python
import functools

import jax
import jax.numpy as jnp
from jax import lax
from jax.experimental import pallas as pl
from jax.experimental.pallas import tpu as pltpu
from jax.sharding import PartitionSpec as P

EPS = 1e-06
MESH = pl.DeviceIdType.MESH
F32 = jnp.float32
BF16 = jnp.bfloat16
VMEM = pltpu.VMEM
ANY = pl.ANY

HEADS = 8
ROWS = 32
EXPERTS = 8
CAP = 12
CHUNKS = 8
CHUNK = 512
GROUPS = 8
GROUP_ROWS = 256
SLOTS = 96
HALF = 1024
HIDDEN = 448
HPAD = 512
DENSE = 88

WIDTHS = (384, 384, 256)
STARTS = (0, 384, 768)
BLOCK_ROWS = (32, 32, 48)
ORDERS = ((2, 1, 0), (1, 0, 2), (0, 2, 1))


def dot(a, b):
    return jnp.dot(a, b, preferred_element_type=F32)


def dot_nt(a, b):
    return lax.dot_general(a, b, (((1,), (1,)), ((), ())), preferred_element_type=F32)


def dot_tn(a, b):
    return lax.dot_general(a, b, (((0,), (0,)), ((), ())), preferred_element_type=F32)


def silu(v):
    return v / (1.0 + jnp.exp(-v))


def rms(v):
    return v * lax.rsqrt(jnp.mean(v * v, axis=-1, keepdims=True) + EPS)


def split(v):
    high = v.astype(BF16)
    return high, (v - high.astype(F32)).astype(BF16)


def mixer_kernel(*refs):
    given, refs = refs[:18], refs[18:]
    state_hbm = given[17]
    state_out, partial, meta = refs[:3]
    held, refs = refs[3:20], refs[20:]
    (
        stream,
        mixer_gain,
        step_t,
        ids,
        weights,
        bias,
        decay,
        skip,
        input_w,
        input_taps,
        input_past,
        maps_w,
        map_taps,
        map_past,
        inner_gain,
        gate_w,
        out_w,
    ) = held
    old, new, dec, write, read, xs_high, xs_low, tmp, y, past, in_sems, sems = refs
    loads = [
        pltpu.make_async_copy(src, dst, in_sems.at[n])
        for n, (src, dst) in enumerate(zip(given, held))
    ]

    def load_state(t):
        cols = pl.ds(pl.multiple_of(t * CHUNK, CHUNK), CHUNK)
        return pltpu.make_async_copy(state_hbm.at[:, cols], old.at[t], sems.at[t])

    def store_state(t):
        cols = pl.ds(pl.multiple_of(t * CHUNK, CHUNK), CHUNK)
        return pltpu.make_async_copy(
            new.at[t], state_out.at[:, cols], sems.at[CHUNKS + t]
        )

    for load in loads[:15]:
        load.start()
    for t in range(CHUNKS):
        load_state(t).start()
    loads[15].start()
    loads[16].start()

    for load in loads[:8]:
        load.wait()
    normed = (rms(stream[...].astype(F32)) * mixer_gain[...]).astype(BF16)
    steps = dot_nt(normed, step_t[...])

    expert_of = lax.broadcasted_iota(jnp.int32, (EXPERTS, ROWS), 0)
    hit0 = (ids[0:1, :] == expert_of).astype(F32)
    hit1 = (ids[1:2, :] == expert_of).astype(F32)
    member = hit0 + hit1
    upper = (
        lax.broadcasted_iota(jnp.int32, (ROWS, ROWS), 0)
        <= lax.broadcasted_iota(jnp.int32, (ROWS, ROWS), 1)
    ).astype(BF16)
    rank = dot(member.astype(BF16), upper) * member
    weight = hit0 * weights[0:1, :] + hit1 * weights[1:2, :]
    w_high = weight.astype(BF16).astype(F32)
    w_low = weight - w_high
    table = jnp.concatenate(
        [rank, w_high, w_low, jnp.zeros((104, ROWS), F32)], axis=0
    ).astype(BF16)
    eye = (
        lax.broadcasted_iota(jnp.int32, (ROWS, ROWS), 0)
        == lax.broadcasted_iota(jnp.int32, (ROWS, ROWS), 1)
    ).astype(BF16)
    by_row = dot_nt(eye, table)
    meta[...] = jnp.concatenate([by_row[0:16], by_row[16:32]], axis=1).astype(BF16)

    for load in loads[8:11]:
        load.wait()
    newest = dot(normed, input_w[...]).astype(BF16).astype(F32)
    conv = newest * input_taps[3:4, :]
    for t in range(3):
        conv = conv + input_past[t].astype(F32) * input_taps[t : t + 1, :]
    conv = silu(conv)

    for load in loads[11:14]:
        load.wait()
    past[...] = map_past[...].astype(F32)
    conv_maps = []
    for m in range(2):
        new_map = dot(normed, maps_w[m]).astype(BF16).astype(F32)
        acc = new_map * map_taps[m, 3:4, :]
        for t in range(3):
            acc = acc + past[pl.ds(2 * t + m, ROWS, stride=6), :] * map_taps[m, t : t + 1, :]
        conv_maps.append(silu(acc))

    lane = lax.broadcasted_iota(jnp.int32, (ROWS, 128), 1)
    low_half = lane < 64

    def both_halves(v):
        turned = pltpu.roll(v, 64, 1)
        return jnp.where(low_half, v, turned), jnp.where(low_half, turned, v)

    write_by_group = both_halves(conv_maps[0])
    read_by_group = both_halves(conv_maps[1])
    for h in range(HEADS):
        rows = pl.ds(h, ROWS, stride=HEADS)
        v = jnp.broadcast_to(steps[:, h : h + 1], (ROWS, 128)) + bias[h]
        step = jnp.maximum(v, 0.0) + jnp.log1p(jnp.exp(-jnp.abs(v)))
        dec[rows, :] = jnp.exp(-decay[h] * step)
        pair = conv[:, 128 * (h // 2) : 128 * (h // 2) + 128]
        mine = low_half if h % 2 == 0 else jnp.logical_not(low_half)
        tmp[rows, :] = jnp.where(mine, step * pair, 0.0)
        write[rows, :] = write_by_group[h // 4]
        read[rows, :] = read_by_group[h // 4]
    high, low = split(tmp[...])
    xs_high[...] = high
    xs_low[...] = low
    y[...] = jnp.zeros_like(y)

    slot = lax.broadcasted_iota(jnp.int32, (128, CHUNK), 0) % 64
    place = lax.broadcasted_iota(jnp.int32, (128, CHUNK), 1) // 64

    def chunk_step(t, carry):
        spread = (slot == place + 8 * t).astype(F32).astype(BF16)
        load_state(t).wait()
        values = dot(xs_high[...], spread) + dot(xs_low[...], spread)
        wide = lambda ref: jnp.concatenate([ref[...]] * (CHUNK // 128), axis=1)
        fresh = wide(dec) * old[t] + values * wide(write)
        new[t] = fresh
        store_state(t).start()
        high, low = split(fresh * wide(read))
        y[...] += dot_nt(high, spread) + dot_nt(low, spread)
        return carry

    lax.fori_loop(0, CHUNKS, chunk_step, 0)

    loads[14].wait()
    loads[15].wait()
    gate = silu(dot(normed, gate_w[...]).astype(BF16).astype(F32))
    pieces = []
    for j in range(HEADS // 2):
        even = y[pl.ds(2 * j, ROWS, stride=HEADS), :]
        odd = y[pl.ds(2 * j + 1, ROWS, stride=HEADS), :]
        gain = jnp.where(low_half, skip[2 * j], skip[2 * j + 1])
        cols = slice(128 * j, 128 * j + 128)
        pieces.append(
            (jnp.where(low_half, even, odd) + gain * conv[:, cols]) * gate[:, cols]
        )
    groups = [jnp.concatenate(pieces[2 * g : 2 * g + 2], axis=1) for g in range(2)]
    inner = jnp.concatenate([rms(g) for g in groups], axis=1) * inner_gain[...]
    loads[16].wait()
    partial[...] = dot(inner.astype(BF16), out_w[...]).astype(BF16)
    for t in range(CHUNKS):
        store_state(t).wait()


def run_mixer(*given):
    vmem = pl.BlockSpec(memory_space=VMEM)
    hbm = pl.BlockSpec(memory_space=pltpu.HBM)
    lanes = lambda: VMEM((256, 128), F32)
    held = [
        (pltpu.SMEM if 5 <= n < 8 else VMEM)(v.shape, v.dtype)
        for n, v in enumerate(given[:17])
    ]
    return pl.pallas_call(
        mixer_kernel,
        out_shape=(
            jax.ShapeDtypeStruct((256, 4096), F32),
            jax.ShapeDtypeStruct((ROWS, 2 * HALF), BF16),
            jax.ShapeDtypeStruct((16, 256), BF16),
        ),
        in_specs=[hbm] * 18,
        out_specs=(hbm, vmem, vmem),
        scratch_shapes=[
            *held,
            VMEM((CHUNKS, 256, CHUNK), F32),
            VMEM((CHUNKS, 256, CHUNK), F32),
            lanes(),
            lanes(),
            lanes(),
            VMEM((256, 128), BF16),
            VMEM((256, 128), BF16),
            lanes(),
            lanes(),
            VMEM((192, 128), F32),
            pltpu.SemaphoreType.DMA((17,)),
            pltpu.SemaphoreType.DMA((2 * CHUNKS,)),
        ],
        compiler_params=pltpu.CompilerParams(vmem_limit_bytes=67043328),
        name="mixer",
    )(*given)


def ffn_kernel(
    partial,
    meta,
    stream_hbm,
    gain_hbm,
    mix_hbm,
    eg_hbm,
    eu_hbm,
    ed_hbm,
    dg_hbm,
    du_hbm,
    dd_hbm,
    out,
    x0,
    x1,
    x2,
    y0,
    y1,
    y2,
    s0,
    s1,
    s2,
    *rest,
):
    landed, rest = rest[:12], rest[12:]
    landing = [landed[3 * k : 3 * k + 3] for k in range(4)]
    (
    other_partial,
    wide,
    mid,
    eg,
    eu,
    ed,
    ed_other,
    dgu,
    dgu_other,
    dd,
    dd_scaled,
    packed,
    slot_weight,
    act,
    act_other,
    left_side,
    result,
    local_sem,
    ag_send,
    ag_recv,
    dd_send,
    dd_recv,
    rs_send,
    rs_recv,
    mi_send,
    mi_recv,
    stream,
    gain,
    mix,
    small_sem,
    ) = rest
    ep = lax.axis_index("ep")
    core = lax.axis_index("tp")
    coords = (ep // 16, (ep // 4) % 4, ep % 4)
    other = 1 - core
    own_cols = pl.multiple_of(core * HALF, HALF)
    other_cols = pl.multiple_of(other * HALF, HALF)
    expert = ep // 8
    mine = (x0, x1, x2)
    theirs = (y0, y1, y2)
    sums = (s0, s1, s2)

    def neighbour(dim, shift):
        moved = list(coords)
        moved[dim] = lax.rem(coords[dim] + shift, 4)
        return (moved[0] * 16 + moved[1] * 4 + moved[2], core)

    partner = (ep, other)

    small = [
        pltpu.make_async_copy(stream_hbm, stream, small_sem.at[0]),
        pltpu.make_async_copy(gain_hbm, gain, small_sem.at[1]),
        pltpu.make_async_copy(mix_hbm, mix, small_sem.at[2]),
    ]
    for load in small:
        load.start()
    barrier = pltpu.get_barrier_semaphore()
    for dim in range(3):
        for shift in (1, 2, 3):
            pl.semaphore_signal(
                barrier, inc=1, device_id=neighbour(dim, shift), device_id_type=MESH
            )
    pl.semaphore_signal(barrier, inc=1, device_id=partner, device_id_type=MESH)
    pl.semaphore_wait(barrier, 10)

    def to_partner(src, dst, n):
        return pltpu.make_async_remote_copy(
            src_ref=src,
            dst_ref=dst,
            send_sem=mi_send.at[n],
            recv_sem=mi_recv.at[n],
            device_id=partner,
            device_id_type=MESH,
        )

    swap_partial = to_partner(partial, other_partial, 0)
    swap_partial.start()
    loads = [
        pltpu.make_async_copy(eg_hbm, eg.at[pl.ds(0, HIDDEN)], local_sem.at[0]),
        pltpu.make_async_copy(eu_hbm, eu.at[pl.ds(0, HIDDEN)], local_sem.at[1]),
        pltpu.make_async_copy(
            ed_hbm.at[:, pl.ds(own_cols, HALF)], ed.at[pl.ds(0, HIDDEN)], local_sem.at[2]
        ),
        pltpu.make_async_copy(dg_hbm, dgu.at[pl.ds(0, DENSE)], local_sem.at[3]),
        pltpu.make_async_copy(du_hbm, dgu.at[pl.ds(128, DENSE)], local_sem.at[4]),
        pltpu.make_async_copy(dd_hbm, dd, local_sem.at[5]),
    ]
    for load in loads:
        load.start()

    for load in small:
        load.wait()
    swap_partial.wait()
    mixed = partial[...].astype(F32) + other_partial[...].astype(F32)
    hidden = stream[...].astype(F32) + mixed
    mid[...] = hidden
    wide[...] = (rms(hidden) * gain[...]).astype(BF16)
    here = coords
    for p in range(3):
        cols = pl.ds(pl.multiple_of(own_cols + STARTS[p], 128), WIDTHS[p])
        mine[p][here[0], here[1], here[2], 0:ROWS, :] = wide[:, cols]
    x2[here[0], here[1], here[2], ROWS : ROWS + 16, :] = meta[...]

    def cut(buf, p, where, half=None, rows=None):
        index = [None, None, None]
        for q in range(3):
            index[ORDERS[p][q]] = pl.ds(0, 4) if where[q] is None else where[q]
        if half is not None:
            free = sorted(ORDERS[p][q] for q in range(3) if where[q] is None)
            if free:
                index[free[0]] = pl.ds(2 * half, 2)
            else:
                rows = pl.ds(0, 16) if half == 0 else pl.ds(16, rows - 16)
        elif rows is not None:
            rows = pl.ds(0, rows)
        if rows is not None and not (half is not None and free):
            index.append(rows)
        return buf.at[tuple(index)]

    def turn(p, k, shift):
        return lax.rem(coords[ORDERS[p][k]] + shift, 4)

    ME, RIGHT, FAR, LEFT = 0, 1, 2, 3
    spots = [[[turn(p, k, shift) for shift in range(4)] for k in range(3)] for p in range(3)]

    class Ring:
        def __init__(self, p, k, at, place, direct=False):
            self.p, self.k, self.place, self.direct = p, k, place, direct
            self.copies = [self.copy(at, ME, None, 1), self.copy(at + 1, ME, None, 3)]
            if direct:
                self.copies.append(self.copy(at + 2, ME, None, 2))
            else:
                self.copies.append(self.copy(at + 2, LEFT, 0, 1))
                self.copies.append(self.copy(at + 3, RIGHT, 1, 3))

        def copy(self, at, shift, half, to):
            p = self.p
            where = list(self.place)
            where[self.k] = spots[p][self.k][shift]
            rows = BLOCK_ROWS[p] if half is not None else None
            ref = cut(mine[p], p, where, half, rows)
            return pltpu.make_async_remote_copy(
                src_ref=ref,
                dst_ref=ref,
                send_sem=ag_send.at[at],
                recv_sem=ag_recv.at[at],
                device_id=neighbour(ORDERS[p][self.k], to),
                device_id_type=MESH,
            )

        def start(self):
            if self.direct:
                self.copies[2].start()
            self.copies[0].start()
            self.copies[1].start()

        def on(self):
            self.copies[0].wait_recv()
            if not self.direct:
                self.copies[2].start()
            self.copies[1].wait_recv()
            if not self.direct:
                self.copies[3].start()

        def end(self):
            for copy in self.copies[2:]:
                copy.wait_recv()

    first, second, third_way = [], [], []
    for p in range(3):
        at = 84 * p
        own = [spots[p][k][ME] for k in range(3)]
        first.append(Ring(p, 0, at, own, True))
        second.append(
            [Ring(p, 1, at + 4 + 4 * u, [spots[p][0][u], None, own[2]], True) for u in range(4)]
        )
        third_way.append(
            [
                [
                    Ring(p, 2, at + 20 + 16 * u + 4 * v, [spots[p][0][u], spots[p][1][v], None])
                    for v in range(4)
                ]
                for u in range(4)
            ]
        )
    rings = [first] + second + [row for part in third_way for row in part]
    hand_overs = []

    def hand_over(p, n, second_at, third_at):
        where = [None, second_at, third_at]
        copy = pltpu.make_async_remote_copy(
            src_ref=cut(mine[p], p, where, None, ROWS),
            dst_ref=cut(theirs[p], p, where, None, ROWS),
            send_sem=dd_send.at[13 * p + n],
            recv_sem=dd_recv.at[13 * p + n],
            device_id=partner,
            device_id_type=MESH,
        )
        copy.start()
        hand_overs.append(copy)

    parts = range(3)
    def launch(*pairs):
        for p in parts:
            for u, v in pairs:
                third_way[p][u][v].start()

    def pass_on(*pairs):
        for p in parts:
            for u, v in pairs:
                third_way[p][u][v].on()

    for p in parts:
        first[p].start()
    for p in parts:
        second[p][ME].start()
    launch((ME, ME))

    early = [
        to_partner(
            ed_hbm.at[:, pl.ds(other_cols, HALF)], ed_other.at[pl.ds(0, HIDDEN)], 1
        ),
        to_partner(dg_hbm, dgu_other.at[pl.ds(0, DENSE)], 2),
        to_partner(du_hbm, dgu_other.at[pl.ds(128, DENSE)], 3),
    ]
    for copy in early:
        copy.start()

    for p in parts:
        first[p].on()
        for u in (LEFT, RIGHT):
            second[p][u].start()
            third_way[p][u][ME].start()
    for p in parts:
        second[p][ME].on()
    launch((ME, RIGHT), (ME, LEFT))
    for p in parts:
        first[p].end()
        second[p][FAR].start()
        third_way[p][FAR][ME].start()
    for p in parts:
        second[p][ME].end()
    launch((ME, FAR))
    pass_on((ME, ME))
    for ref in (eg, eu, ed, ed_other):
        ref[HIDDEN:HPAD, :] = jnp.zeros((HPAD - HIDDEN, ref.shape[1]), BF16)
    for ref in (dgu, dgu_other):
        ref[DENSE:128, :] = jnp.zeros((128 - DENSE, HALF), BF16)
        ref[128 + DENSE : 256, :] = jnp.zeros((128 - DENSE, HALF), BF16)
    dd_scaled[DENSE:128, :] = jnp.zeros((128 - DENSE, HALF), BF16)
    for g in range(GROUPS):
        result[g, SLOTS:128, :] = jnp.zeros((128 - SLOTS, HALF), BF16)
    for p in parts:
        second[p][LEFT].on()
        second[p][RIGHT].on()
    launch((LEFT, RIGHT), (RIGHT, RIGHT), (LEFT, LEFT), (RIGHT, LEFT))
    pass_on((LEFT, ME), (RIGHT, ME), (ME, RIGHT), (ME, LEFT))
    for p in parts:
        second[p][LEFT].end()
        second[p][RIGHT].end()
    launch((LEFT, FAR), (RIGHT, FAR))
    for p in parts:
        second[p][FAR].on()
    launch((FAR, RIGHT), (FAR, LEFT))
    for p in parts:
        second[p][FAR].end()
    launch((FAR, FAR))
    pass_on((FAR, ME), (ME, FAR))
    for p in parts:
        hand_over(p, 0, None, spots[p][2][ME])
        hand_over(p, 1, spots[p][1][ME], spots[p][2][LEFT])
        hand_over(p, 2, spots[p][1][ME], spots[p][2][RIGHT])

    def finish(v, n):
        for p in parts:
            for u in range(4):
                third_way[p][u][v].end()
            hand_over(p, n, spots[p][1][v], spots[p][2][FAR])

    def sides(v, n):
        for p in parts:
            hand_over(p, n, spots[p][1][v], spots[p][2][LEFT])
            hand_over(p, n + 1, spots[p][1][v], spots[p][2][RIGHT])

    pass_on((LEFT, RIGHT), (RIGHT, RIGHT), (LEFT, LEFT), (RIGHT, LEFT))
    finish(ME, 3)
    pass_on((LEFT, FAR), (RIGHT, FAR), (FAR, RIGHT), (FAR, LEFT))
    sides(RIGHT, 4)
    sides(LEFT, 6)
    pass_on((FAR, FAR))
    sides(FAR, 8)
    finish(RIGHT, 10)
    finish(LEFT, 11)
    finish(FAR, 12)
    for load in loads:
        load.wait()
    for copy in early:
        copy.wait()
    for group in rings:
        for ring in group:
            for copy in ring.copies:
                copy.wait_send()
    for copy in hand_overs:
        copy.wait()

    pick_row = lax.broadcasted_iota(jnp.int32, (128, 128), 0)
    pick_rank = (pick_row == expert).astype(F32).astype(BF16)
    pick_weight = (
        jnp.logical_or(pick_row == expert + 8, pick_row == expert + 16)
    ).astype(F32).astype(BF16)
    lane = lax.broadcasted_iota(jnp.int32, (GROUP_ROWS, 128), 1)
    source = lax.broadcasted_iota(jnp.int32, (GROUP_ROWS, 128), 0) // ROWS

    def group_of(bufs, g):
        z, y = g // 2, 2 * lax.rem(g, 2)
        return jnp.concatenate(
            [
                bufs[p][z, pl.ds(y, 2), :, 0:ROWS, :].reshape(GROUP_ROWS, WIDTHS[p])
                for p in range(3)
            ],
            axis=1,
        )

    def pack_group(g, carry):
        z, y = g // 2, 2 * lax.rem(g, 2)
        tags = x2[z, pl.ds(y, 2), :, ROWS : ROWS + 16, :].reshape(8, 16, 256)
        tags = jnp.concatenate([tags[:, :, 0:128], tags[:, :, 128:256]], axis=1)
        tags = tags.reshape(GROUP_ROWS, 128)
        rank = dot(tags, pick_rank).astype(jnp.int32)
        hit = jnp.logical_and(rank > 0, rank + (CAP * source - 1) == lane)
        table = hit.astype(F32).astype(BF16)
        left_side[g, :, 0:128] = table
        used = table[:, 0:SLOTS]
        slots = pl.ds(pl.multiple_of(g * SLOTS, SLOTS), SLOTS)
        packed[slots, pl.ds(own_cols, HALF)] = dot_tn(used, group_of(mine, g)).astype(BF16)
        packed[slots, pl.ds(other_cols, HALF)] = dot_tn(used, group_of(theirs, g)).astype(
            BF16
        )
        slot_tags = dot_tn(used, tags).astype(BF16)
        slot_weight[slots, :] = dot(slot_tags, pick_weight)
        return carry

    lax.fori_loop(0, GROUPS, pack_group, 0, unroll=2)

    sends = []
    for i in range(2):
        units = pl.ds(256 * i, 256)
        gate = dot_nt(packed[...], eg[units, :])
        up = dot_nt(packed[...], eu[units, :])
        act[:, units] = (silu(gate) * up * slot_weight[:, 0:1]).astype(BF16)
        copy = to_partner(act.at[:, units], act_other.at[:, units], 4 + i)
        copy.start()
        sends.append(copy)

    def dense_group(g, carry):
        both = dot_nt(group_of(mine, g), dgu[...]) + dot_nt(group_of(theirs, g), dgu_other[...])
        left_side[g, :, 128:256] = (silu(both[:, 0:128]) * both[:, 128:256]).astype(BF16)
        return carry

    lax.fori_loop(0, GROUPS, dense_group, 0, unroll=2)
    share = 1.0 / (1.0 + jnp.exp(-mix[...]))
    dd_scaled[0:DENSE, :] = (dd[...].astype(F32) * share).astype(BF16)

    class Back:
        def __init__(self, p, k, at, place, slot):
            self.p, self.k, self.place, self.slot = p, k, place, slot
            self.halves, self.wholes = landing[0][p], landing[1][p]
            self.copies = [
                self.copy(at, FAR, 0, 1, self.halves.at[slot, 0]),
                self.copy(at + 1, FAR, 1, 3, self.halves.at[slot, 1]),
                self.copy(at + 2, RIGHT, None, 1, self.wholes.at[slot, 0]),
                self.copy(at + 3, LEFT, None, 3, self.wholes.at[slot, 1]),
            ]

        def spot(self, shift):
            where = list(self.place)
            where[self.k] = spots[self.p][self.k][shift]
            return where

        def copy(self, at, shift, half, to, target):
            p = self.p
            rows = ROWS if half is not None else None
            return pltpu.make_async_remote_copy(
                src_ref=cut(sums[p], p, self.spot(shift), half, rows),
                dst_ref=target,
                send_sem=rs_send.at[at],
                recv_sem=rs_recv.at[at],
                device_id=neighbour(ORDERS[p][self.k], to),
                device_id_type=MESH,
            )

        def start(self):
            self.copies[0].start()
            self.copies[1].start()

        def add_half(self, shift, half):
            p, got = self.p, self.halves
            where = self.spot(shift)
            place = [None, None, None]
            for q in range(3):
                place[ORDERS[p][q]] = where[q]
            free = [d for d in range(3) if place[d] is None]
            for t in range(2):
                place[free[0]] = 2 * half + t
                ref = sums[p].at[tuple(place)]
                ref[...] = ref[...] + got[self.slot, half, t]

        def on(self):
            self.copies[0].wait_recv()
            self.add_half(RIGHT, 0)
            self.copies[2].start()
            self.copies[1].wait_recv()
            self.add_half(LEFT, 1)
            self.copies[3].start()

        def end(self):
            p, got = self.p, self.wholes
            self.copies[2].wait_recv()
            self.copies[3].wait_recv()
            where = self.spot(ME)
            place = [None, None, None]
            for q in range(3):
                place[ORDERS[p][q]] = where[q]
            free = [d for d in range(3) if place[d] is None]
            for t in range(4):
                place[free[0]] = t
                ref = sums[p].at[tuple(place)]
                total = ref[...].astype(F32) + got[self.slot, 0, t].astype(F32)
                ref[...] = (total + got[self.slot, 1, t].astype(F32)).astype(BF16)

    class Straight:
        def __init__(self, p, k, at, place):
            self.p, self.k, self.place, self.wholes = p, k, place, landing[2 + k][p]
            self.copies = [self.copy(at + u - 1, u) for u in (RIGHT, FAR, LEFT)]

        def copy(self, at, u):
            p = self.p
            where = list(self.place)
            where[self.k] = spots[p][self.k][u]
            return pltpu.make_async_remote_copy(
                src_ref=cut(sums[p], p, where),
                dst_ref=self.wholes.at[u - 1],
                send_sem=rs_send.at[at],
                recv_sem=rs_recv.at[at],
                device_id=neighbour(ORDERS[p][self.k], u),
                device_id_type=MESH,
            )

        def send(self, u):
            self.copies[u - 1].start()

        def arrive(self):
            for copy in self.copies:
                copy.wait_recv()

        def add(self, first_at):
            p, got = self.p, self.wholes
            place = [None, None, None]
            for q in range(3):
                place[ORDERS[p][q]] = spots[p][q][ME]
            place[ORDERS[p][0]] = first_at
            ref = sums[p].at[tuple(place)]
            total = ref[...].astype(F32)
            for n in range(3):
                total = total + got[n, first_at].astype(F32)
            ref[...] = total.astype(BF16)

    third, middle, last = [], [], []
    for p in parts:
        at = 24 * p
        own = [spots[p][k][ME] for k in range(3)]
        third.append(
            [Back(p, 2, at + 4 * u, [None, spots[p][1][u], None], u) for u in range(4)]
        )
        middle.append(Straight(p, 1, at + 16, [None, None, own[2]]))
        last.append(Straight(p, 0, at + 20, own))
    order = (FAR, LEFT, RIGHT, ME)
    for send in sends:
        send.wait()
    for p in parts:
        cols = slice(STARTS[p], STARTS[p] + WIDTHS[p])
        back = dot(act[...], ed[:, cols]) + dot(act_other[...], ed_other[:, cols])
        result[:, 0:SLOTS, cols] = back.astype(BF16).reshape(GROUPS, SLOTS, WIDTHS[p])

        def spread_group(g, carry):
            z, y = g // 2, 2 * lax.rem(g, 2)
            right_side = jnp.concatenate([result[g, :, cols], dd_scaled[:, cols]], axis=0)
            total = dot(left_side[g], right_side).astype(BF16)
            sums[p][z, pl.ds(y, 2)] = total.reshape(2, 4, ROWS, WIDTHS[p])
            return carry

        lax.fori_loop(0, GROUPS, spread_group, 0, unroll=2)
        for u in order:
            third[p][u].start()
    for u in order:
        for p in parts:
            third[p][u].on()
    for u in order:
        for p in parts:
            third[p][u].end()
            if u != ME:
                middle[p].send(u)
    for p in parts:
        middle[p].arrive()
        for u in order:
            middle[p].add(spots[p][0][u])
            if u != ME:
                last[p].send(u)
    for p in parts:
        last[p].arrive()
        got = last[p].wholes
        total = mid[:, pl.ds(pl.multiple_of(own_cols + STARTS[p], 128), WIDTHS[p])]
        total = total + sums[p][here[0], here[1], here[2]].astype(F32)
        for n in range(3):
            total = total + got[n].astype(F32)
        out[:, STARTS[p] : STARTS[p] + WIDTHS[p]] = total.astype(BF16)
    for group in third + [middle, last]:
        for back in group:
            for copy in back.copies:
                copy.wait_send()


def run_ffn(partial, meta, stream, gain, mix, eg, eu, ed, dg, du, dd):
    vmem = pl.BlockSpec(memory_space=VMEM)
    hbm = pl.BlockSpec(memory_space=pltpu.HBM)
    blocks = lambda *lead: [VMEM((*lead, WIDTHS[p]), BF16) for p in range(3)]
    sem = pltpu.SemaphoreType.DMA
    return pl.pallas_call(
        ffn_kernel,
        out_shape=jax.ShapeDtypeStruct((ROWS, HALF), BF16),
        in_specs=[vmem] * 2 + [hbm] * 9,
        out_specs=vmem,
        scratch_shapes=[
            *[VMEM((4, 4, 4, BLOCK_ROWS[p], WIDTHS[p]), BF16) for p in range(3)],
            *blocks(4, 4, 4, ROWS),
            *blocks(4, 4, 4, ROWS),
            *blocks(4, 2, 2, ROWS),
            *blocks(4, 2, 4, ROWS),
            *blocks(3, ROWS),
            *blocks(3, 4, ROWS),
            VMEM((ROWS, 2 * HALF), BF16),
            VMEM((ROWS, 2 * HALF), BF16),
            VMEM((ROWS, 2 * HALF), F32),
            VMEM((HPAD, 2 * HALF), BF16),
            VMEM((HPAD, 2 * HALF), BF16),
            VMEM((HPAD, HALF), BF16),
            VMEM((HPAD, HALF), BF16),
            VMEM((256, HALF), BF16),
            VMEM((256, HALF), BF16),
            VMEM((DENSE, HALF), BF16),
            VMEM((128, HALF), BF16),
            VMEM((GROUPS * SLOTS, 2 * HALF), BF16),
            VMEM((GROUPS * SLOTS, 128), F32),
            VMEM((GROUPS * SLOTS, HPAD), BF16),
            VMEM((GROUPS * SLOTS, HPAD), BF16),
            VMEM((GROUPS, GROUP_ROWS, 256), BF16),
            VMEM((GROUPS, 128, HALF), BF16),
            sem((6,)),
            sem((252,)),
            sem((252,)),
            sem((39,)),
            sem((39,)),
            sem((72,)),
            sem((72,)),
            sem((6,)),
            sem((6,)),
            VMEM((ROWS, 2 * HALF), BF16),
            VMEM((1, 2 * HALF), F32),
            VMEM((1, HALF), F32),
            sem((3,)),
        ],
        compiler_params=pltpu.CompilerParams(
            collective_id=0, has_side_effects=True, vmem_limit_bytes=67043328
        ),
        name="ffn",
    )(partial, meta, stream, gain, mix, eg, eu, ed, dg, du, dd)


def local(
    stream,
    mixer_gain,
    gate_proj,
    input_proj,
    state_maps,
    step_proj,
    step_bias,
    decay_rate,
    input_taps,
    map_taps,
    input_past,
    map_past,
    head_state,
    skip_gain,
    inner_gain,
    mixer_out,
    channel_gain,
    expert_ids,
    expert_weight,
    expert_gate,
    expert_up,
    expert_down,
    dense_gate,
    dense_up,
    dense_down,
    dense_mix,
):
    state_out, partial, meta = run_mixer(
        stream,
        mixer_gain.reshape(1, -1),
        step_proj.T,
        expert_ids.T,
        expert_weight.T,
        step_bias,
        decay_rate,
        skip_gain,
        input_proj,
        input_taps,
        jnp.transpose(input_past, (1, 0, 2)),
        state_maps,
        map_taps,
        jnp.transpose(map_past, (0, 2, 1, 3)).reshape(192, 128),
        inner_gain.reshape(1, -1),
        gate_proj,
        mixer_out,
        head_state.reshape(256, 4096),
    )
    out = run_ffn(
        partial,
        meta,
        stream,
        channel_gain.reshape(1, -1),
        dense_mix.reshape(1, -1),
        expert_gate.T,
        expert_up.T,
        expert_down,
        dense_gate.T,
        dense_up.T,
        dense_down,
    )
    return out, state_out.reshape(head_state.shape)


def solution(mesh):
    placed = (
        P("ep", None),
        P(),
        P(None, "tp"),
        P(None, "tp"),
        P(None, None, "tp"),
        P(None, "tp"),
        P("tp"),
        P("tp"),
        P(None, "tp"),
        P(None, None, "tp"),
        P("ep", None, "tp"),
        P("ep", None, None, "tp"),
        P("ep", "tp", None),
        P("tp"),
        P("tp"),
        P("tp", None),
        P(),
        P("ep", None),
        P("ep", None),
        P(None, ("ep", "tp")),
        P(None, ("ep", "tp")),
        P(("ep", "tp"), None),
        P("tp", "ep"),
        P("tp", "ep"),
        P("ep", "tp"),
        P("tp"),
    )
    return jax.shard_map(
        local,
        mesh=mesh,
        in_specs=placed,
        out_specs=(P("ep", "tp"), P("ep", "tp", None)),
        check_vma=False,
    )
```

```python
import functools

import jax
import jax.numpy as jnp
from jax import lax
from jax.experimental import pallas as pl
from jax.experimental.pallas import tpu as pltpu
from jax.sharding import PartitionSpec as P

EPS = 1e-06
MESH = pl.DeviceIdType.MESH
F32 = jnp.float32
BF16 = jnp.bfloat16
VMEM = pltpu.VMEM
ANY = pl.ANY

HEADS = 8
ROWS = 32
EXPERTS = 8
CAP = 12
CHUNKS = 8
CHUNK = 512
GROUPS = 8
GROUP_ROWS = 256
SLOTS = 96
HALF = 1024
HIDDEN = 448
HPAD = 512
DENSE = 88
WIDTH = 2048
INNER = 2048
META = 2560
CARRY = 2816

WIDTHS = (384, 384, 256)
STARTS = (0, 384, 768)
BLOCK_ROWS = (32, 32, 48)
ORDERS = ((2, 1, 0), (1, 0, 2), (0, 2, 1))


def dot(a, b):
    return jnp.dot(a, b, preferred_element_type=F32)


def dot_nt(a, b):
    return lax.dot_general(a, b, (((1,), (1,)), ((), ())), preferred_element_type=F32)


def dot_tn(a, b):
    return lax.dot_general(a, b, (((0,), (0,)), ((), ())), preferred_element_type=F32)


def silu(v):
    return v / (1.0 + jnp.exp(-v))


def rms(v):
    return v * lax.rsqrt(jnp.mean(v * v, axis=-1, keepdims=True) + EPS)


def split(v):
    high = v.astype(BF16)
    return high, (v - high.astype(F32)).astype(BF16)


def mixer_kernel(*refs):
    given, refs = refs[:19], refs[19:]
    state_hbm = given[18]
    state_out, carry_hbm = refs[:2]
    held, refs = refs[2:20], refs[20:]
    (
        stream,
        mixer_gain,
        step_t,
        ids,
        weights,
        bias,
        decay,
        skip,
        input_w,
        input_taps,
        input_past,
        maps_w,
        map_taps,
        map_past,
        inner_gain,
        gate_w,
        channel_gain,
        mix,
    ) = held
    old, new, dec, write, read, xs_high, xs_low, tmp, y, past, carry, in_sems, sems, out_sems = (
        refs
    )
    loads = [
        pltpu.make_async_copy(src, dst, in_sems.at[n])
        for n, (src, dst) in enumerate(zip(given, held))
    ]

    def load_state(t):
        cols = pl.ds(pl.multiple_of(t * CHUNK, CHUNK), CHUNK)
        return pltpu.make_async_copy(state_hbm.at[:, cols], old.at[t], sems.at[t])

    def store_state(t):
        cols = pl.ds(pl.multiple_of(t * CHUNK, CHUNK), CHUNK)
        return pltpu.make_async_copy(
            new.at[t], state_out.at[:, cols], sems.at[CHUNKS + t]
        )

    for load in loads[:15]:
        load.start()
    for t in range(CHUNKS):
        load_state(t).start()
    for load in loads[15:]:
        load.start()

    for load in loads[:8]:
        load.wait()
    normed = (rms(stream[...].astype(F32)) * mixer_gain[...]).astype(BF16)
    steps = dot_nt(normed, step_t[...])

    expert_of = lax.broadcasted_iota(jnp.int32, (EXPERTS, ROWS), 0)
    hit0 = (ids[0:1, :] == expert_of).astype(F32)
    hit1 = (ids[1:2, :] == expert_of).astype(F32)
    member = hit0 + hit1
    upper = (
        lax.broadcasted_iota(jnp.int32, (ROWS, ROWS), 0)
        <= lax.broadcasted_iota(jnp.int32, (ROWS, ROWS), 1)
    ).astype(BF16)
    rank = dot(member.astype(BF16), upper) * member
    weight = hit0 * weights[0:1, :] + hit1 * weights[1:2, :]
    w_high = weight.astype(BF16).astype(F32)
    w_low = weight - w_high
    table = jnp.concatenate(
        [rank, w_high, w_low, jnp.zeros((104, ROWS), F32)], axis=0
    ).astype(BF16)
    eye = (
        lax.broadcasted_iota(jnp.int32, (ROWS, ROWS), 0)
        == lax.broadcasted_iota(jnp.int32, (ROWS, ROWS), 1)
    ).astype(BF16)
    by_row = dot_nt(eye, table)
    carry[0:16, META : META + 256] = jnp.concatenate([by_row[0:16], by_row[16:32]], axis=1)
    carry[0:ROWS, 0:WIDTH] = stream[...].astype(F32)

    for load in loads[8:11]:
        load.wait()
    newest = dot(normed, input_w[...]).astype(BF16).astype(F32)
    conv = newest * input_taps[3:4, :]
    for t in range(3):
        conv = conv + input_past[t].astype(F32) * input_taps[t : t + 1, :]
    conv = silu(conv)

    for load in loads[11:14]:
        load.wait()
    past[...] = map_past[...].astype(F32)
    conv_maps = []
    for m in range(2):
        new_map = dot(normed, maps_w[m]).astype(BF16).astype(F32)
        acc = new_map * map_taps[m, 3:4, :]
        for t in range(3):
            acc = acc + past[pl.ds(2 * t + m, ROWS, stride=6), :] * map_taps[m, t : t + 1, :]
        conv_maps.append(silu(acc))

    lane = lax.broadcasted_iota(jnp.int32, (ROWS, 128), 1)
    low_half = lane < 64

    def both_halves(v):
        turned = pltpu.roll(v, 64, 1)
        return jnp.where(low_half, v, turned), jnp.where(low_half, turned, v)

    write_by_group = both_halves(conv_maps[0])
    read_by_group = both_halves(conv_maps[1])
    for h in range(HEADS):
        rows = pl.ds(h, ROWS, stride=HEADS)
        v = jnp.broadcast_to(steps[:, h : h + 1], (ROWS, 128)) + bias[h]
        step = jnp.maximum(v, 0.0) + jnp.log1p(jnp.exp(-jnp.abs(v)))
        dec[rows, :] = jnp.exp(-decay[h] * step)
        pair = conv[:, 128 * (h // 2) : 128 * (h // 2) + 128]
        mine = low_half if h % 2 == 0 else jnp.logical_not(low_half)
        tmp[rows, :] = jnp.where(mine, step * pair, 0.0)
        write[rows, :] = write_by_group[h // 4]
        read[rows, :] = read_by_group[h // 4]
    high, low = split(tmp[...])
    xs_high[...] = high
    xs_low[...] = low
    y[...] = jnp.zeros_like(y)

    slot = lax.broadcasted_iota(jnp.int32, (128, CHUNK), 0) % 64
    place = lax.broadcasted_iota(jnp.int32, (128, CHUNK), 1) // 64

    def chunk_step(t, carry):
        spread = (slot == place + 8 * t).astype(F32).astype(BF16)
        load_state(t).wait()
        values = dot(xs_high[...], spread) + dot(xs_low[...], spread)
        wide = lambda ref: jnp.concatenate([ref[...]] * (CHUNK // 128), axis=1)
        fresh = wide(dec) * old[t] + values * wide(write)
        new[t] = fresh
        store_state(t).start()
        high, low = split(fresh * wide(read))
        y[...] += dot_nt(high, spread) + dot_nt(low, spread)
        return carry

    lax.fori_loop(0, CHUNKS, chunk_step, 0)

    for load in loads[14:]:
        load.wait()
    carry[ROWS : ROWS + 1, 0:WIDTH] = channel_gain[...]
    carry[ROWS + 1 : ROWS + 2, 0:HALF] = mix[...]
    out_parts = []
    for n, (first, size) in enumerate(((0, WIDTH), (META, 256), (INNER, 512))):
        where = (pl.ds(0, ROWS + 8), pl.ds(first, size))
        out_parts.append(
            pltpu.make_async_copy(carry.at[where], carry_hbm.at[where], out_sems.at[n])
        )
    out_parts[0].start()
    out_parts[1].start()
    gate = silu(dot(normed, gate_w[...]).astype(BF16).astype(F32))
    pieces = []
    for j in range(HEADS // 2):
        even = y[pl.ds(2 * j, ROWS, stride=HEADS), :]
        odd = y[pl.ds(2 * j + 1, ROWS, stride=HEADS), :]
        gain = jnp.where(low_half, skip[2 * j], skip[2 * j + 1])
        cols = slice(128 * j, 128 * j + 128)
        pieces.append(
            (jnp.where(low_half, even, odd) + gain * conv[:, cols]) * gate[:, cols]
        )
    groups = [jnp.concatenate(pieces[2 * g : 2 * g + 2], axis=1) for g in range(2)]
    inner = jnp.concatenate([rms(g) for g in groups], axis=1) * inner_gain[...]
    carry[0:ROWS, INNER : INNER + 512] = inner
    out_parts[2].start()
    for part in out_parts:
        part.wait()
    for t in range(CHUNKS):
        store_state(t).wait()


def run_mixer(*given):
    hbm = pl.BlockSpec(memory_space=pltpu.HBM)
    lanes = lambda: VMEM((256, 128), F32)
    held = [
        (pltpu.SMEM if 5 <= n < 8 else VMEM)(v.shape, v.dtype)
        for n, v in enumerate(given[:18])
    ]
    return pl.pallas_call(
        mixer_kernel,
        out_shape=(
            jax.ShapeDtypeStruct((256, 4096), F32),
            jax.ShapeDtypeStruct((ROWS + 8, CARRY), F32),
        ),
        in_specs=[hbm] * 19,
        out_specs=(hbm, hbm),
        scratch_shapes=[
            *held,
            VMEM((CHUNKS, 256, CHUNK), F32),
            VMEM((CHUNKS, 256, CHUNK), F32),
            lanes(),
            lanes(),
            lanes(),
            VMEM((256, 128), BF16),
            VMEM((256, 128), BF16),
            lanes(),
            lanes(),
            VMEM((192, 128), F32),
            VMEM((ROWS + 8, CARRY), F32),
            pltpu.SemaphoreType.DMA((18,)),
            pltpu.SemaphoreType.DMA((2 * CHUNKS,)),
            pltpu.SemaphoreType.DMA((3,)),
        ],
        compiler_params=pltpu.CompilerParams(vmem_limit_bytes=67043328),
        name="mixer",
    )(*given)


def ffn_kernel(
    carry_hbm,
    ow_hbm,
    eg_hbm,
    eu_hbm,
    ed_hbm,
    dg_hbm,
    du_hbm,
    dd_hbm,
    out,
    x0,
    x1,
    x2,
    y0,
    y1,
    y2,
    s0,
    s1,
    s2,
    *rest,
):
    landed, rest = rest[:12], rest[12:]
    landing = [landed[3 * k : 3 * k + 3] for k in range(4)]
    (
    other_partial,
    wide,
    mid,
    eg,
    eu,
    ed,
    ed_other,
    dgu,
    dgu_other,
    dd,
    dd_scaled,
    packed,
    slot_weight,
    act,
    act_other,
    left_side,
    result,
    local_sem,
    ag_send,
    ag_recv,
    dd_send,
    dd_recv,
    rs_send,
    rs_recv,
    mi_send,
    mi_recv,
        carry,
        out_w,
        partial,
        small_sem,
    ) = rest
    ep = lax.axis_index("ep")
    core = lax.axis_index("tp")
    coords = (ep // 16, (ep // 4) % 4, ep % 4)
    other = 1 - core
    own_cols = pl.multiple_of(core * HALF, HALF)
    other_cols = pl.multiple_of(other * HALF, HALF)
    expert = ep // 8
    mine = (x0, x1, x2)
    theirs = (y0, y1, y2)
    sums = (s0, s1, s2)

    def neighbour(dim, shift):
        moved = list(coords)
        moved[dim] = lax.rem(coords[dim] + shift, 4)
        return (moved[0] * 16 + moved[1] * 4 + moved[2], core)

    partner = (ep, other)

    small = [
        pltpu.make_async_copy(carry_hbm, carry, small_sem.at[0]),
        pltpu.make_async_copy(ow_hbm, out_w, small_sem.at[1]),
    ]
    for load in small:
        load.start()
    barrier = pltpu.get_barrier_semaphore()
    for dim in range(3):
        for shift in (1, 2, 3):
            pl.semaphore_signal(
                barrier, inc=1, device_id=neighbour(dim, shift), device_id_type=MESH
            )
    pl.semaphore_signal(barrier, inc=1, device_id=partner, device_id_type=MESH)
    for load in small:
        load.wait()
    inner = carry[0:ROWS, INNER : INNER + 512].astype(BF16)
    partial[...] = dot(inner, out_w[...]).astype(BF16)
    pl.semaphore_wait(barrier, 10)

    def to_partner(src, dst, n):
        return pltpu.make_async_remote_copy(
            src_ref=src,
            dst_ref=dst,
            send_sem=mi_send.at[n],
            recv_sem=mi_recv.at[n],
            device_id=partner,
            device_id_type=MESH,
        )

    swap_partial = to_partner(partial, other_partial, 0)
    swap_partial.start()
    loads = [
        pltpu.make_async_copy(eg_hbm, eg.at[pl.ds(0, HIDDEN)], local_sem.at[0]),
        pltpu.make_async_copy(eu_hbm, eu.at[pl.ds(0, HIDDEN)], local_sem.at[1]),
        pltpu.make_async_copy(
            ed_hbm.at[:, pl.ds(own_cols, HALF)], ed.at[pl.ds(0, HIDDEN)], local_sem.at[2]
        ),
        pltpu.make_async_copy(dg_hbm, dgu.at[pl.ds(0, DENSE)], local_sem.at[3]),
        pltpu.make_async_copy(du_hbm, dgu.at[pl.ds(128, DENSE)], local_sem.at[4]),
        pltpu.make_async_copy(dd_hbm, dd, local_sem.at[5]),
    ]
    for load in loads:
        load.start()

    swap_partial.wait()
    mixed = partial[...].astype(F32) + other_partial[...].astype(F32)
    hidden = carry[0:ROWS, 0:WIDTH] + mixed
    mid[...] = hidden
    wide[...] = (rms(hidden) * carry[ROWS : ROWS + 1, 0:WIDTH]).astype(BF16)
    here = coords
    for p in range(3):
        cols = pl.ds(pl.multiple_of(own_cols + STARTS[p], 128), WIDTHS[p])
        mine[p][here[0], here[1], here[2], 0:ROWS, :] = wide[:, cols]
    x2[here[0], here[1], here[2], ROWS : ROWS + 16, :] = carry[0:16, META : META + 256].astype(
        BF16
    )

    def cut(buf, p, where, half=None, rows=None):
        index = [None, None, None]
        for q in range(3):
            index[ORDERS[p][q]] = pl.ds(0, 4) if where[q] is None else where[q]
        if half is not None:
            free = sorted(ORDERS[p][q] for q in range(3) if where[q] is None)
            if free:
                index[free[0]] = pl.ds(2 * half, 2)
            else:
                rows = pl.ds(0, 16) if half == 0 else pl.ds(16, rows - 16)
        elif rows is not None:
            rows = pl.ds(0, rows)
        if rows is not None and not (half is not None and free):
            index.append(rows)
        return buf.at[tuple(index)]

    def turn(p, k, shift):
        return lax.rem(coords[ORDERS[p][k]] + shift, 4)

    ME, RIGHT, FAR, LEFT = 0, 1, 2, 3
    spots = [[[turn(p, k, shift) for shift in range(4)] for k in range(3)] for p in range(3)]

    class Ring:
        def __init__(self, p, k, at, place, direct=False):
            self.p, self.k, self.place, self.direct = p, k, place, direct
            self.copies = [self.copy(at, ME, None, 1), self.copy(at + 1, ME, None, 3)]
            if direct:
                self.copies.append(self.copy(at + 2, ME, None, 2))
            else:
                self.copies.append(self.copy(at + 2, LEFT, 0, 1))
                self.copies.append(self.copy(at + 3, RIGHT, 1, 3))

        def copy(self, at, shift, half, to):
            p = self.p
            where = list(self.place)
            where[self.k] = spots[p][self.k][shift]
            rows = BLOCK_ROWS[p] if half is not None else None
            ref = cut(mine[p], p, where, half, rows)
            return pltpu.make_async_remote_copy(
                src_ref=ref,
                dst_ref=ref,
                send_sem=ag_send.at[at],
                recv_sem=ag_recv.at[at],
                device_id=neighbour(ORDERS[p][self.k], to),
                device_id_type=MESH,
            )

        def start(self):
            if self.direct:
                self.copies[2].start()
            self.copies[0].start()
            self.copies[1].start()

        def on(self):
            self.copies[0].wait_recv()
            if not self.direct:
                self.copies[2].start()
            self.copies[1].wait_recv()
            if not self.direct:
                self.copies[3].start()

        def end(self):
            for copy in self.copies[2:]:
                copy.wait_recv()

    first, second, third_way = [], [], []
    for p in range(3):
        at = 84 * p
        own = [spots[p][k][ME] for k in range(3)]
        first.append(Ring(p, 0, at, own, True))
        second.append(
            [Ring(p, 1, at + 4 + 4 * u, [spots[p][0][u], None, own[2]], True) for u in range(4)]
        )
        third_way.append(
            [
                [
                    Ring(
                        p,
                        2,
                        at + 20 + 16 * u + 4 * v,
                        [spots[p][0][u], spots[p][1][v], None],
                        FAR in (u, v) and ME not in (u, v),
                    )
                    for v in range(4)
                ]
                for u in range(4)
            ]
        )
    rings = [first] + second + [row for part in third_way for row in part]
    hand_overs = []

    def hand_over(p, n, second_at, third_at):
        where = [None, second_at, third_at]
        copy = pltpu.make_async_remote_copy(
            src_ref=cut(mine[p], p, where, None, ROWS),
            dst_ref=cut(theirs[p], p, where, None, ROWS),
            send_sem=dd_send.at[13 * p + n],
            recv_sem=dd_recv.at[13 * p + n],
            device_id=partner,
            device_id_type=MESH,
        )
        copy.start()
        hand_overs.append(copy)

    parts = range(3)
    def launch(*pairs):
        for p in parts:
            for u, v in pairs:
                third_way[p][u][v].start()

    def pass_on(*pairs):
        for p in parts:
            for u, v in pairs:
                third_way[p][u][v].on()

    for p in parts:
        first[p].start()
    for p in parts:
        second[p][ME].start()
    launch((ME, ME))

    early = [
        to_partner(
            ed_hbm.at[:, pl.ds(other_cols, HALF)], ed_other.at[pl.ds(0, HIDDEN)], 1
        ),
        to_partner(dg_hbm, dgu_other.at[pl.ds(0, DENSE)], 2),
        to_partner(du_hbm, dgu_other.at[pl.ds(128, DENSE)], 3),
    ]
    for copy in early:
        copy.start()

    for p in parts:
        first[p].on()
        for u in (LEFT, RIGHT):
            second[p][u].start()
            third_way[p][u][ME].start()
    for p in parts:
        second[p][ME].on()
    launch((ME, RIGHT), (ME, LEFT))
    for p in parts:
        first[p].end()
        second[p][FAR].start()
        third_way[p][FAR][ME].start()
    for p in parts:
        second[p][ME].end()
    launch((ME, FAR))
    pass_on((ME, ME))
    for ref in (eg, eu, ed, ed_other):
        ref[HIDDEN:HPAD, :] = jnp.zeros((HPAD - HIDDEN, ref.shape[1]), BF16)
    for ref in (dgu, dgu_other):
        ref[DENSE:128, :] = jnp.zeros((128 - DENSE, HALF), BF16)
        ref[128 + DENSE : 256, :] = jnp.zeros((128 - DENSE, HALF), BF16)
    dd_scaled[DENSE:128, :] = jnp.zeros((128 - DENSE, HALF), BF16)
    for g in range(GROUPS):
        result[g, SLOTS:128, :] = jnp.zeros((128 - SLOTS, HALF), BF16)
    for p in parts:
        second[p][LEFT].on()
        second[p][RIGHT].on()
    launch((LEFT, RIGHT), (RIGHT, RIGHT), (LEFT, LEFT), (RIGHT, LEFT))
    pass_on((LEFT, ME), (RIGHT, ME), (ME, RIGHT), (ME, LEFT))
    for p in parts:
        second[p][LEFT].end()
        second[p][RIGHT].end()
    launch((LEFT, FAR), (RIGHT, FAR))
    for p in parts:
        second[p][FAR].on()
    launch((FAR, RIGHT), (FAR, LEFT))
    for p in parts:
        second[p][FAR].end()
    launch((FAR, FAR))
    pass_on((FAR, ME), (ME, FAR))
    for p in parts:
        hand_over(p, 0, None, spots[p][2][ME])
        hand_over(p, 1, spots[p][1][ME], spots[p][2][LEFT])
        hand_over(p, 2, spots[p][1][ME], spots[p][2][RIGHT])

    def finish(v, n):
        for p in parts:
            for u in range(4):
                third_way[p][u][v].end()
            hand_over(p, n, spots[p][1][v], spots[p][2][FAR])

    def sides(v, n):
        for p in parts:
            hand_over(p, n, spots[p][1][v], spots[p][2][LEFT])
            hand_over(p, n + 1, spots[p][1][v], spots[p][2][RIGHT])

    pass_on((LEFT, RIGHT), (RIGHT, RIGHT), (LEFT, LEFT), (RIGHT, LEFT))
    finish(ME, 3)
    pass_on((LEFT, FAR), (RIGHT, FAR), (FAR, RIGHT), (FAR, LEFT))
    sides(RIGHT, 4)
    sides(LEFT, 6)
    pass_on((FAR, FAR))
    sides(FAR, 8)
    finish(RIGHT, 10)
    finish(LEFT, 11)
    finish(FAR, 12)
    pick_row = lax.broadcasted_iota(jnp.int32, (128, 128), 0)
    pick_rank = (pick_row == expert).astype(F32).astype(BF16)
    pick_weight = (
        jnp.logical_or(pick_row == expert + 8, pick_row == expert + 16)
    ).astype(F32).astype(BF16)
    lane = lax.broadcasted_iota(jnp.int32, (GROUP_ROWS, 128), 1)
    source = lax.broadcasted_iota(jnp.int32, (GROUP_ROWS, 128), 0) // ROWS

    def group_of(bufs, g):
        z, y = g // 2, 2 * lax.rem(g, 2)
        return jnp.concatenate(
            [
                bufs[p][z, pl.ds(y, 2), :, 0:ROWS, :].reshape(GROUP_ROWS, WIDTHS[p])
                for p in range(3)
            ],
            axis=1,
        )

    def pack_group(g, carry):
        z, y = g // 2, 2 * lax.rem(g, 2)
        tags = x2[z, pl.ds(y, 2), :, ROWS : ROWS + 16, :].reshape(8, 16, 256)
        tags = jnp.concatenate([tags[:, :, 0:128], tags[:, :, 128:256]], axis=1)
        tags = tags.reshape(GROUP_ROWS, 128)
        rank = dot(tags, pick_rank).astype(jnp.int32)
        hit = jnp.logical_and(rank > 0, rank + (CAP * source - 1) == lane)
        table = hit.astype(F32).astype(BF16)
        left_side[g, :, 0:128] = table
        used = table[:, 0:SLOTS]
        slots = pl.ds(pl.multiple_of(g * SLOTS, SLOTS), SLOTS)
        packed[slots, pl.ds(own_cols, HALF)] = dot_tn(used, group_of(mine, g)).astype(BF16)
        slot_tags = dot_tn(used, tags).astype(BF16)
        slot_weight[slots, :] = dot(slot_tags, pick_weight)
        return carry

    lax.fori_loop(0, GROUPS, pack_group, 0, unroll=2)
    for load in loads:
        load.wait()
    for copy in early:
        copy.wait()
    for group in rings:
        for ring in group:
            for copy in ring.copies:
                copy.wait_send()
    for copy in hand_overs:
        copy.wait()

    def pack_other(g, carry):
        used = left_side[g, :, 0:SLOTS]
        slots = pl.ds(pl.multiple_of(g * SLOTS, SLOTS), SLOTS)
        packed[slots, pl.ds(other_cols, HALF)] = dot_tn(used, group_of(theirs, g)).astype(
            BF16
        )
        return carry

    lax.fori_loop(0, GROUPS, pack_other, 0, unroll=2)

    sends = []
    for i in range(2):
        units = pl.ds(256 * i, 256)
        gate = dot_nt(packed[...], eg[units, :])
        up = dot_nt(packed[...], eu[units, :])
        act[:, units] = (silu(gate) * up * slot_weight[:, 0:1]).astype(BF16)
        copy = to_partner(act.at[:, units], act_other.at[:, units], 4 + i)
        copy.start()
        sends.append(copy)

    def dense_group(g, carry):
        both = dot_nt(group_of(mine, g), dgu[...]) + dot_nt(group_of(theirs, g), dgu_other[...])
        left_side[g, :, 128:256] = (silu(both[:, 0:128]) * both[:, 128:256]).astype(BF16)
        return carry

    lax.fori_loop(0, GROUPS, dense_group, 0, unroll=2)
    share = 1.0 / (1.0 + jnp.exp(-carry[ROWS + 1 : ROWS + 2, 0:HALF]))
    dd_scaled[0:DENSE, :] = (dd[...].astype(F32) * share).astype(BF16)

    class Back:
        def __init__(self, p, k, at, place, slot):
            self.p, self.k, self.place, self.slot = p, k, place, slot
            self.halves, self.wholes = landing[0][p], landing[1][p]
            self.copies = [
                self.copy(at, FAR, 0, 1, self.halves.at[slot, 0]),
                self.copy(at + 1, FAR, 1, 3, self.halves.at[slot, 1]),
                self.copy(at + 2, RIGHT, None, 1, self.wholes.at[slot, 0]),
                self.copy(at + 3, LEFT, None, 3, self.wholes.at[slot, 1]),
            ]

        def spot(self, shift):
            where = list(self.place)
            where[self.k] = spots[self.p][self.k][shift]
            return where

        def copy(self, at, shift, half, to, target):
            p = self.p
            rows = ROWS if half is not None else None
            return pltpu.make_async_remote_copy(
                src_ref=cut(sums[p], p, self.spot(shift), half, rows),
                dst_ref=target,
                send_sem=rs_send.at[at],
                recv_sem=rs_recv.at[at],
                device_id=neighbour(ORDERS[p][self.k], to),
                device_id_type=MESH,
            )

        def start(self):
            self.copies[0].start()
            self.copies[1].start()

        def add_half(self, shift, half):
            p, got = self.p, self.halves
            where = self.spot(shift)
            place = [None, None, None]
            for q in range(3):
                place[ORDERS[p][q]] = where[q]
            free = [d for d in range(3) if place[d] is None]
            for t in range(2):
                place[free[0]] = 2 * half + t
                ref = sums[p].at[tuple(place)]
                ref[...] = ref[...] + got[self.slot, half, t]

        def on(self):
            self.copies[0].wait_recv()
            self.add_half(RIGHT, 0)
            self.copies[2].start()
            self.copies[1].wait_recv()
            self.add_half(LEFT, 1)
            self.copies[3].start()

        def end(self):
            p, got = self.p, self.wholes
            self.copies[2].wait_recv()
            self.copies[3].wait_recv()
            where = self.spot(ME)
            place = [None, None, None]
            for q in range(3):
                place[ORDERS[p][q]] = where[q]
            free = [d for d in range(3) if place[d] is None]
            for t in range(4):
                place[free[0]] = t
                ref = sums[p].at[tuple(place)]
                total = ref[...].astype(F32) + got[self.slot, 0, t].astype(F32)
                ref[...] = (total + got[self.slot, 1, t].astype(F32)).astype(BF16)

    class Straight:
        def __init__(self, p, k, at, place):
            self.p, self.k, self.place, self.wholes = p, k, place, landing[2 + k][p]
            self.copies = [self.copy(at + u - 1, u) for u in (RIGHT, FAR, LEFT)]

        def copy(self, at, u):
            p = self.p
            where = list(self.place)
            where[self.k] = spots[p][self.k][u]
            return pltpu.make_async_remote_copy(
                src_ref=cut(sums[p], p, where),
                dst_ref=self.wholes.at[u - 1],
                send_sem=rs_send.at[at],
                recv_sem=rs_recv.at[at],
                device_id=neighbour(ORDERS[p][self.k], u),
                device_id_type=MESH,
            )

        def send(self, u):
            self.copies[u - 1].start()

        def arrive(self):
            for copy in self.copies:
                copy.wait_recv()

        def add(self, first_at):
            p, got = self.p, self.wholes
            place = [None, None, None]
            for q in range(3):
                place[ORDERS[p][q]] = spots[p][q][ME]
            place[ORDERS[p][0]] = first_at
            ref = sums[p].at[tuple(place)]
            total = ref[...].astype(F32)
            for n in range(3):
                total = total + got[n, first_at].astype(F32)
            ref[...] = total.astype(BF16)

    third, middle, last = [], [], []
    for p in parts:
        at = 24 * p
        own = [spots[p][k][ME] for k in range(3)]
        third.append(
            [Back(p, 2, at + 4 * u, [None, spots[p][1][u], None], u) for u in range(4)]
        )
        middle.append(Straight(p, 1, at + 16, [None, None, own[2]]))
        last.append(Straight(p, 0, at + 20, own))
    order = (FAR, LEFT, RIGHT, ME)
    for send in sends:
        send.wait()
    for p in parts:
        cols = slice(STARTS[p], STARTS[p] + WIDTHS[p])
        back = dot(act[...], ed[:, cols]) + dot(act_other[...], ed_other[:, cols])
        result[:, 0:SLOTS, cols] = back.astype(BF16).reshape(GROUPS, SLOTS, WIDTHS[p])

        def spread_group(g, carry):
            z, y = g // 2, 2 * lax.rem(g, 2)
            right_side = jnp.concatenate([result[g, :, cols], dd_scaled[:, cols]], axis=0)
            total = dot(left_side[g], right_side).astype(BF16)
            sums[p][z, pl.ds(y, 2)] = total.reshape(2, 4, ROWS, WIDTHS[p])
            return carry

        lax.fori_loop(0, GROUPS, spread_group, 0, unroll=2)
        for u in order:
            third[p][u].start()
    for u in order:
        for p in parts:
            third[p][u].on()
    for u in order:
        for p in parts:
            third[p][u].end()
            if u != ME:
                middle[p].send(u)
    for p in parts:
        middle[p].arrive()
        for u in order:
            middle[p].add(spots[p][0][u])
            if u != ME:
                last[p].send(u)
    for p in parts:
        last[p].arrive()
        got = last[p].wholes
        total = mid[:, pl.ds(pl.multiple_of(own_cols + STARTS[p], 128), WIDTHS[p])]
        total = total + sums[p][here[0], here[1], here[2]].astype(F32)
        for n in range(3):
            total = total + got[n].astype(F32)
        out[:, STARTS[p] : STARTS[p] + WIDTHS[p]] = total.astype(BF16)
    for group in third + [middle, last]:
        for back in group:
            for copy in back.copies:
                copy.wait_send()


def run_ffn(carry, out_w, eg, eu, ed, dg, du, dd):
    vmem = pl.BlockSpec(memory_space=VMEM)
    hbm = pl.BlockSpec(memory_space=pltpu.HBM)
    blocks = lambda *lead: [VMEM((*lead, WIDTHS[p]), BF16) for p in range(3)]
    sem = pltpu.SemaphoreType.DMA
    return pl.pallas_call(
        ffn_kernel,
        out_shape=jax.ShapeDtypeStruct((ROWS, HALF), BF16),
        in_specs=[hbm] * 8,
        out_specs=vmem,
        scratch_shapes=[
            *[VMEM((4, 4, 4, BLOCK_ROWS[p], WIDTHS[p]), BF16) for p in range(3)],
            *blocks(4, 4, 4, ROWS),
            *blocks(4, 4, 4, ROWS),
            *blocks(4, 2, 2, ROWS),
            *blocks(4, 2, 4, ROWS),
            *blocks(3, ROWS),
            *blocks(3, 4, ROWS),
            VMEM((ROWS, 2 * HALF), BF16),
            VMEM((ROWS, 2 * HALF), BF16),
            VMEM((ROWS, 2 * HALF), F32),
            VMEM((HPAD, 2 * HALF), BF16),
            VMEM((HPAD, 2 * HALF), BF16),
            VMEM((HPAD, HALF), BF16),
            VMEM((HPAD, HALF), BF16),
            VMEM((256, HALF), BF16),
            VMEM((256, HALF), BF16),
            VMEM((DENSE, HALF), BF16),
            VMEM((128, HALF), BF16),
            VMEM((GROUPS * SLOTS, 2 * HALF), BF16),
            VMEM((GROUPS * SLOTS, 128), F32),
            VMEM((GROUPS * SLOTS, HPAD), BF16),
            VMEM((GROUPS * SLOTS, HPAD), BF16),
            VMEM((GROUPS, GROUP_ROWS, 256), BF16),
            VMEM((GROUPS, 128, HALF), BF16),
            sem((6,)),
            sem((252,)),
            sem((252,)),
            sem((39,)),
            sem((39,)),
            sem((72,)),
            sem((72,)),
            sem((6,)),
            sem((6,)),
            VMEM((ROWS + 8, CARRY), F32),
            VMEM((512, 2 * HALF), BF16),
            VMEM((ROWS, 2 * HALF), BF16),
            sem((2,)),
        ],
        compiler_params=pltpu.CompilerParams(
            collective_id=0, has_side_effects=True, vmem_limit_bytes=67043328
        ),
        name="ffn",
    )(carry, out_w, eg, eu, ed, dg, du, dd)


def local(
    stream,
    mixer_gain,
    gate_proj,
    input_proj,
    state_maps,
    step_proj,
    step_bias,
    decay_rate,
    input_taps,
    map_taps,
    input_past,
    map_past,
    head_state,
    skip_gain,
    inner_gain,
    mixer_out,
    channel_gain,
    expert_ids,
    expert_weight,
    expert_gate,
    expert_up,
    expert_down,
    dense_gate,
    dense_up,
    dense_down,
    dense_mix,
):
    state_out, carry = run_mixer(
        stream,
        mixer_gain.reshape(1, -1),
        step_proj.T,
        expert_ids.T,
        expert_weight.T,
        step_bias,
        decay_rate,
        skip_gain,
        input_proj,
        input_taps,
        jnp.transpose(input_past, (1, 0, 2)),
        state_maps,
        map_taps,
        jnp.transpose(map_past, (0, 2, 1, 3)).reshape(192, 128),
        inner_gain.reshape(1, -1),
        gate_proj,
        channel_gain.reshape(1, -1),
        dense_mix.reshape(1, -1),
        head_state.reshape(256, 4096),
    )
    out = run_ffn(
        carry,
        mixer_out,
        expert_gate.T,
        expert_up.T,
        expert_down,
        dense_gate.T,
        dense_up.T,
        dense_down,
    )
    return out, state_out.reshape(head_state.shape)


def solution(mesh):
    placed = (
        P("ep", None),
        P(),
        P(None, "tp"),
        P(None, "tp"),
        P(None, None, "tp"),
        P(None, "tp"),
        P("tp"),
        P("tp"),
        P(None, "tp"),
        P(None, None, "tp"),
        P("ep", None, "tp"),
        P("ep", None, None, "tp"),
        P("ep", "tp", None),
        P("tp"),
        P("tp"),
        P("tp", None),
        P(),
        P("ep", None),
        P("ep", None),
        P(None, ("ep", "tp")),
        P(None, ("ep", "tp")),
        P(("ep", "tp"), None),
        P("tp", "ep"),
        P("tp", "ep"),
        P("ep", "tp"),
        P("tp"),
    )
    return jax.shard_map(
        local,
        mesh=mesh,
        in_specs=placed,
        out_specs=(P("ep", "tp"), P("ep", "tp", None)),
        check_vma=False,
    )
```

```python
import functools

import jax
import jax.numpy as jnp
from jax import lax
from jax.experimental import pallas as pl
from jax.experimental.pallas import tpu as pltpu
from jax.sharding import PartitionSpec as P

EPS = 1e-06
MESH = pl.DeviceIdType.MESH
F32 = jnp.float32
BF16 = jnp.bfloat16
VMEM = pltpu.VMEM
ANY = pl.ANY

HEADS = 8
ROWS = 32
EXPERTS = 8
CAP = 12
CHUNKS = 8
CHUNK = 512
GROUPS = 8
GROUP_ROWS = 256
SLOTS = 96
HALF = 1024
HIDDEN = 448
HPAD = 512
DENSE = 88
WIDTH = 2048
INNER = 2048
META = 2560
CARRY = 2816

WIDTHS = (384, 384, 256)
STARTS = (0, 384, 768)
BLOCK_ROWS = (32, 32, 48)
ORDERS = ((2, 1, 0), (1, 0, 2), (0, 2, 1))


def dot(a, b):
    return jnp.dot(a, b, preferred_element_type=F32)


def dot_nt(a, b):
    return lax.dot_general(a, b, (((1,), (1,)), ((), ())), preferred_element_type=F32)


def dot_tn(a, b):
    return lax.dot_general(a, b, (((0,), (0,)), ((), ())), preferred_element_type=F32)


def silu(v):
    return v / (1.0 + jnp.exp(-v))


def rms(v):
    return v * lax.rsqrt(jnp.mean(v * v, axis=-1, keepdims=True) + EPS)


def split(v):
    high = v.astype(BF16)
    return high, (v - high.astype(F32)).astype(BF16)


def mixer_kernel(*refs):
    given, refs = refs[:19], refs[19:]
    state_hbm = given[18]
    state_out, carry_hbm = refs[:2]
    held, refs = refs[2:20], refs[20:]
    (
        stream,
        mixer_gain,
        step_t,
        ids,
        weights,
        bias,
        decay,
        skip,
        input_w,
        input_taps,
        input_past,
        maps_w,
        map_taps,
        map_past,
        inner_gain,
        gate_w,
        channel_gain,
        mix,
    ) = held
    old, new, dec, write, read, xs_high, xs_low, tmp, y, past, carry, in_sems, sems, out_sems = (
        refs
    )
    loads = [
        pltpu.make_async_copy(src, dst, in_sems.at[n])
        for n, (src, dst) in enumerate(zip(given, held))
    ]

    def load_state(t):
        cols = pl.ds(pl.multiple_of(t * CHUNK, CHUNK), CHUNK)
        return pltpu.make_async_copy(state_hbm.at[:, cols], old.at[t], sems.at[t])

    def store_state(t):
        cols = pl.ds(pl.multiple_of(t * CHUNK, CHUNK), CHUNK)
        return pltpu.make_async_copy(
            new.at[t], state_out.at[:, cols], sems.at[CHUNKS + t]
        )

    for load in loads[:15]:
        load.start()
    for t in range(CHUNKS):
        load_state(t).start()
    for load in loads[15:]:
        load.start()

    for load in loads[:8]:
        load.wait()
    normed = (rms(stream[...].astype(F32)) * mixer_gain[...]).astype(BF16)
    steps = dot_nt(normed, step_t[...])

    expert_of = lax.broadcasted_iota(jnp.int32, (EXPERTS, ROWS), 0)
    hit0 = (ids[0:1, :] == expert_of).astype(F32)
    hit1 = (ids[1:2, :] == expert_of).astype(F32)
    member = hit0 + hit1
    upper = (
        lax.broadcasted_iota(jnp.int32, (ROWS, ROWS), 0)
        <= lax.broadcasted_iota(jnp.int32, (ROWS, ROWS), 1)
    ).astype(BF16)
    rank = dot(member.astype(BF16), upper) * member
    weight = hit0 * weights[0:1, :] + hit1 * weights[1:2, :]
    w_high = weight.astype(BF16).astype(F32)
    w_low = weight - w_high
    table = jnp.concatenate(
        [rank, w_high, w_low, jnp.zeros((104, ROWS), F32)], axis=0
    ).astype(BF16)
    eye = (
        lax.broadcasted_iota(jnp.int32, (ROWS, ROWS), 0)
        == lax.broadcasted_iota(jnp.int32, (ROWS, ROWS), 1)
    ).astype(BF16)
    by_row = dot_nt(eye, table)
    carry[0:16, META : META + 256] = jnp.concatenate([by_row[0:16], by_row[16:32]], axis=1)
    carry[0:ROWS, 0:WIDTH] = stream[...].astype(F32)

    for load in loads[8:11]:
        load.wait()
    newest = dot(normed, input_w[...]).astype(BF16).astype(F32)
    conv = newest * input_taps[3:4, :]
    for t in range(3):
        conv = conv + input_past[t].astype(F32) * input_taps[t : t + 1, :]
    conv = silu(conv)

    for load in loads[11:14]:
        load.wait()
    past[...] = map_past[...].astype(F32)
    conv_maps = []
    for m in range(2):
        new_map = dot(normed, maps_w[m]).astype(BF16).astype(F32)
        acc = new_map * map_taps[m, 3:4, :]
        for t in range(3):
            acc = acc + past[pl.ds(2 * t + m, ROWS, stride=6), :] * map_taps[m, t : t + 1, :]
        conv_maps.append(silu(acc))

    lane = lax.broadcasted_iota(jnp.int32, (ROWS, 128), 1)
    low_half = lane < 64

    def both_halves(v):
        turned = pltpu.roll(v, 64, 1)
        return jnp.where(low_half, v, turned), jnp.where(low_half, turned, v)

    write_by_group = both_halves(conv_maps[0])
    read_by_group = both_halves(conv_maps[1])
    for h in range(HEADS):
        rows = pl.ds(h, ROWS, stride=HEADS)
        v = jnp.broadcast_to(steps[:, h : h + 1], (ROWS, 128)) + bias[h]
        step = jnp.maximum(v, 0.0) + jnp.log1p(jnp.exp(-jnp.abs(v)))
        dec[rows, :] = jnp.exp(-decay[h] * step)
        pair = conv[:, 128 * (h // 2) : 128 * (h // 2) + 128]
        mine = low_half if h % 2 == 0 else jnp.logical_not(low_half)
        tmp[rows, :] = jnp.where(mine, step * pair, 0.0)
        write[rows, :] = write_by_group[h // 4]
        read[rows, :] = read_by_group[h // 4]
    high, low = split(tmp[...])
    xs_high[...] = high
    xs_low[...] = low
    y[...] = jnp.zeros_like(y)

    slot = lax.broadcasted_iota(jnp.int32, (128, CHUNK), 0) % 64
    place = lax.broadcasted_iota(jnp.int32, (128, CHUNK), 1) // 64

    def chunk_step(t, carry):
        spread = (slot == place + 8 * t).astype(F32).astype(BF16)
        load_state(t).wait()
        values = dot(xs_high[...], spread) + dot(xs_low[...], spread)
        wide = lambda ref: jnp.concatenate([ref[...]] * (CHUNK // 128), axis=1)
        fresh = wide(dec) * old[t] + values * wide(write)
        new[t] = fresh
        store_state(t).start()
        high, low = split(fresh * wide(read))
        y[...] += dot_nt(high, spread) + dot_nt(low, spread)
        return carry

    lax.fori_loop(0, CHUNKS, chunk_step, 0, unroll=4)

    for load in loads[14:]:
        load.wait()
    carry[ROWS : ROWS + 1, 0:WIDTH] = channel_gain[...]
    carry[ROWS + 1 : ROWS + 2, 0:HALF] = mix[...]
    out_parts = []
    for n, (first, size) in enumerate(((0, WIDTH), (META, 256), (INNER, 512))):
        where = (pl.ds(0, ROWS + 8), pl.ds(first, size))
        out_parts.append(
            pltpu.make_async_copy(carry.at[where], carry_hbm.at[where], out_sems.at[n])
        )
    out_parts[0].start()
    out_parts[1].start()
    gate = silu(dot(normed, gate_w[...]).astype(BF16).astype(F32))
    pieces = []
    for j in range(HEADS // 2):
        even = y[pl.ds(2 * j, ROWS, stride=HEADS), :]
        odd = y[pl.ds(2 * j + 1, ROWS, stride=HEADS), :]
        gain = jnp.where(low_half, skip[2 * j], skip[2 * j + 1])
        cols = slice(128 * j, 128 * j + 128)
        pieces.append(
            (jnp.where(low_half, even, odd) + gain * conv[:, cols]) * gate[:, cols]
        )
    groups = [jnp.concatenate(pieces[2 * g : 2 * g + 2], axis=1) for g in range(2)]
    inner = jnp.concatenate([rms(g) for g in groups], axis=1) * inner_gain[...]
    carry[0:ROWS, INNER : INNER + 512] = inner
    out_parts[2].start()
    for part in out_parts:
        part.wait()
    for t in range(CHUNKS):
        store_state(t).wait()


def run_mixer(*given):
    hbm = pl.BlockSpec(memory_space=pltpu.HBM)
    lanes = lambda: VMEM((256, 128), F32)
    held = [
        (pltpu.SMEM if 5 <= n < 8 else VMEM)(v.shape, v.dtype)
        for n, v in enumerate(given[:18])
    ]
    return pl.pallas_call(
        mixer_kernel,
        out_shape=(
            jax.ShapeDtypeStruct((256, 4096), F32),
            jax.ShapeDtypeStruct((ROWS + 8, CARRY), F32),
        ),
        in_specs=[hbm] * 19,
        out_specs=(hbm, hbm),
        scratch_shapes=[
            *held,
            VMEM((CHUNKS, 256, CHUNK), F32),
            VMEM((CHUNKS, 256, CHUNK), F32),
            lanes(),
            lanes(),
            lanes(),
            VMEM((256, 128), BF16),
            VMEM((256, 128), BF16),
            lanes(),
            lanes(),
            VMEM((192, 128), F32),
            VMEM((ROWS + 8, CARRY), F32),
            pltpu.SemaphoreType.DMA((18,)),
            pltpu.SemaphoreType.DMA((2 * CHUNKS,)),
            pltpu.SemaphoreType.DMA((3,)),
        ],
        compiler_params=pltpu.CompilerParams(vmem_limit_bytes=67043328),
        name="mixer",
    )(*given)


def ffn_kernel(
    carry_hbm,
    ow_hbm,
    eg_hbm,
    eu_hbm,
    ed_hbm,
    dg_hbm,
    du_hbm,
    dd_hbm,
    out,
    x0,
    x1,
    x2,
    y0,
    y1,
    y2,
    s0,
    s1,
    s2,
    *rest,
):
    landed, rest = rest[:12], rest[12:]
    landing = [landed[3 * k : 3 * k + 3] for k in range(4)]
    (
    other_partial,
    wide,
    mid,
    eg,
    eu,
    ed,
    ed_other,
    dgu,
    dgu_other,
    dd,
    dd_scaled,
    packed,
    slot_weight,
    act,
    act_other,
    left_side,
    result,
    local_sem,
    ag_send,
    ag_recv,
    dd_send,
    dd_recv,
    rs_send,
    rs_recv,
    mi_send,
    mi_recv,
        carry,
        out_w,
        partial,
        small_sem,
    ) = rest
    ep = lax.axis_index("ep")
    core = lax.axis_index("tp")
    coords = (ep // 16, (ep // 4) % 4, ep % 4)
    other = 1 - core
    own_cols = pl.multiple_of(core * HALF, HALF)
    other_cols = pl.multiple_of(other * HALF, HALF)
    expert = ep // 8
    mine = (x0, x1, x2)
    theirs = (y0, y1, y2)
    sums = (s0, s1, s2)

    def neighbour(dim, shift):
        moved = list(coords)
        moved[dim] = lax.rem(coords[dim] + shift, 4)
        return (moved[0] * 16 + moved[1] * 4 + moved[2], core)

    partner = (ep, other)

    small = [
        pltpu.make_async_copy(carry_hbm, carry, small_sem.at[0]),
        pltpu.make_async_copy(ow_hbm, out_w, small_sem.at[1]),
    ]
    for load in small:
        load.start()
    barrier = pltpu.get_barrier_semaphore()
    for dim in range(3):
        for shift in (1, 2, 3):
            pl.semaphore_signal(
                barrier, inc=1, device_id=neighbour(dim, shift), device_id_type=MESH
            )
    pl.semaphore_signal(barrier, inc=1, device_id=partner, device_id_type=MESH)
    for load in small:
        load.wait()
    inner = carry[0:ROWS, INNER : INNER + 512].astype(BF16)
    partial[...] = dot(inner, out_w[...]).astype(BF16)
    pl.semaphore_wait(barrier, 10)

    def to_partner(src, dst, n):
        return pltpu.make_async_remote_copy(
            src_ref=src,
            dst_ref=dst,
            send_sem=mi_send.at[n],
            recv_sem=mi_recv.at[n],
            device_id=partner,
            device_id_type=MESH,
        )

    swap_partial = to_partner(partial, other_partial, 0)
    swap_partial.start()
    loads = [
        pltpu.make_async_copy(eg_hbm, eg.at[pl.ds(0, HIDDEN)], local_sem.at[0]),
        pltpu.make_async_copy(eu_hbm, eu.at[pl.ds(0, HIDDEN)], local_sem.at[1]),
        pltpu.make_async_copy(
            ed_hbm.at[:, pl.ds(own_cols, HALF)], ed.at[pl.ds(0, HIDDEN)], local_sem.at[2]
        ),
        pltpu.make_async_copy(dg_hbm, dgu.at[pl.ds(0, DENSE)], local_sem.at[3]),
        pltpu.make_async_copy(du_hbm, dgu.at[pl.ds(128, DENSE)], local_sem.at[4]),
        pltpu.make_async_copy(dd_hbm, dd, local_sem.at[5]),
    ]
    for load in loads:
        load.start()

    swap_partial.wait()
    mixed = partial[...].astype(F32) + other_partial[...].astype(F32)
    hidden = carry[0:ROWS, 0:WIDTH] + mixed
    mid[...] = hidden
    wide[...] = (rms(hidden) * carry[ROWS : ROWS + 1, 0:WIDTH]).astype(BF16)
    here = coords
    for p in range(3):
        cols = pl.ds(pl.multiple_of(own_cols + STARTS[p], 128), WIDTHS[p])
        mine[p][here[0], here[1], here[2], 0:ROWS, :] = wide[:, cols]
    x2[here[0], here[1], here[2], ROWS : ROWS + 16, :] = carry[0:16, META : META + 256].astype(
        BF16
    )

    def cut(buf, p, where, half=None, rows=None):
        index = [None, None, None]
        for q in range(3):
            index[ORDERS[p][q]] = pl.ds(0, 4) if where[q] is None else where[q]
        if half is not None:
            free = sorted(ORDERS[p][q] for q in range(3) if where[q] is None)
            if free:
                index[free[0]] = pl.ds(2 * half, 2)
            else:
                rows = pl.ds(0, 16) if half == 0 else pl.ds(16, rows - 16)
        elif rows is not None:
            rows = pl.ds(0, rows)
        if rows is not None and not (half is not None and free):
            index.append(rows)
        return buf.at[tuple(index)]

    def turn(p, k, shift):
        return lax.rem(coords[ORDERS[p][k]] + shift, 4)

    ME, RIGHT, FAR, LEFT = 0, 1, 2, 3
    spots = [[[turn(p, k, shift) for shift in range(4)] for k in range(3)] for p in range(3)]

    class Ring:
        def __init__(self, p, k, at, place, direct=False):
            self.p, self.k, self.place, self.direct = p, k, place, direct
            self.copies = [self.copy(at, ME, None, 1), self.copy(at + 1, ME, None, 3)]
            if direct:
                self.copies.append(self.copy(at + 2, ME, None, 2))
            else:
                self.copies.append(self.copy(at + 2, LEFT, 0, 1))
                self.copies.append(self.copy(at + 3, RIGHT, 1, 3))

        def copy(self, at, shift, half, to):
            p = self.p
            where = list(self.place)
            where[self.k] = spots[p][self.k][shift]
            rows = BLOCK_ROWS[p] if half is not None else None
            ref = cut(mine[p], p, where, half, rows)
            return pltpu.make_async_remote_copy(
                src_ref=ref,
                dst_ref=ref,
                send_sem=ag_send.at[at],
                recv_sem=ag_recv.at[at],
                device_id=neighbour(ORDERS[p][self.k], to),
                device_id_type=MESH,
            )

        def start(self):
            if self.direct:
                self.copies[2].start()
            self.copies[0].start()
            self.copies[1].start()

        def on(self):
            self.copies[0].wait_recv()
            if not self.direct:
                self.copies[2].start()
            self.copies[1].wait_recv()
            if not self.direct:
                self.copies[3].start()

        def end(self):
            for copy in self.copies[2:]:
                copy.wait_recv()

    first, second, third_way = [], [], []
    for p in range(3):
        at = 84 * p
        own = [spots[p][k][ME] for k in range(3)]
        first.append(Ring(p, 0, at, own, True))
        second.append(
            [Ring(p, 1, at + 4 + 4 * u, [spots[p][0][u], None, own[2]], True) for u in range(4)]
        )
        third_way.append(
            [
                [
                    Ring(
                        p,
                        2,
                        at + 20 + 16 * u + 4 * v,
                        [spots[p][0][u], spots[p][1][v], None],
                        FAR in (u, v) and ME not in (u, v),
                    )
                    for v in range(4)
                ]
                for u in range(4)
            ]
        )
    rings = [first] + second + [row for part in third_way for row in part]
    hand_overs = []

    def hand_over(p, n, second_at, third_at):
        where = [None, second_at, third_at]
        copy = pltpu.make_async_remote_copy(
            src_ref=cut(mine[p], p, where, None, ROWS),
            dst_ref=cut(theirs[p], p, where, None, ROWS),
            send_sem=dd_send.at[13 * p + n],
            recv_sem=dd_recv.at[13 * p + n],
            device_id=partner,
            device_id_type=MESH,
        )
        copy.start()
        hand_overs.append(copy)

    parts = range(3)
    def launch(*pairs):
        for p in parts:
            for u, v in pairs:
                third_way[p][u][v].start()

    def pass_on(*pairs):
        for p in parts:
            for u, v in pairs:
                third_way[p][u][v].on()

    for p in parts:
        first[p].start()
    for p in parts:
        second[p][ME].start()
    launch((ME, ME))

    early = [
        to_partner(
            ed_hbm.at[:, pl.ds(other_cols, HALF)], ed_other.at[pl.ds(0, HIDDEN)], 1
        ),
        to_partner(dg_hbm, dgu_other.at[pl.ds(0, DENSE)], 2),
        to_partner(du_hbm, dgu_other.at[pl.ds(128, DENSE)], 3),
    ]
    for copy in early:
        copy.start()

    for p in parts:
        first[p].on()
        for u in (LEFT, RIGHT):
            second[p][u].start()
            third_way[p][u][ME].start()
    for p in parts:
        second[p][ME].on()
    launch((ME, RIGHT), (ME, LEFT))
    for p in parts:
        first[p].end()
        second[p][FAR].start()
        third_way[p][FAR][ME].start()
    for p in parts:
        second[p][ME].end()
    launch((ME, FAR))
    pass_on((ME, ME))
    for ref in (eg, eu, ed, ed_other):
        ref[HIDDEN:HPAD, :] = jnp.zeros((HPAD - HIDDEN, ref.shape[1]), BF16)
    for ref in (dgu, dgu_other):
        ref[DENSE:128, :] = jnp.zeros((128 - DENSE, HALF), BF16)
        ref[128 + DENSE : 256, :] = jnp.zeros((128 - DENSE, HALF), BF16)
    dd_scaled[DENSE:128, :] = jnp.zeros((128 - DENSE, HALF), BF16)
    for g in range(GROUPS):
        result[g, SLOTS:128, :] = jnp.zeros((128 - SLOTS, HALF), BF16)
    for p in parts:
        second[p][LEFT].on()
        second[p][RIGHT].on()
    launch((LEFT, RIGHT), (RIGHT, RIGHT), (LEFT, LEFT), (RIGHT, LEFT))
    pass_on((LEFT, ME), (RIGHT, ME), (ME, RIGHT), (ME, LEFT))
    for p in parts:
        second[p][LEFT].end()
        second[p][RIGHT].end()
    launch((LEFT, FAR), (RIGHT, FAR))
    for p in parts:
        second[p][FAR].on()
    launch((FAR, RIGHT), (FAR, LEFT))
    for p in parts:
        second[p][FAR].end()
    launch((FAR, FAR))
    pass_on((FAR, ME), (ME, FAR))
    for p in parts:
        hand_over(p, 0, None, spots[p][2][ME])
        hand_over(p, 1, spots[p][1][ME], spots[p][2][LEFT])
        hand_over(p, 2, spots[p][1][ME], spots[p][2][RIGHT])

    def finish(v, n):
        for p in parts:
            for u in range(4):
                third_way[p][u][v].end()
            hand_over(p, n, spots[p][1][v], spots[p][2][FAR])

    def sides(v, n):
        for p in parts:
            hand_over(p, n, spots[p][1][v], spots[p][2][LEFT])
            hand_over(p, n + 1, spots[p][1][v], spots[p][2][RIGHT])

    pass_on((LEFT, RIGHT), (RIGHT, RIGHT), (LEFT, LEFT), (RIGHT, LEFT))
    finish(ME, 3)
    pass_on((LEFT, FAR), (RIGHT, FAR), (FAR, RIGHT), (FAR, LEFT))
    sides(RIGHT, 4)
    sides(LEFT, 6)
    pass_on((FAR, FAR))
    sides(FAR, 8)
    finish(RIGHT, 10)
    finish(LEFT, 11)
    finish(FAR, 12)
    pick_row = lax.broadcasted_iota(jnp.int32, (128, 128), 0)
    pick_rank = (pick_row == expert).astype(F32).astype(BF16)
    pick_weight = (
        jnp.logical_or(pick_row == expert + 8, pick_row == expert + 16)
    ).astype(F32).astype(BF16)
    lane = lax.broadcasted_iota(jnp.int32, (GROUP_ROWS, 128), 1)
    source = lax.broadcasted_iota(jnp.int32, (GROUP_ROWS, 128), 0) // ROWS

    def group_of(bufs, g):
        z, y = g // 2, 2 * lax.rem(g, 2)
        return jnp.concatenate(
            [
                bufs[p][z, pl.ds(y, 2), :, 0:ROWS, :].reshape(GROUP_ROWS, WIDTHS[p])
                for p in range(3)
            ],
            axis=1,
        )

    def pack_group(g, carry):
        z, y = g // 2, 2 * lax.rem(g, 2)
        tags = x2[z, pl.ds(y, 2), :, ROWS : ROWS + 16, :].reshape(8, 16, 256)
        tags = jnp.concatenate([tags[:, :, 0:128], tags[:, :, 128:256]], axis=1)
        tags = tags.reshape(GROUP_ROWS, 128)
        rank = dot(tags, pick_rank).astype(jnp.int32)
        hit = jnp.logical_and(rank > 0, rank + (CAP * source - 1) == lane)
        table = hit.astype(F32).astype(BF16)
        left_side[g, :, 0:128] = table
        used = table[:, 0:SLOTS]
        slots = pl.ds(pl.multiple_of(g * SLOTS, SLOTS), SLOTS)
        packed[slots, pl.ds(own_cols, HALF)] = dot_tn(used, group_of(mine, g)).astype(BF16)
        slot_tags = dot_tn(used, tags).astype(BF16)
        slot_weight[slots, :] = dot(slot_tags, pick_weight)
        return carry

    lax.fori_loop(0, GROUPS, pack_group, 0, unroll=8)
    for load in loads:
        load.wait()
    for copy in early:
        copy.wait()
    for group in rings:
        for ring in group:
            for copy in ring.copies:
                copy.wait_send()
    for copy in hand_overs:
        copy.wait()

    def pack_other(g, carry):
        used = left_side[g, :, 0:SLOTS]
        slots = pl.ds(pl.multiple_of(g * SLOTS, SLOTS), SLOTS)
        packed[slots, pl.ds(other_cols, HALF)] = dot_tn(used, group_of(theirs, g)).astype(
            BF16
        )
        return carry

    lax.fori_loop(0, GROUPS, pack_other, 0, unroll=8)

    sends = []
    for i in range(2):
        units = pl.ds(256 * i, 256)
        gate = dot_nt(packed[...], eg[units, :])
        up = dot_nt(packed[...], eu[units, :])
        act[:, units] = (silu(gate) * up * slot_weight[:, 0:1]).astype(BF16)
        copy = to_partner(act.at[:, units], act_other.at[:, units], 4 + i)
        copy.start()
        sends.append(copy)

    def dense_group(g, carry):
        both = dot_nt(group_of(mine, g), dgu[...]) + dot_nt(group_of(theirs, g), dgu_other[...])
        left_side[g, :, 128:256] = (silu(both[:, 0:128]) * both[:, 128:256]).astype(BF16)
        return carry

    lax.fori_loop(0, GROUPS, dense_group, 0, unroll=8)
    share = 1.0 / (1.0 + jnp.exp(-carry[ROWS + 1 : ROWS + 2, 0:HALF]))
    dd_scaled[0:DENSE, :] = (dd[...].astype(F32) * share).astype(BF16)

    class Back:
        def __init__(self, p, k, at, place, slot):
            self.p, self.k, self.place, self.slot = p, k, place, slot
            self.halves, self.wholes = landing[0][p], landing[1][p]
            self.copies = [
                self.copy(at, FAR, 0, 1, self.halves.at[slot, 0]),
                self.copy(at + 1, FAR, 1, 3, self.halves.at[slot, 1]),
                self.copy(at + 2, RIGHT, None, 1, self.wholes.at[slot, 0]),
                self.copy(at + 3, LEFT, None, 3, self.wholes.at[slot, 1]),
            ]

        def spot(self, shift):
            where = list(self.place)
            where[self.k] = spots[self.p][self.k][shift]
            return where

        def copy(self, at, shift, half, to, target):
            p = self.p
            rows = ROWS if half is not None else None
            return pltpu.make_async_remote_copy(
                src_ref=cut(sums[p], p, self.spot(shift), half, rows),
                dst_ref=target,
                send_sem=rs_send.at[at],
                recv_sem=rs_recv.at[at],
                device_id=neighbour(ORDERS[p][self.k], to),
                device_id_type=MESH,
            )

        def start(self):
            self.copies[0].start()
            self.copies[1].start()

        def add_half(self, shift, half):
            p, got = self.p, self.halves
            where = self.spot(shift)
            place = [None, None, None]
            for q in range(3):
                place[ORDERS[p][q]] = where[q]
            free = [d for d in range(3) if place[d] is None]
            for t in range(2):
                place[free[0]] = 2 * half + t
                ref = sums[p].at[tuple(place)]
                ref[...] = ref[...] + got[self.slot, half, t]

        def on(self):
            self.copies[0].wait_recv()
            self.add_half(RIGHT, 0)
            self.copies[2].start()
            self.copies[1].wait_recv()
            self.add_half(LEFT, 1)
            self.copies[3].start()

        def end(self):
            p, got = self.p, self.wholes
            self.copies[2].wait_recv()
            self.copies[3].wait_recv()
            where = self.spot(ME)
            place = [None, None, None]
            for q in range(3):
                place[ORDERS[p][q]] = where[q]
            free = [d for d in range(3) if place[d] is None]
            for t in range(4):
                place[free[0]] = t
                ref = sums[p].at[tuple(place)]
                total = ref[...].astype(F32) + got[self.slot, 0, t].astype(F32)
                ref[...] = (total + got[self.slot, 1, t].astype(F32)).astype(BF16)

    class Straight:
        def __init__(self, p, k, at, place):
            self.p, self.k, self.place, self.wholes = p, k, place, landing[2 + k][p]
            self.copies = [self.copy(at + u - 1, u) for u in (RIGHT, FAR, LEFT)]

        def copy(self, at, u):
            p = self.p
            where = list(self.place)
            where[self.k] = spots[p][self.k][u]
            return pltpu.make_async_remote_copy(
                src_ref=cut(sums[p], p, where),
                dst_ref=self.wholes.at[u - 1],
                send_sem=rs_send.at[at],
                recv_sem=rs_recv.at[at],
                device_id=neighbour(ORDERS[p][self.k], u),
                device_id_type=MESH,
            )

        def send(self, u):
            self.copies[u - 1].start()

        def arrive(self):
            for copy in self.copies:
                copy.wait_recv()

        def add(self, first_at):
            p, got = self.p, self.wholes
            place = [None, None, None]
            for q in range(3):
                place[ORDERS[p][q]] = spots[p][q][ME]
            place[ORDERS[p][0]] = first_at
            ref = sums[p].at[tuple(place)]
            total = ref[...].astype(F32)
            for n in range(3):
                total = total + got[n, first_at].astype(F32)
            ref[...] = total.astype(BF16)

    third, middle, last = [], [], []
    for p in parts:
        at = 24 * p
        own = [spots[p][k][ME] for k in range(3)]
        third.append(
            [Back(p, 2, at + 4 * u, [None, spots[p][1][u], None], u) for u in range(4)]
        )
        middle.append(Straight(p, 1, at + 16, [None, None, own[2]]))
        last.append(Straight(p, 0, at + 20, own))
    order = (FAR, LEFT, RIGHT, ME)
    for send in sends:
        send.wait()
    for p in parts:
        cols = slice(STARTS[p], STARTS[p] + WIDTHS[p])
        for n in ((0, 1), (2,), (3,))[p]:
            some = slice(256 * n, 256 * n + 256)
            back = dot(act[...], ed[:, some]) + dot(act_other[...], ed_other[:, some])
            result[:, 0:SLOTS, some] = back.astype(BF16).reshape(GROUPS, SLOTS, 256)

        def spread_group(g, carry):
            z, y = g // 2, 2 * lax.rem(g, 2)
            right_side = jnp.concatenate([result[g, :, cols], dd_scaled[:, cols]], axis=0)
            total = dot(left_side[g], right_side).astype(BF16)
            sums[p][z, pl.ds(y, 2)] = total.reshape(2, 4, ROWS, WIDTHS[p])
            return carry

        lax.fori_loop(0, GROUPS, spread_group, 0, unroll=8)
        for u in order:
            third[p][u].start()
    for u in order:
        for p in parts:
            third[p][u].on()
    for u in order:
        for p in parts:
            third[p][u].end()
            if u != ME:
                middle[p].send(u)
    for p in parts:
        middle[p].arrive()
        for u in order:
            middle[p].add(spots[p][0][u])
            if u != ME:
                last[p].send(u)
    for p in parts:
        last[p].arrive()
        got = last[p].wholes
        total = mid[:, pl.ds(pl.multiple_of(own_cols + STARTS[p], 128), WIDTHS[p])]
        total = total + sums[p][here[0], here[1], here[2]].astype(F32)
        for n in range(3):
            total = total + got[n].astype(F32)
        out[:, STARTS[p] : STARTS[p] + WIDTHS[p]] = total.astype(BF16)
    for group in third + [middle, last]:
        for back in group:
            for copy in back.copies:
                copy.wait_send()


def run_ffn(carry, out_w, eg, eu, ed, dg, du, dd):
    vmem = pl.BlockSpec(memory_space=VMEM)
    hbm = pl.BlockSpec(memory_space=pltpu.HBM)
    blocks = lambda *lead: [VMEM((*lead, WIDTHS[p]), BF16) for p in range(3)]
    sem = pltpu.SemaphoreType.DMA
    return pl.pallas_call(
        ffn_kernel,
        out_shape=jax.ShapeDtypeStruct((ROWS, HALF), BF16),
        in_specs=[hbm] * 8,
        out_specs=vmem,
        scratch_shapes=[
            *[VMEM((4, 4, 4, BLOCK_ROWS[p], WIDTHS[p]), BF16) for p in range(3)],
            *blocks(4, 4, 4, ROWS),
            *blocks(4, 4, 4, ROWS),
            *blocks(4, 2, 2, ROWS),
            *blocks(4, 2, 4, ROWS),
            *blocks(3, ROWS),
            *blocks(3, 4, ROWS),
            VMEM((ROWS, 2 * HALF), BF16),
            VMEM((ROWS, 2 * HALF), BF16),
            VMEM((ROWS, 2 * HALF), F32),
            VMEM((HPAD, 2 * HALF), BF16),
            VMEM((HPAD, 2 * HALF), BF16),
            VMEM((HPAD, HALF), BF16),
            VMEM((HPAD, HALF), BF16),
            VMEM((256, HALF), BF16),
            VMEM((256, HALF), BF16),
            VMEM((DENSE, HALF), BF16),
            VMEM((128, HALF), BF16),
            VMEM((GROUPS * SLOTS, 2 * HALF), BF16),
            VMEM((GROUPS * SLOTS, 128), F32),
            VMEM((GROUPS * SLOTS, HPAD), BF16),
            VMEM((GROUPS * SLOTS, HPAD), BF16),
            VMEM((GROUPS, GROUP_ROWS, 256), BF16),
            VMEM((GROUPS, 128, HALF), BF16),
            sem((6,)),
            sem((252,)),
            sem((252,)),
            sem((39,)),
            sem((39,)),
            sem((72,)),
            sem((72,)),
            sem((6,)),
            sem((6,)),
            VMEM((ROWS + 8, CARRY), F32),
            VMEM((512, 2 * HALF), BF16),
            VMEM((ROWS, 2 * HALF), BF16),
            sem((2,)),
        ],
        compiler_params=pltpu.CompilerParams(
            collective_id=0, has_side_effects=True, vmem_limit_bytes=67043328
        ),
        name="ffn",
    )(carry, out_w, eg, eu, ed, dg, du, dd)


def local(
    stream,
    mixer_gain,
    gate_proj,
    input_proj,
    state_maps,
    step_proj,
    step_bias,
    decay_rate,
    input_taps,
    map_taps,
    input_past,
    map_past,
    head_state,
    skip_gain,
    inner_gain,
    mixer_out,
    channel_gain,
    expert_ids,
    expert_weight,
    expert_gate,
    expert_up,
    expert_down,
    dense_gate,
    dense_up,
    dense_down,
    dense_mix,
):
    state_out, carry = run_mixer(
        stream,
        mixer_gain.reshape(1, -1),
        step_proj.T,
        expert_ids.T,
        expert_weight.T,
        step_bias,
        decay_rate,
        skip_gain,
        input_proj,
        input_taps,
        jnp.transpose(input_past, (1, 0, 2)),
        state_maps,
        map_taps,
        jnp.transpose(map_past, (0, 2, 1, 3)).reshape(192, 128),
        inner_gain.reshape(1, -1),
        gate_proj,
        channel_gain.reshape(1, -1),
        dense_mix.reshape(1, -1),
        head_state.reshape(256, 4096),
    )
    out = run_ffn(
        carry,
        mixer_out,
        expert_gate.T,
        expert_up.T,
        expert_down,
        dense_gate.T,
        dense_up.T,
        dense_down,
    )
    return out, state_out.reshape(head_state.shape)


def solution(mesh):
    placed = (
        P("ep", None),
        P(),
        P(None, "tp"),
        P(None, "tp"),
        P(None, None, "tp"),
        P(None, "tp"),
        P("tp"),
        P("tp"),
        P(None, "tp"),
        P(None, None, "tp"),
        P("ep", None, "tp"),
        P("ep", None, None, "tp"),
        P("ep", "tp", None),
        P("tp"),
        P("tp"),
        P("tp", None),
        P(),
        P("ep", None),
        P("ep", None),
        P(None, ("ep", "tp")),
        P(None, ("ep", "tp")),
        P(("ep", "tp"), None),
        P("tp", "ep"),
        P("tp", "ep"),
        P("ep", "tp"),
        P("tp"),
    )
    return jax.shard_map(
        local,
        mesh=mesh,
        in_specs=placed,
        out_specs=(P("ep", "tp"), P("ep", "tp", None)),
        check_vma=False,
    )
```

```python
import functools

import jax
import jax.numpy as jnp
from jax import lax
from jax.experimental import pallas as pl
from jax.experimental.pallas import tpu as pltpu
from jax.sharding import PartitionSpec as P

EPS = 1e-06
MESH = pl.DeviceIdType.MESH
F32 = jnp.float32
BF16 = jnp.bfloat16
VMEM = pltpu.VMEM
ANY = pl.ANY

HEADS = 8
ROWS = 32
EXPERTS = 8
CAP = 12
CHUNKS = 8
CHUNK = 512
GROUPS = 8
GROUP_ROWS = 256
SLOTS = 96
HALF = 1024
HIDDEN = 448
HPAD = 512
DENSE = 88
WIDTH = 2048
META = 2048
CARRY = 2304

WIDTHS = (384, 384, 256)
STARTS = (0, 384, 768)
BLOCK_ROWS = (32, 32, 48)
ORDERS = ((2, 1, 0), (1, 0, 2), (0, 2, 1))


def dot(a, b):
    return jnp.dot(a, b, preferred_element_type=F32)


def dot_nt(a, b):
    return lax.dot_general(a, b, (((1,), (1,)), ((), ())), preferred_element_type=F32)


def dot_tn(a, b):
    return lax.dot_general(a, b, (((0,), (0,)), ((), ())), preferred_element_type=F32)


def silu(v):
    return v / (1.0 + jnp.exp(-v))


def rms(v):
    return v * lax.rsqrt(jnp.mean(v * v, axis=-1, keepdims=True) + EPS)


def split(v):
    high = v.astype(BF16)
    return high, (v - high.astype(F32)).astype(BF16)


def mixer_kernel(*refs):
    given, refs = refs[:20], refs[20:]
    state_hbm = given[19]
    state_out, carry_hbm, partial_hbm = refs[:3]
    held, refs = refs[3:22], refs[22:]
    (
        stream,
        mixer_gain,
        step_t,
        ids,
        weights,
        bias,
        decay,
        skip,
        input_w,
        input_taps,
        input_past,
        maps_w,
        map_taps,
        map_past,
        inner_gain,
        gate_w,
        channel_gain,
        mix,
        out_w,
    ) = held
    old, new, dec, write, read, xs, tmp, y, past, carry, partial, in_sems, sems, out_sems = refs
    loads = [
        pltpu.make_async_copy(src, dst, in_sems.at[n])
        for n, (src, dst) in enumerate(zip(given, held))
    ]

    def load_state(t):
        cols = pl.ds(pl.multiple_of(t * CHUNK, CHUNK), CHUNK)
        return pltpu.make_async_copy(state_hbm.at[:, cols], old.at[t], sems.at[t])

    def store_state(t):
        cols = pl.ds(pl.multiple_of(t * CHUNK, CHUNK), CHUNK)
        return pltpu.make_async_copy(
            new.at[t], state_out.at[:, cols], sems.at[CHUNKS + t]
        )

    for load in loads[:15]:
        load.start()
    for t in range(CHUNKS):
        load_state(t).start()
    for load in loads[15:]:
        load.start()

    for load in loads[:8]:
        load.wait()
    normed = (rms(stream[...].astype(F32)) * mixer_gain[...]).astype(BF16)
    steps = dot_nt(normed, step_t[...])

    expert_of = lax.broadcasted_iota(jnp.int32, (EXPERTS, ROWS), 0)
    hit0 = (ids[0:1, :] == expert_of).astype(F32)
    hit1 = (ids[1:2, :] == expert_of).astype(F32)
    member = hit0 + hit1
    upper = (
        lax.broadcasted_iota(jnp.int32, (ROWS, ROWS), 0)
        <= lax.broadcasted_iota(jnp.int32, (ROWS, ROWS), 1)
    ).astype(BF16)
    rank = dot(member.astype(BF16), upper) * member
    weight = hit0 * weights[0:1, :] + hit1 * weights[1:2, :]
    w_high = weight.astype(BF16).astype(F32)
    w_low = weight - w_high
    table = jnp.concatenate(
        [rank, w_high, w_low, jnp.zeros((104, ROWS), F32)], axis=0
    ).astype(BF16)
    eye = (
        lax.broadcasted_iota(jnp.int32, (ROWS, ROWS), 0)
        == lax.broadcasted_iota(jnp.int32, (ROWS, ROWS), 1)
    ).astype(BF16)
    by_row = dot_nt(eye, table)
    carry[0:16, META : META + 256] = jnp.concatenate([by_row[0:16], by_row[16:32]], axis=1)
    carry[0:ROWS, 0:WIDTH] = stream[...].astype(F32)

    for load in loads[8:11]:
        load.wait()
    newest = dot(normed, input_w[...]).astype(BF16).astype(F32)
    conv = newest * input_taps[3:4, :]
    for t in range(3):
        conv = conv + input_past[t].astype(F32) * input_taps[t : t + 1, :]
    conv = silu(conv)

    for load in loads[11:14]:
        load.wait()
    past[...] = map_past[...].astype(F32)
    conv_maps = []
    for m in range(2):
        new_map = dot(normed, maps_w[m]).astype(BF16).astype(F32)
        acc = new_map * map_taps[m, 3:4, :]
        for t in range(3):
            acc = acc + past[pl.ds(2 * t + m, ROWS, stride=6), :] * map_taps[m, t : t + 1, :]
        conv_maps.append(silu(acc))

    lane = lax.broadcasted_iota(jnp.int32, (ROWS, 128), 1)
    low_half = lane < 64

    def both_halves(v):
        turned = pltpu.roll(v, 64, 1)
        return jnp.where(low_half, v, turned), jnp.where(low_half, turned, v)

    write_by_group = both_halves(conv_maps[0])
    read_by_group = both_halves(conv_maps[1])
    for h in range(HEADS):
        rows = pl.ds(h, ROWS, stride=HEADS)
        v = jnp.broadcast_to(steps[:, h : h + 1], (ROWS, 128)) + bias[h]
        step = jnp.maximum(v, 0.0) + jnp.log1p(jnp.exp(-jnp.abs(v)))
        dec[rows, :] = jnp.exp(-decay[h] * step)
        pair = conv[:, 128 * (h // 2) : 128 * (h // 2) + 128]
        mine = low_half if h % 2 == 0 else jnp.logical_not(low_half)
        tmp[rows, :] = jnp.where(mine, step * pair, 0.0)
        write[rows, :] = write_by_group[h // 4]
        read[rows, :] = read_by_group[h // 4]
    high, low = split(tmp[...])
    xs[:, 0:128] = high
    xs[:, 128:256] = low
    y[...] = jnp.zeros_like(y)

    slot = lax.broadcasted_iota(jnp.int32, (256, CHUNK), 0) % 64
    place = lax.broadcasted_iota(jnp.int32, (256, CHUNK), 1) // 64

    def chunk_step(t, carry):
        spread = (slot == place + 8 * t).astype(F32).astype(BF16)
        load_state(t).wait()
        values = dot(xs[...], spread)
        wide = lambda ref: jnp.concatenate([ref[...]] * (CHUNK // 128), axis=1)
        fresh = wide(dec) * old[t] + values * wide(write)
        new[t] = fresh
        store_state(t).start()
        both = dot_nt(jnp.concatenate(split(fresh * wide(read)), axis=0), spread[0:128])
        y[...] += both[0:256] + both[256:512]
        return carry

    lax.fori_loop(0, CHUNKS, chunk_step, 0, unroll=4)

    for load in loads[14:18]:
        load.wait()
    carry[ROWS : ROWS + 1, 0:WIDTH] = channel_gain[...]
    carry[ROWS + 1 : ROWS + 2, 0:HALF] = mix[...]
    out_parts = []
    for n, (first, size) in enumerate(((0, WIDTH), (META, 256))):
        where = (pl.ds(0, ROWS + 8), pl.ds(first, size))
        out_parts.append(
            pltpu.make_async_copy(carry.at[where], carry_hbm.at[where], out_sems.at[n])
        )
    out_parts[0].start()
    out_parts[1].start()
    gate = silu(dot(normed, gate_w[...]).astype(BF16).astype(F32))
    pieces = []
    for j in range(HEADS // 2):
        even = y[pl.ds(2 * j, ROWS, stride=HEADS), :]
        odd = y[pl.ds(2 * j + 1, ROWS, stride=HEADS), :]
        gain = jnp.where(low_half, skip[2 * j], skip[2 * j + 1])
        cols = slice(128 * j, 128 * j + 128)
        pieces.append(
            (jnp.where(low_half, even, odd) + gain * conv[:, cols]) * gate[:, cols]
        )
    groups = [jnp.concatenate(pieces[2 * g : 2 * g + 2], axis=1) for g in range(2)]
    inner = jnp.concatenate([rms(g) for g in groups], axis=1) * inner_gain[...]
    loads[18].wait()
    partial[...] = dot(inner.astype(BF16), out_w[...]).astype(BF16)
    out_parts.append(pltpu.make_async_copy(partial, partial_hbm, out_sems.at[2]))
    out_parts[2].start()
    for part in out_parts:
        part.wait()
    for t in range(CHUNKS):
        store_state(t).wait()


def run_mixer(*given):
    hbm = pl.BlockSpec(memory_space=pltpu.HBM)
    lanes = lambda: VMEM((256, 128), F32)
    held = [
        (pltpu.SMEM if 5 <= n < 8 else VMEM)(v.shape, v.dtype)
        for n, v in enumerate(given[:19])
    ]
    return pl.pallas_call(
        mixer_kernel,
        out_shape=(
            jax.ShapeDtypeStruct((256, 4096), F32),
            jax.ShapeDtypeStruct((ROWS + 8, CARRY), F32),
            jax.ShapeDtypeStruct((ROWS, 2 * HALF), BF16),
        ),
        in_specs=[hbm] * 20,
        out_specs=(hbm, hbm, hbm),
        scratch_shapes=[
            *held,
            VMEM((CHUNKS, 256, CHUNK), F32),
            VMEM((CHUNKS, 256, CHUNK), F32),
            lanes(),
            lanes(),
            lanes(),
            VMEM((256, 256), BF16),
            lanes(),
            lanes(),
            VMEM((192, 128), F32),
            VMEM((ROWS + 8, CARRY), F32),
            VMEM((ROWS, 2 * HALF), BF16),
            pltpu.SemaphoreType.DMA((19,)),
            pltpu.SemaphoreType.DMA((2 * CHUNKS,)),
            pltpu.SemaphoreType.DMA((3,)),
        ],
        compiler_params=pltpu.CompilerParams(vmem_limit_bytes=67043328),
        name="mixer",
    )(*given)


def ffn_kernel(
    carry_hbm,
    partial_hbm,
    eg_hbm,
    eu_hbm,
    ed_hbm,
    dg_hbm,
    du_hbm,
    dd_hbm,
    out,
    x0,
    x1,
    x2,
    y0,
    y1,
    y2,
    s0,
    s1,
    s2,
    *rest,
):
    landed, rest = rest[:12], rest[12:]
    landing = [landed[3 * k : 3 * k + 3] for k in range(4)]
    (
    other_partial,
    wide,
    mid,
    eg,
    eu,
    ed,
    ed_other,
    dgu,
    dgu_other,
    dd,
    dd_scaled,
    packed,
    slot_weight,
    act,
    act_other,
    left_side,
    result,
    local_sem,
    ag_send,
    ag_recv,
    dd_send,
    dd_recv,
    rs_send,
    rs_recv,
    mi_send,
    mi_recv,
        carry,
        partial,
        small_sem,
    ) = rest
    ep = lax.axis_index("ep")
    core = lax.axis_index("tp")
    coords = (ep // 16, (ep // 4) % 4, ep % 4)
    other = 1 - core
    own_cols = pl.multiple_of(core * HALF, HALF)
    other_cols = pl.multiple_of(other * HALF, HALF)
    expert = ep // 8
    mine = (x0, x1, x2)
    theirs = (y0, y1, y2)
    sums = (s0, s1, s2)

    def neighbour(dim, shift):
        moved = list(coords)
        moved[dim] = lax.rem(coords[dim] + shift, 4)
        return (moved[0] * 16 + moved[1] * 4 + moved[2], core)

    partner = (ep, other)

    small = [
        pltpu.make_async_copy(partial_hbm, partial, small_sem.at[0]),
        pltpu.make_async_copy(carry_hbm, carry, small_sem.at[1]),
    ]
    for load in small:
        load.start()
    barrier = pltpu.get_barrier_semaphore()
    for dim in range(3):
        for shift in (1, 2, 3):
            pl.semaphore_signal(
                barrier, inc=1, device_id=neighbour(dim, shift), device_id_type=MESH
            )
    pl.semaphore_signal(barrier, inc=1, device_id=partner, device_id_type=MESH)
    small[0].wait()
    pl.semaphore_wait(barrier, 10)

    def to_partner(src, dst, n):
        return pltpu.make_async_remote_copy(
            src_ref=src,
            dst_ref=dst,
            send_sem=mi_send.at[n],
            recv_sem=mi_recv.at[n],
            device_id=partner,
            device_id_type=MESH,
        )

    swap_partial = to_partner(partial, other_partial, 0)
    swap_partial.start()
    loads = [
        pltpu.make_async_copy(eg_hbm, eg.at[pl.ds(0, HIDDEN)], local_sem.at[0]),
        pltpu.make_async_copy(eu_hbm, eu.at[pl.ds(0, HIDDEN)], local_sem.at[1]),
        pltpu.make_async_copy(
            ed_hbm.at[:, pl.ds(own_cols, HALF)], ed.at[pl.ds(0, HIDDEN)], local_sem.at[2]
        ),
        pltpu.make_async_copy(dg_hbm, dgu.at[pl.ds(0, DENSE)], local_sem.at[3]),
        pltpu.make_async_copy(du_hbm, dgu.at[pl.ds(128, DENSE)], local_sem.at[4]),
        pltpu.make_async_copy(dd_hbm, dd, local_sem.at[5]),
    ]
    for load in loads:
        load.start()

    small[1].wait()
    swap_partial.wait()
    mixed = partial[...].astype(F32) + other_partial[...].astype(F32)
    hidden = carry[0:ROWS, 0:WIDTH] + mixed
    mid[...] = hidden
    wide[...] = (rms(hidden) * carry[ROWS : ROWS + 1, 0:WIDTH]).astype(BF16)
    here = coords
    for p in range(3):
        cols = pl.ds(pl.multiple_of(own_cols + STARTS[p], 128), WIDTHS[p])
        mine[p][here[0], here[1], here[2], 0:ROWS, :] = wide[:, cols]
    x2[here[0], here[1], here[2], ROWS : ROWS + 16, :] = carry[0:16, META : META + 256].astype(
        BF16
    )

    def cut(buf, p, where, half=None, rows=None):
        index = [None, None, None]
        for q in range(3):
            index[ORDERS[p][q]] = pl.ds(0, 4) if where[q] is None else where[q]
        if half is not None:
            free = sorted(ORDERS[p][q] for q in range(3) if where[q] is None)
            if free:
                index[free[0]] = pl.ds(2 * half, 2)
            else:
                rows = pl.ds(0, 16) if half == 0 else pl.ds(16, rows - 16)
        elif rows is not None:
            rows = pl.ds(0, rows)
        if rows is not None and not (half is not None and free):
            index.append(rows)
        return buf.at[tuple(index)]

    def turn(p, k, shift):
        return lax.rem(coords[ORDERS[p][k]] + shift, 4)

    ME, RIGHT, FAR, LEFT = 0, 1, 2, 3
    spots = [[[turn(p, k, shift) for shift in range(4)] for k in range(3)] for p in range(3)]

    class Ring:
        def __init__(self, p, k, at, place, direct=False):
            self.p, self.k, self.place, self.direct = p, k, place, direct
            self.copies = [self.copy(at, ME, None, 1), self.copy(at + 1, ME, None, 3)]
            if direct:
                self.copies.append(self.copy(at + 2, ME, None, 2))
            else:
                self.copies.append(self.copy(at + 2, LEFT, 0, 1))
                self.copies.append(self.copy(at + 3, RIGHT, 1, 3))

        def copy(self, at, shift, half, to):
            p = self.p
            where = list(self.place)
            where[self.k] = spots[p][self.k][shift]
            rows = BLOCK_ROWS[p] if half is not None else None
            ref = cut(mine[p], p, where, half, rows)
            return pltpu.make_async_remote_copy(
                src_ref=ref,
                dst_ref=ref,
                send_sem=ag_send.at[at],
                recv_sem=ag_recv.at[at],
                device_id=neighbour(ORDERS[p][self.k], to),
                device_id_type=MESH,
            )

        def start(self):
            if self.direct:
                self.copies[2].start()
            self.copies[0].start()
            self.copies[1].start()

        def on(self):
            self.copies[0].wait_recv()
            if not self.direct:
                self.copies[2].start()
            self.copies[1].wait_recv()
            if not self.direct:
                self.copies[3].start()

        def end(self):
            for copy in self.copies[2:]:
                copy.wait_recv()

    first, second, third_way = [], [], []
    for p in range(3):
        at = 84 * p
        own = [spots[p][k][ME] for k in range(3)]
        first.append(Ring(p, 0, at, own, True))
        second.append(
            [Ring(p, 1, at + 4 + 4 * u, [spots[p][0][u], None, own[2]], True) for u in range(4)]
        )
        third_way.append(
            [
                [
                    Ring(
                        p,
                        2,
                        at + 20 + 16 * u + 4 * v,
                        [spots[p][0][u], spots[p][1][v], None],
                        FAR in (u, v) and ME not in (u, v),
                    )
                    for v in range(4)
                ]
                for u in range(4)
            ]
        )
    rings = [first] + second + [row for part in third_way for row in part]
    hand_overs = []

    def hand_over(p, n, second_at, third_at):
        where = [None, second_at, third_at]
        copy = pltpu.make_async_remote_copy(
            src_ref=cut(mine[p], p, where, None, ROWS),
            dst_ref=cut(theirs[p], p, where, None, ROWS),
            send_sem=dd_send.at[13 * p + n],
            recv_sem=dd_recv.at[13 * p + n],
            device_id=partner,
            device_id_type=MESH,
        )
        copy.start()
        hand_overs.append(copy)

    parts = range(3)
    def launch(*pairs):
        for p in parts:
            for u, v in pairs:
                third_way[p][u][v].start()

    def pass_on(*pairs):
        for p in parts:
            for u, v in pairs:
                third_way[p][u][v].on()

    for p in parts:
        first[p].start()
    for p in parts:
        second[p][ME].start()
    launch((ME, ME))

    early = [
        to_partner(
            ed_hbm.at[:, pl.ds(other_cols, HALF)], ed_other.at[pl.ds(0, HIDDEN)], 1
        ),
        to_partner(dg_hbm, dgu_other.at[pl.ds(0, DENSE)], 2),
        to_partner(du_hbm, dgu_other.at[pl.ds(128, DENSE)], 3),
    ]
    for copy in early:
        copy.start()

    for p in parts:
        first[p].on()
        for u in (LEFT, RIGHT):
            second[p][u].start()
            third_way[p][u][ME].start()
    for p in parts:
        second[p][ME].on()
    launch((ME, RIGHT), (ME, LEFT))
    for p in parts:
        first[p].end()
        second[p][FAR].start()
        third_way[p][FAR][ME].start()
    for p in parts:
        second[p][ME].end()
    launch((ME, FAR))
    pass_on((ME, ME))
    for ref in (eg, eu, ed, ed_other):
        ref[HIDDEN:HPAD, :] = jnp.zeros((HPAD - HIDDEN, ref.shape[1]), BF16)
    for ref in (dgu, dgu_other):
        ref[DENSE:128, :] = jnp.zeros((128 - DENSE, HALF), BF16)
        ref[128 + DENSE : 256, :] = jnp.zeros((128 - DENSE, HALF), BF16)
    dd_scaled[DENSE:128, :] = jnp.zeros((128 - DENSE, HALF), BF16)
    for g in range(GROUPS):
        result[g, SLOTS:128, :] = jnp.zeros((128 - SLOTS, HALF), BF16)
    for p in parts:
        second[p][LEFT].on()
        second[p][RIGHT].on()
    launch((LEFT, RIGHT), (RIGHT, RIGHT), (LEFT, LEFT), (RIGHT, LEFT))
    pass_on((LEFT, ME), (RIGHT, ME), (ME, RIGHT), (ME, LEFT))
    for p in parts:
        second[p][LEFT].end()
        second[p][RIGHT].end()
    launch((LEFT, FAR), (RIGHT, FAR))
    for p in parts:
        second[p][FAR].on()
    launch((FAR, RIGHT), (FAR, LEFT))
    for p in parts:
        second[p][FAR].end()
    launch((FAR, FAR))
    pass_on((FAR, ME), (ME, FAR))
    for p in parts:
        hand_over(p, 0, None, spots[p][2][ME])
        hand_over(p, 1, spots[p][1][ME], spots[p][2][LEFT])
        hand_over(p, 2, spots[p][1][ME], spots[p][2][RIGHT])

    def finish(v, n):
        for p in parts:
            for u in range(4):
                third_way[p][u][v].end()
            hand_over(p, n, spots[p][1][v], spots[p][2][FAR])

    def sides(v, n):
        for p in parts:
            hand_over(p, n, spots[p][1][v], spots[p][2][LEFT])
            hand_over(p, n + 1, spots[p][1][v], spots[p][2][RIGHT])

    pass_on((LEFT, RIGHT), (RIGHT, RIGHT), (LEFT, LEFT), (RIGHT, LEFT))
    finish(ME, 3)
    pass_on((LEFT, FAR), (RIGHT, FAR), (FAR, RIGHT), (FAR, LEFT))
    sides(RIGHT, 4)
    sides(LEFT, 6)
    pass_on((FAR, FAR))
    sides(FAR, 8)
    finish(RIGHT, 10)
    finish(LEFT, 11)
    finish(FAR, 12)
    pick_row = lax.broadcasted_iota(jnp.int32, (128, 128), 0)
    pick_rank = (pick_row == expert).astype(F32).astype(BF16)
    pick_weight = (
        jnp.logical_or(pick_row == expert + 8, pick_row == expert + 16)
    ).astype(F32).astype(BF16)
    lane = lax.broadcasted_iota(jnp.int32, (GROUP_ROWS, 128), 1)
    source = lax.broadcasted_iota(jnp.int32, (GROUP_ROWS, 128), 0) // ROWS

    def group_of(bufs, g):
        z, y = g // 2, 2 * lax.rem(g, 2)
        return jnp.concatenate(
            [
                bufs[p][z, pl.ds(y, 2), :, 0:ROWS, :].reshape(GROUP_ROWS, WIDTHS[p])
                for p in range(3)
            ],
            axis=1,
        )

    def pack_group(g, carry):
        z, y = g // 2, 2 * lax.rem(g, 2)
        tags = x2[z, pl.ds(y, 2), :, ROWS : ROWS + 16, :].reshape(8, 16, 256)
        tags = jnp.concatenate([tags[:, :, 0:128], tags[:, :, 128:256]], axis=1)
        tags = tags.reshape(GROUP_ROWS, 128)
        rank = dot(tags, pick_rank).astype(jnp.int32)
        hit = jnp.logical_and(rank > 0, rank + (CAP * source - 1) == lane)
        table = hit.astype(F32).astype(BF16)
        left_side[g, :, 0:128] = table
        used = table[:, 0:SLOTS]
        slots = pl.ds(pl.multiple_of(g * SLOTS, SLOTS), SLOTS)
        packed[slots, pl.ds(own_cols, HALF)] = dot_tn(used, group_of(mine, g)).astype(BF16)
        slot_tags = dot_tn(used, tags).astype(BF16)
        slot_weight[slots, :] = dot(slot_tags, pick_weight)
        return carry

    lax.fori_loop(0, GROUPS, pack_group, 0, unroll=8)
    for load in loads:
        load.wait()
    for copy in early:
        copy.wait()
    for group in rings:
        for ring in group:
            for copy in ring.copies:
                copy.wait_send()
    for copy in hand_overs:
        copy.wait()

    def pack_other(g, carry):
        used = left_side[g, :, 0:SLOTS]
        slots = pl.ds(pl.multiple_of(g * SLOTS, SLOTS), SLOTS)
        packed[slots, pl.ds(other_cols, HALF)] = dot_tn(used, group_of(theirs, g)).astype(
            BF16
        )
        return carry

    lax.fori_loop(0, GROUPS, pack_other, 0, unroll=8)

    sends = []
    for i in range(2):
        units = pl.ds(256 * i, 256)
        gate = dot_nt(packed[...], eg[units, :])
        up = dot_nt(packed[...], eu[units, :])
        act[:, units] = (silu(gate) * up * slot_weight[:, 0:1]).astype(BF16)
        copy = to_partner(act.at[:, units], act_other.at[:, units], 4 + i)
        copy.start()
        sends.append(copy)

    def dense_group(g, carry):
        both = dot_nt(group_of(mine, g), dgu[...]) + dot_nt(group_of(theirs, g), dgu_other[...])
        left_side[g, :, 128:256] = (silu(both[:, 0:128]) * both[:, 128:256]).astype(BF16)
        return carry

    lax.fori_loop(0, GROUPS, dense_group, 0, unroll=8)
    share = 1.0 / (1.0 + jnp.exp(-carry[ROWS + 1 : ROWS + 2, 0:HALF]))
    dd_scaled[0:DENSE, :] = (dd[...].astype(F32) * share).astype(BF16)

    class Back:
        def __init__(self, p, k, at, place, slot):
            self.p, self.k, self.place, self.slot = p, k, place, slot
            self.halves, self.wholes = landing[0][p], landing[1][p]
            self.copies = [
                self.copy(at, FAR, 0, 1, self.halves.at[slot, 0]),
                self.copy(at + 1, FAR, 1, 3, self.halves.at[slot, 1]),
                self.copy(at + 2, RIGHT, None, 1, self.wholes.at[slot, 0]),
                self.copy(at + 3, LEFT, None, 3, self.wholes.at[slot, 1]),
            ]

        def spot(self, shift):
            where = list(self.place)
            where[self.k] = spots[self.p][self.k][shift]
            return where

        def copy(self, at, shift, half, to, target):
            p = self.p
            rows = ROWS if half is not None else None
            return pltpu.make_async_remote_copy(
                src_ref=cut(sums[p], p, self.spot(shift), half, rows),
                dst_ref=target,
                send_sem=rs_send.at[at],
                recv_sem=rs_recv.at[at],
                device_id=neighbour(ORDERS[p][self.k], to),
                device_id_type=MESH,
            )

        def start(self):
            self.copies[0].start()
            self.copies[1].start()

        def add_half(self, shift, half):
            p, got = self.p, self.halves
            where = self.spot(shift)
            place = [None, None, None]
            for q in range(3):
                place[ORDERS[p][q]] = where[q]
            free = [d for d in range(3) if place[d] is None]
            for t in range(2):
                place[free[0]] = 2 * half + t
                ref = sums[p].at[tuple(place)]
                ref[...] = ref[...] + got[self.slot, half, t]

        def on(self):
            self.copies[0].wait_recv()
            self.add_half(RIGHT, 0)
            self.copies[2].start()
            self.copies[1].wait_recv()
            self.add_half(LEFT, 1)
            self.copies[3].start()

        def end(self):
            p, got = self.p, self.wholes
            self.copies[2].wait_recv()
            self.copies[3].wait_recv()
            where = self.spot(ME)
            place = [None, None, None]
            for q in range(3):
                place[ORDERS[p][q]] = where[q]
            free = [d for d in range(3) if place[d] is None]
            for t in range(4):
                place[free[0]] = t
                ref = sums[p].at[tuple(place)]
                total = ref[...].astype(F32) + got[self.slot, 0, t].astype(F32)
                ref[...] = (total + got[self.slot, 1, t].astype(F32)).astype(BF16)

    class Straight:
        def __init__(self, p, k, at, place):
            self.p, self.k, self.place, self.wholes = p, k, place, landing[2 + k][p]
            self.copies = [self.copy(at + u - 1, u) for u in (RIGHT, FAR, LEFT)]

        def copy(self, at, u):
            p = self.p
            where = list(self.place)
            where[self.k] = spots[p][self.k][u]
            return pltpu.make_async_remote_copy(
                src_ref=cut(sums[p], p, where),
                dst_ref=self.wholes.at[u - 1],
                send_sem=rs_send.at[at],
                recv_sem=rs_recv.at[at],
                device_id=neighbour(ORDERS[p][self.k], u),
                device_id_type=MESH,
            )

        def send(self, u):
            self.copies[u - 1].start()

        def arrive(self):
            for copy in self.copies:
                copy.wait_recv()

        def add(self, first_at):
            p, got = self.p, self.wholes
            place = [None, None, None]
            for q in range(3):
                place[ORDERS[p][q]] = spots[p][q][ME]
            place[ORDERS[p][0]] = first_at
            ref = sums[p].at[tuple(place)]
            total = ref[...].astype(F32)
            for n in range(3):
                total = total + got[n, first_at].astype(F32)
            ref[...] = total.astype(BF16)

    third, middle, last = [], [], []
    for p in parts:
        at = 24 * p
        own = [spots[p][k][ME] for k in range(3)]
        third.append(
            [Back(p, 2, at + 4 * u, [None, spots[p][1][u], None], u) for u in range(4)]
        )
        middle.append(Straight(p, 1, at + 16, [None, None, own[2]]))
        last.append(Straight(p, 0, at + 20, own))
    order = (FAR, LEFT, RIGHT, ME)
    for send in sends:
        send.wait()
    for p in parts:
        cols = slice(STARTS[p], STARTS[p] + WIDTHS[p])
        for n in ((0, 1), (2,), (3,))[p]:
            some = slice(256 * n, 256 * n + 256)
            back = dot(act[...], ed[:, some]) + dot(act_other[...], ed_other[:, some])
            result[:, 0:SLOTS, some] = back.astype(BF16).reshape(GROUPS, SLOTS, 256)

        def spread_group(g, carry):
            z, y = g // 2, 2 * lax.rem(g, 2)
            right_side = jnp.concatenate([result[g, :, cols], dd_scaled[:, cols]], axis=0)
            total = dot(left_side[g], right_side).astype(BF16)
            sums[p][z, pl.ds(y, 2)] = total.reshape(2, 4, ROWS, WIDTHS[p])
            return carry

        lax.fori_loop(0, GROUPS, spread_group, 0, unroll=8)
        for u in order:
            third[p][u].start()
    for u in order:
        for p in parts:
            third[p][u].on()
    for u in order:
        for p in parts:
            third[p][u].end()
            if u != ME:
                middle[p].send(u)
    for p in parts:
        middle[p].arrive()
        for u in order:
            middle[p].add(spots[p][0][u])
            if u != ME:
                last[p].send(u)
    for p in parts:
        last[p].arrive()
        got = last[p].wholes
        total = mid[:, pl.ds(pl.multiple_of(own_cols + STARTS[p], 128), WIDTHS[p])]
        total = total + sums[p][here[0], here[1], here[2]].astype(F32)
        for n in range(3):
            total = total + got[n].astype(F32)
        out[:, STARTS[p] : STARTS[p] + WIDTHS[p]] = total.astype(BF16)
    for group in third + [middle, last]:
        for back in group:
            for copy in back.copies:
                copy.wait_send()


def run_ffn(carry, partial, eg, eu, ed, dg, du, dd):
    vmem = pl.BlockSpec(memory_space=VMEM)
    hbm = pl.BlockSpec(memory_space=pltpu.HBM)
    blocks = lambda *lead: [VMEM((*lead, WIDTHS[p]), BF16) for p in range(3)]
    sem = pltpu.SemaphoreType.DMA
    return pl.pallas_call(
        ffn_kernel,
        out_shape=jax.ShapeDtypeStruct((ROWS, HALF), BF16),
        in_specs=[hbm] * 8,
        out_specs=vmem,
        scratch_shapes=[
            *[VMEM((4, 4, 4, BLOCK_ROWS[p], WIDTHS[p]), BF16) for p in range(3)],
            *blocks(4, 4, 4, ROWS),
            *blocks(4, 4, 4, ROWS),
            *blocks(4, 2, 2, ROWS),
            *blocks(4, 2, 4, ROWS),
            *blocks(3, ROWS),
            *blocks(3, 4, ROWS),
            VMEM((ROWS, 2 * HALF), BF16),
            VMEM((ROWS, 2 * HALF), BF16),
            VMEM((ROWS, 2 * HALF), F32),
            VMEM((HPAD, 2 * HALF), BF16),
            VMEM((HPAD, 2 * HALF), BF16),
            VMEM((HPAD, HALF), BF16),
            VMEM((HPAD, HALF), BF16),
            VMEM((256, HALF), BF16),
            VMEM((256, HALF), BF16),
            VMEM((DENSE, HALF), BF16),
            VMEM((128, HALF), BF16),
            VMEM((GROUPS * SLOTS, 2 * HALF), BF16),
            VMEM((GROUPS * SLOTS, 128), F32),
            VMEM((GROUPS * SLOTS, HPAD), BF16),
            VMEM((GROUPS * SLOTS, HPAD), BF16),
            VMEM((GROUPS, GROUP_ROWS, 256), BF16),
            VMEM((GROUPS, 128, HALF), BF16),
            sem((6,)),
            sem((252,)),
            sem((252,)),
            sem((39,)),
            sem((39,)),
            sem((72,)),
            sem((72,)),
            sem((6,)),
            sem((6,)),
            VMEM((ROWS + 8, CARRY), F32),
            VMEM((ROWS, 2 * HALF), BF16),
            sem((2,)),
        ],
        compiler_params=pltpu.CompilerParams(
            collective_id=0, has_side_effects=True, vmem_limit_bytes=67043328
        ),
        name="ffn",
    )(carry, partial, eg, eu, ed, dg, du, dd)


def local(
    stream,
    mixer_gain,
    gate_proj,
    input_proj,
    state_maps,
    step_proj,
    step_bias,
    decay_rate,
    input_taps,
    map_taps,
    input_past,
    map_past,
    head_state,
    skip_gain,
    inner_gain,
    mixer_out,
    channel_gain,
    expert_ids,
    expert_weight,
    expert_gate,
    expert_up,
    expert_down,
    dense_gate,
    dense_up,
    dense_down,
    dense_mix,
):
    state_out, carry, partial = run_mixer(
        stream,
        mixer_gain.reshape(1, -1),
        step_proj.T,
        expert_ids.T,
        expert_weight.T,
        step_bias,
        decay_rate,
        skip_gain,
        input_proj,
        input_taps,
        jnp.transpose(input_past, (1, 0, 2)),
        state_maps,
        map_taps,
        jnp.transpose(map_past, (0, 2, 1, 3)).reshape(192, 128),
        inner_gain.reshape(1, -1),
        gate_proj,
        channel_gain.reshape(1, -1),
        dense_mix.reshape(1, -1),
        mixer_out,
        head_state.reshape(256, 4096),
    )
    out = run_ffn(
        carry,
        partial,
        expert_gate.T,
        expert_up.T,
        expert_down,
        dense_gate.T,
        dense_up.T,
        dense_down,
    )
    return out, state_out.reshape(head_state.shape)


def solution(mesh):
    placed = (
        P("ep", None),
        P(),
        P(None, "tp"),
        P(None, "tp"),
        P(None, None, "tp"),
        P(None, "tp"),
        P("tp"),
        P("tp"),
        P(None, "tp"),
        P(None, None, "tp"),
        P("ep", None, "tp"),
        P("ep", None, None, "tp"),
        P("ep", "tp", None),
        P("tp"),
        P("tp"),
        P("tp", None),
        P(),
        P("ep", None),
        P("ep", None),
        P(None, ("ep", "tp")),
        P(None, ("ep", "tp")),
        P(("ep", "tp"), None),
        P("tp", "ep"),
        P("tp", "ep"),
        P("ep", "tp"),
        P("tp"),
    )
    return jax.shard_map(
        local,
        mesh=mesh,
        in_specs=placed,
        out_specs=(P("ep", "tp"), P("ep", "tp", None)),
        check_vma=False,
    )
```

```python
import functools

import jax
import jax.numpy as jnp
from jax import lax
from jax.experimental import pallas as pl
from jax.experimental.pallas import tpu as pltpu
from jax.sharding import PartitionSpec as P

EPS = 1e-06
MESH = pl.DeviceIdType.MESH
F32 = jnp.float32
BF16 = jnp.bfloat16
VMEM = pltpu.VMEM
ANY = pl.ANY

HEADS = 8
ROWS = 32
EXPERTS = 8
CAP = 12
CHUNKS = 8
CHUNK = 512
GROUPS = 8
GROUP_ROWS = 256
SLOTS = 96
HALF = 1024
HIDDEN = 448
HPAD = 512
DENSE = 88
WIDTH = 2048
META = 2048
CARRY = 2304

WIDTHS = (384, 384, 256)
STARTS = (0, 384, 768)
BLOCK_ROWS = (32, 32, 48)
ORDERS = ((2, 1, 0), (1, 0, 2), (0, 2, 1))


def dot(a, b):
    return jnp.dot(a, b, preferred_element_type=F32)


def dot_nt(a, b):
    return lax.dot_general(a, b, (((1,), (1,)), ((), ())), preferred_element_type=F32)


def dot_tn(a, b):
    return lax.dot_general(a, b, (((0,), (0,)), ((), ())), preferred_element_type=F32)


def silu(v):
    return v / (1.0 + jnp.exp(-v))


def rms(v):
    return v * lax.rsqrt(jnp.mean(v * v, axis=-1, keepdims=True) + EPS)


def split(v):
    high = v.astype(BF16)
    return high, (v - high.astype(F32)).astype(BF16)


def mixer_kernel(*refs):
    given, refs = refs[:20], refs[20:]
    state_hbm = given[19]
    state_out, carry_hbm, partial_hbm = refs[:3]
    held, refs = refs[3:22], refs[22:]
    (
        stream,
        mixer_gain,
        step_t,
        ids,
        weights,
        bias,
        decay,
        skip,
        input_w,
        input_taps,
        input_past,
        maps_w,
        map_taps,
        map_past,
        inner_gain,
        gate_w,
        channel_gain,
        mix,
        out_w,
    ) = held
    old, new, dec, write, read, xs, tmp, y, past, carry, partial, in_sems, sems, out_sems = refs
    loads = [
        pltpu.make_async_copy(src, dst, in_sems.at[n])
        for n, (src, dst) in enumerate(zip(given, held))
    ]

    def load_state(t):
        cols = pl.ds(pl.multiple_of(t * CHUNK, CHUNK), CHUNK)
        return pltpu.make_async_copy(state_hbm.at[:, cols], old.at[t], sems.at[t])

    def store_state(t):
        cols = pl.ds(pl.multiple_of(t * CHUNK, CHUNK), CHUNK)
        return pltpu.make_async_copy(
            new.at[t], state_out.at[:, cols], sems.at[CHUNKS + t]
        )

    for load in loads[:18]:
        load.start()
    for t in range(CHUNKS):
        load_state(t).start()
    loads[18].start()

    for load in loads[:8]:
        load.wait()
    normed = (rms(stream[...].astype(F32)) * mixer_gain[...]).astype(BF16)
    steps = dot_nt(normed, step_t[...])

    expert_of = lax.broadcasted_iota(jnp.int32, (EXPERTS, ROWS), 0)
    hit0 = (ids[0:1, :] == expert_of).astype(F32)
    hit1 = (ids[1:2, :] == expert_of).astype(F32)
    member = hit0 + hit1
    upper = (
        lax.broadcasted_iota(jnp.int32, (ROWS, ROWS), 0)
        <= lax.broadcasted_iota(jnp.int32, (ROWS, ROWS), 1)
    ).astype(BF16)
    rank = dot(member.astype(BF16), upper) * member
    weight = hit0 * weights[0:1, :] + hit1 * weights[1:2, :]
    w_high = weight.astype(BF16).astype(F32)
    w_low = weight - w_high
    table = jnp.concatenate(
        [rank, w_high, w_low, jnp.zeros((104, ROWS), F32)], axis=0
    ).astype(BF16)
    eye = (
        lax.broadcasted_iota(jnp.int32, (ROWS, ROWS), 0)
        == lax.broadcasted_iota(jnp.int32, (ROWS, ROWS), 1)
    ).astype(BF16)
    by_row = dot_nt(eye, table)
    carry[0:16, META : META + 256] = jnp.concatenate([by_row[0:16], by_row[16:32]], axis=1)
    carry[0:ROWS, 0:WIDTH] = stream[...].astype(F32)

    for load in loads[8:11]:
        load.wait()
    newest = dot(normed, input_w[...]).astype(BF16).astype(F32)
    conv = newest * input_taps[3:4, :]
    for t in range(3):
        conv = conv + input_past[t].astype(F32) * input_taps[t : t + 1, :]
    conv = silu(conv)

    for load in loads[11:14]:
        load.wait()
    past[...] = map_past[...].astype(F32)
    conv_maps = []
    for m in range(2):
        new_map = dot(normed, maps_w[m]).astype(BF16).astype(F32)
        acc = new_map * map_taps[m, 3:4, :]
        for t in range(3):
            acc = acc + past[pl.ds(2 * t + m, ROWS, stride=6), :] * map_taps[m, t : t + 1, :]
        conv_maps.append(silu(acc))

    lane = lax.broadcasted_iota(jnp.int32, (ROWS, 128), 1)
    low_half = lane < 64

    def both_halves(v):
        turned = pltpu.roll(v, 64, 1)
        return jnp.where(low_half, v, turned), jnp.where(low_half, turned, v)

    write_by_group = both_halves(conv_maps[0])
    read_by_group = both_halves(conv_maps[1])
    for h in range(HEADS):
        rows = pl.ds(h, ROWS, stride=HEADS)
        v = jnp.broadcast_to(steps[:, h : h + 1], (ROWS, 128)) + bias[h]
        step = jnp.maximum(v, 0.0) + jnp.log1p(jnp.exp(-jnp.abs(v)))
        dec[rows, :] = jnp.exp(-decay[h] * step)
        pair = conv[:, 128 * (h // 2) : 128 * (h // 2) + 128]
        mine = low_half if h % 2 == 0 else jnp.logical_not(low_half)
        tmp[rows, :] = jnp.where(mine, step * pair, 0.0)
        write[rows, :] = write_by_group[h // 4]
        read[rows, :] = read_by_group[h // 4]
    high, low = split(tmp[...])
    xs[:, 0:128] = high
    xs[:, 128:256] = low
    y[...] = jnp.zeros_like(y)

    for load in loads[14:18]:
        load.wait()
    carry[ROWS : ROWS + 1, 0:WIDTH] = channel_gain[...]
    carry[ROWS + 1 : ROWS + 2, 0:HALF] = mix[...]
    out_parts = []
    for n, (first, size) in enumerate(((0, WIDTH), (META, 256))):
        where = (pl.ds(0, ROWS + 8), pl.ds(first, size))
        out_parts.append(
            pltpu.make_async_copy(carry.at[where], carry_hbm.at[where], out_sems.at[n])
        )
    out_parts[0].start()
    out_parts[1].start()
    gate = silu(dot(normed, gate_w[...]).astype(BF16).astype(F32))
    slot = lax.broadcasted_iota(jnp.int32, (256, CHUNK), 0) % 64
    place = lax.broadcasted_iota(jnp.int32, (256, CHUNK), 1) // 64

    def chunk_step(t, carry):
        spread = (slot == place + 8 * t).astype(F32).astype(BF16)
        load_state(t).wait()
        values = dot(xs[...], spread)
        wide = lambda ref: jnp.concatenate([ref[...]] * (CHUNK // 128), axis=1)
        fresh = wide(dec) * old[t] + values * wide(write)
        new[t] = fresh
        store_state(t).start()
        both = dot_nt(jnp.concatenate(split(fresh * wide(read)), axis=0), spread[0:128])
        y[...] += both[0:256] + both[256:512]
        return carry

    lax.fori_loop(0, CHUNKS, chunk_step, 0, unroll=4)

    pieces = []
    for j in range(HEADS // 2):
        even = y[pl.ds(2 * j, ROWS, stride=HEADS), :]
        odd = y[pl.ds(2 * j + 1, ROWS, stride=HEADS), :]
        gain = jnp.where(low_half, skip[2 * j], skip[2 * j + 1])
        cols = slice(128 * j, 128 * j + 128)
        pieces.append(
            (jnp.where(low_half, even, odd) + gain * conv[:, cols]) * gate[:, cols]
        )
    groups = [jnp.concatenate(pieces[2 * g : 2 * g + 2], axis=1) for g in range(2)]
    inner = jnp.concatenate([rms(g) for g in groups], axis=1) * inner_gain[...]
    loads[18].wait()
    partial[...] = dot(inner.astype(BF16), out_w[...]).astype(BF16)
    out_parts.append(pltpu.make_async_copy(partial, partial_hbm, out_sems.at[2]))
    out_parts[2].start()
    for part in out_parts:
        part.wait()
    for t in range(CHUNKS):
        store_state(t).wait()


def run_mixer(*given):
    hbm = pl.BlockSpec(memory_space=pltpu.HBM)
    lanes = lambda: VMEM((256, 128), F32)
    held = [
        (pltpu.SMEM if 5 <= n < 8 else VMEM)(v.shape, v.dtype)
        for n, v in enumerate(given[:19])
    ]
    return pl.pallas_call(
        mixer_kernel,
        out_shape=(
            jax.ShapeDtypeStruct((256, 4096), F32),
            jax.ShapeDtypeStruct((ROWS + 8, CARRY), F32),
            jax.ShapeDtypeStruct((ROWS, 2 * HALF), BF16),
        ),
        in_specs=[hbm] * 20,
        out_specs=(hbm, hbm, hbm),
        scratch_shapes=[
            *held,
            VMEM((CHUNKS, 256, CHUNK), F32),
            VMEM((CHUNKS, 256, CHUNK), F32),
            lanes(),
            lanes(),
            lanes(),
            VMEM((256, 256), BF16),
            lanes(),
            lanes(),
            VMEM((192, 128), F32),
            VMEM((ROWS + 8, CARRY), F32),
            VMEM((ROWS, 2 * HALF), BF16),
            pltpu.SemaphoreType.DMA((19,)),
            pltpu.SemaphoreType.DMA((2 * CHUNKS,)),
            pltpu.SemaphoreType.DMA((3,)),
        ],
        compiler_params=pltpu.CompilerParams(vmem_limit_bytes=67043328),
        name="mixer",
    )(*given)


def ffn_kernel(
    carry_hbm,
    partial_hbm,
    eg_hbm,
    eu_hbm,
    ed_hbm,
    dg_hbm,
    du_hbm,
    dd_hbm,
    out,
    x0,
    x1,
    x2,
    y0,
    y1,
    y2,
    s0,
    s1,
    s2,
    *rest,
):
    landed, rest = rest[:12], rest[12:]
    landing = [landed[3 * k : 3 * k + 3] for k in range(4)]
    (
    other_partial,
    wide,
    mid,
    eg,
    eu,
    ed,
    ed_other,
    dgu,
    dgu_other,
    dd,
    dd_scaled,
    packed,
    slot_weight,
    act,
    act_other,
    left_side,
    result,
    local_sem,
    ag_send,
    ag_recv,
    dd_send,
    dd_recv,
    rs_send,
    rs_recv,
    mi_send,
    mi_recv,
        carry,
        partial,
        gate_own,
        up_own,
        small_sem,
    ) = rest
    ep = lax.axis_index("ep")
    core = lax.axis_index("tp")
    coords = (ep // 16, (ep // 4) % 4, ep % 4)
    other = 1 - core
    own_cols = pl.multiple_of(core * HALF, HALF)
    other_cols = pl.multiple_of(other * HALF, HALF)
    expert = ep // 8
    mine = (x0, x1, x2)
    theirs = (y0, y1, y2)
    sums = (s0, s1, s2)

    def neighbour(dim, shift):
        moved = list(coords)
        moved[dim] = lax.rem(coords[dim] + shift, 4)
        return (moved[0] * 16 + moved[1] * 4 + moved[2], core)

    partner = (ep, other)

    small = [
        pltpu.make_async_copy(partial_hbm, partial, small_sem.at[0]),
        pltpu.make_async_copy(carry_hbm, carry, small_sem.at[1]),
    ]
    for load in small:
        load.start()
    barrier = pltpu.get_barrier_semaphore()
    for dim in range(3):
        for shift in (1, 2, 3):
            pl.semaphore_signal(
                barrier, inc=1, device_id=neighbour(dim, shift), device_id_type=MESH
            )
    pl.semaphore_signal(barrier, inc=1, device_id=partner, device_id_type=MESH)
    small[0].wait()
    pl.semaphore_wait(barrier, 10)

    def to_partner(src, dst, n):
        return pltpu.make_async_remote_copy(
            src_ref=src,
            dst_ref=dst,
            send_sem=mi_send.at[n],
            recv_sem=mi_recv.at[n],
            device_id=partner,
            device_id_type=MESH,
        )

    swap_partial = to_partner(partial, other_partial, 0)
    swap_partial.start()
    loads = [
        pltpu.make_async_copy(eg_hbm, eg.at[pl.ds(0, HIDDEN)], local_sem.at[0]),
        pltpu.make_async_copy(eu_hbm, eu.at[pl.ds(0, HIDDEN)], local_sem.at[1]),
        pltpu.make_async_copy(
            ed_hbm.at[:, pl.ds(own_cols, HALF)], ed.at[pl.ds(0, HIDDEN)], local_sem.at[2]
        ),
        pltpu.make_async_copy(dg_hbm, dgu.at[pl.ds(0, DENSE)], local_sem.at[3]),
        pltpu.make_async_copy(du_hbm, dgu.at[pl.ds(128, DENSE)], local_sem.at[4]),
        pltpu.make_async_copy(dd_hbm, dd, local_sem.at[5]),
    ]
    for load in loads:
        load.start()

    small[1].wait()
    swap_partial.wait()
    mixed = partial[...].astype(F32) + other_partial[...].astype(F32)
    hidden = carry[0:ROWS, 0:WIDTH] + mixed
    mid[...] = hidden
    wide[...] = (rms(hidden) * carry[ROWS : ROWS + 1, 0:WIDTH]).astype(BF16)
    here = coords
    for p in range(3):
        cols = pl.ds(pl.multiple_of(own_cols + STARTS[p], 128), WIDTHS[p])
        mine[p][here[0], here[1], here[2], 0:ROWS, :] = wide[:, cols]
    x2[here[0], here[1], here[2], ROWS : ROWS + 16, :] = carry[0:16, META : META + 256].astype(
        BF16
    )

    def cut(buf, p, where, half=None, rows=None):
        index = [None, None, None]
        for q in range(3):
            index[ORDERS[p][q]] = pl.ds(0, 4) if where[q] is None else where[q]
        if half is not None:
            free = sorted(ORDERS[p][q] for q in range(3) if where[q] is None)
            if free:
                index[free[0]] = pl.ds(2 * half, 2)
            else:
                rows = pl.ds(0, 16) if half == 0 else pl.ds(16, rows - 16)
        elif rows is not None:
            rows = pl.ds(0, rows)
        if rows is not None and not (half is not None and free):
            index.append(rows)
        return buf.at[tuple(index)]

    def turn(p, k, shift):
        return lax.rem(coords[ORDERS[p][k]] + shift, 4)

    ME, RIGHT, FAR, LEFT = 0, 1, 2, 3
    spots = [[[turn(p, k, shift) for shift in range(4)] for k in range(3)] for p in range(3)]

    class Ring:
        def __init__(self, p, k, at, place, direct=False):
            self.p, self.k, self.place, self.direct = p, k, place, direct
            self.copies = [self.copy(at, ME, None, 1), self.copy(at + 1, ME, None, 3)]
            if direct:
                self.copies.append(self.copy(at + 2, ME, None, 2))
            else:
                self.copies.append(self.copy(at + 2, LEFT, 0, 1))
                self.copies.append(self.copy(at + 3, RIGHT, 1, 3))

        def copy(self, at, shift, half, to):
            p = self.p
            where = list(self.place)
            where[self.k] = spots[p][self.k][shift]
            rows = BLOCK_ROWS[p] if half is not None else None
            ref = cut(mine[p], p, where, half, rows)
            return pltpu.make_async_remote_copy(
                src_ref=ref,
                dst_ref=ref,
                send_sem=ag_send.at[at],
                recv_sem=ag_recv.at[at],
                device_id=neighbour(ORDERS[p][self.k], to),
                device_id_type=MESH,
            )

        def start(self):
            if self.direct:
                self.copies[2].start()
            self.copies[0].start()
            self.copies[1].start()

        def on(self):
            self.copies[0].wait_recv()
            if not self.direct:
                self.copies[2].start()
            self.copies[1].wait_recv()
            if not self.direct:
                self.copies[3].start()

        def end(self):
            for copy in self.copies[2:]:
                copy.wait_recv()

    first, second, third_way = [], [], []
    for p in range(3):
        at = 84 * p
        own = [spots[p][k][ME] for k in range(3)]
        first.append(Ring(p, 0, at, own, True))
        second.append(
            [Ring(p, 1, at + 4 + 4 * u, [spots[p][0][u], None, own[2]], True) for u in range(4)]
        )
        third_way.append(
            [
                [
                    Ring(
                        p,
                        2,
                        at + 20 + 16 * u + 4 * v,
                        [spots[p][0][u], spots[p][1][v], None],
                        FAR in (u, v) and ME not in (u, v),
                    )
                    for v in range(4)
                ]
                for u in range(4)
            ]
        )
    rings = [first] + second + [row for part in third_way for row in part]
    hand_overs = []

    def hand_over(p, n, second_at, third_at):
        where = [None, second_at, third_at]
        copy = pltpu.make_async_remote_copy(
            src_ref=cut(mine[p], p, where, None, ROWS),
            dst_ref=cut(theirs[p], p, where, None, ROWS),
            send_sem=dd_send.at[13 * p + n],
            recv_sem=dd_recv.at[13 * p + n],
            device_id=partner,
            device_id_type=MESH,
        )
        copy.start()
        hand_overs.append(copy)

    parts = range(3)
    def launch(*pairs):
        for p in parts:
            for u, v in pairs:
                third_way[p][u][v].start()

    def pass_on(*pairs):
        for p in parts:
            for u, v in pairs:
                third_way[p][u][v].on()

    for p in parts:
        first[p].start()
    for p in parts:
        second[p][ME].start()
    launch((ME, ME))

    early = [
        to_partner(
            ed_hbm.at[:, pl.ds(other_cols, HALF)], ed_other.at[pl.ds(0, HIDDEN)], 1
        ),
        to_partner(dg_hbm, dgu_other.at[pl.ds(0, DENSE)], 2),
        to_partner(du_hbm, dgu_other.at[pl.ds(128, DENSE)], 3),
    ]
    for copy in early:
        copy.start()

    for p in parts:
        first[p].on()
        for u in (LEFT, RIGHT):
            second[p][u].start()
            third_way[p][u][ME].start()
    for p in parts:
        second[p][ME].on()
    launch((ME, RIGHT), (ME, LEFT))
    for p in parts:
        first[p].end()
        second[p][FAR].start()
        third_way[p][FAR][ME].start()
    for p in parts:
        second[p][ME].end()
    launch((ME, FAR))
    pass_on((ME, ME))
    for ref in (eg, eu, ed, ed_other):
        ref[HIDDEN:HPAD, :] = jnp.zeros((HPAD - HIDDEN, ref.shape[1]), BF16)
    for ref in (dgu, dgu_other):
        ref[DENSE:128, :] = jnp.zeros((128 - DENSE, HALF), BF16)
        ref[128 + DENSE : 256, :] = jnp.zeros((128 - DENSE, HALF), BF16)
    dd_scaled[DENSE:128, :] = jnp.zeros((128 - DENSE, HALF), BF16)
    for g in range(GROUPS):
        result[g, SLOTS:128, :] = jnp.zeros((128 - SLOTS, HALF), BF16)
    for p in parts:
        second[p][LEFT].on()
        second[p][RIGHT].on()
    launch((LEFT, RIGHT), (RIGHT, RIGHT), (LEFT, LEFT), (RIGHT, LEFT))
    pass_on((LEFT, ME), (RIGHT, ME), (ME, RIGHT), (ME, LEFT))
    for p in parts:
        second[p][LEFT].end()
        second[p][RIGHT].end()
    launch((LEFT, FAR), (RIGHT, FAR))
    for p in parts:
        second[p][FAR].on()
    launch((FAR, RIGHT), (FAR, LEFT))
    for p in parts:
        second[p][FAR].end()
    launch((FAR, FAR))
    pass_on((FAR, ME), (ME, FAR))
    for p in parts:
        hand_over(p, 0, None, spots[p][2][ME])
        hand_over(p, 1, spots[p][1][ME], spots[p][2][LEFT])
        hand_over(p, 2, spots[p][1][ME], spots[p][2][RIGHT])

    def finish(v, n):
        for p in parts:
            for u in range(4):
                third_way[p][u][v].end()
            hand_over(p, n, spots[p][1][v], spots[p][2][FAR])

    def sides(v, n):
        for p in parts:
            hand_over(p, n, spots[p][1][v], spots[p][2][LEFT])
            hand_over(p, n + 1, spots[p][1][v], spots[p][2][RIGHT])

    pass_on((LEFT, RIGHT), (RIGHT, RIGHT), (LEFT, LEFT), (RIGHT, LEFT))
    finish(ME, 3)
    pass_on((LEFT, FAR), (RIGHT, FAR), (FAR, RIGHT), (FAR, LEFT))
    sides(RIGHT, 4)
    sides(LEFT, 6)
    pass_on((FAR, FAR))
    sides(FAR, 8)
    finish(RIGHT, 10)
    finish(LEFT, 11)
    finish(FAR, 12)
    pick_row = lax.broadcasted_iota(jnp.int32, (128, 128), 0)
    pick_rank = (pick_row == expert).astype(F32).astype(BF16)
    pick_weight = (
        jnp.logical_or(pick_row == expert + 8, pick_row == expert + 16)
    ).astype(F32).astype(BF16)
    lane = lax.broadcasted_iota(jnp.int32, (GROUP_ROWS, 128), 1)
    source = lax.broadcasted_iota(jnp.int32, (GROUP_ROWS, 128), 0) // ROWS

    def group_of(bufs, g):
        z, y = g // 2, 2 * lax.rem(g, 2)
        return jnp.concatenate(
            [
                bufs[p][z, pl.ds(y, 2), :, 0:ROWS, :].reshape(GROUP_ROWS, WIDTHS[p])
                for p in range(3)
            ],
            axis=1,
        )

    def pack_group(g, carry):
        z, y = g // 2, 2 * lax.rem(g, 2)
        tags = x2[z, pl.ds(y, 2), :, ROWS : ROWS + 16, :].reshape(8, 16, 256)
        tags = jnp.concatenate([tags[:, :, 0:128], tags[:, :, 128:256]], axis=1)
        tags = tags.reshape(GROUP_ROWS, 128)
        rank = dot(tags, pick_rank).astype(jnp.int32)
        hit = jnp.logical_and(rank > 0, rank + (CAP * source - 1) == lane)
        table = hit.astype(F32).astype(BF16)
        left_side[g, :, 0:128] = table
        used = table[:, 0:SLOTS]
        slots = pl.ds(pl.multiple_of(g * SLOTS, SLOTS), SLOTS)
        packed[slots, pl.ds(own_cols, HALF)] = dot_tn(used, group_of(mine, g)).astype(BF16)
        slot_tags = dot_tn(used, tags).astype(BF16)
        slot_weight[slots, :] = dot(slot_tags, pick_weight)
        return carry

    lax.fori_loop(0, GROUPS, pack_group, 0, unroll=8)
    for load in loads:
        load.wait()
    own = pl.ds(own_cols, HALF)
    rest_cols = pl.ds(other_cols, HALF)
    for i in range(2):
        units = pl.ds(256 * i, 256)
        gate_own[:, units] = dot_nt(packed[:, own], eg[units, own])
        up_own[:, units] = dot_nt(packed[:, own], eu[units, own])
    for copy in early:
        copy.wait()
    for copy in hand_overs:
        copy.wait()

    def pack_other(g, carry):
        used = left_side[g, :, 0:SLOTS]
        slots = pl.ds(pl.multiple_of(g * SLOTS, SLOTS), SLOTS)
        packed[slots, pl.ds(other_cols, HALF)] = dot_tn(used, group_of(theirs, g)).astype(
            BF16
        )
        return carry

    lax.fori_loop(0, GROUPS, pack_other, 0, unroll=8)

    sends = []
    for i in range(2):
        units = pl.ds(256 * i, 256)
        gate = gate_own[:, units] + dot_nt(packed[:, rest_cols], eg[units, rest_cols])
        up = up_own[:, units] + dot_nt(packed[:, rest_cols], eu[units, rest_cols])
        act[:, units] = (silu(gate) * up * slot_weight[:, 0:1]).astype(BF16)
        copy = to_partner(act.at[:, units], act_other.at[:, units], 4 + i)
        copy.start()
        sends.append(copy)

    def dense_group(g, carry):
        both = dot_nt(group_of(mine, g), dgu[...]) + dot_nt(group_of(theirs, g), dgu_other[...])
        left_side[g, :, 128:256] = (silu(both[:, 0:128]) * both[:, 128:256]).astype(BF16)
        return carry

    lax.fori_loop(0, GROUPS, dense_group, 0, unroll=8)
    share = 1.0 / (1.0 + jnp.exp(-carry[ROWS + 1 : ROWS + 2, 0:HALF]))
    dd_scaled[0:DENSE, :] = (dd[...].astype(F32) * share).astype(BF16)

    class Back:
        def __init__(self, p, k, at, place, slot):
            self.p, self.k, self.place, self.slot = p, k, place, slot
            self.halves, self.wholes = landing[0][p], landing[1][p]
            self.copies = [
                self.copy(at, FAR, 0, 1, self.halves.at[slot, 0]),
                self.copy(at + 1, FAR, 1, 3, self.halves.at[slot, 1]),
                self.copy(at + 2, RIGHT, None, 1, self.wholes.at[slot, 0]),
                self.copy(at + 3, LEFT, None, 3, self.wholes.at[slot, 1]),
            ]

        def spot(self, shift):
            where = list(self.place)
            where[self.k] = spots[self.p][self.k][shift]
            return where

        def copy(self, at, shift, half, to, target):
            p = self.p
            rows = ROWS if half is not None else None
            return pltpu.make_async_remote_copy(
                src_ref=cut(sums[p], p, self.spot(shift), half, rows),
                dst_ref=target,
                send_sem=rs_send.at[at],
                recv_sem=rs_recv.at[at],
                device_id=neighbour(ORDERS[p][self.k], to),
                device_id_type=MESH,
            )

        def start(self):
            self.copies[0].start()
            self.copies[1].start()

        def add_half(self, shift, half):
            p, got = self.p, self.halves
            where = self.spot(shift)
            place = [None, None, None]
            for q in range(3):
                place[ORDERS[p][q]] = where[q]
            free = [d for d in range(3) if place[d] is None]
            for t in range(2):
                place[free[0]] = 2 * half + t
                ref = sums[p].at[tuple(place)]
                ref[...] = ref[...] + got[self.slot, half, t]

        def on(self):
            self.copies[0].wait_recv()
            self.add_half(RIGHT, 0)
            self.copies[2].start()
            self.copies[1].wait_recv()
            self.add_half(LEFT, 1)
            self.copies[3].start()

        def end(self):
            p, got = self.p, self.wholes
            self.copies[2].wait_recv()
            self.copies[3].wait_recv()
            where = self.spot(ME)
            place = [None, None, None]
            for q in range(3):
                place[ORDERS[p][q]] = where[q]
            free = [d for d in range(3) if place[d] is None]
            for t in range(4):
                place[free[0]] = t
                ref = sums[p].at[tuple(place)]
                total = ref[...].astype(F32) + got[self.slot, 0, t].astype(F32)
                ref[...] = (total + got[self.slot, 1, t].astype(F32)).astype(BF16)

    class Straight:
        def __init__(self, p, k, at, place):
            self.p, self.k, self.place, self.wholes = p, k, place, landing[2 + k][p]
            self.copies = [self.copy(at + u - 1, u) for u in (RIGHT, FAR, LEFT)]

        def copy(self, at, u):
            p = self.p
            where = list(self.place)
            where[self.k] = spots[p][self.k][u]
            return pltpu.make_async_remote_copy(
                src_ref=cut(sums[p], p, where),
                dst_ref=self.wholes.at[u - 1],
                send_sem=rs_send.at[at],
                recv_sem=rs_recv.at[at],
                device_id=neighbour(ORDERS[p][self.k], u),
                device_id_type=MESH,
            )

        def send(self, u):
            self.copies[u - 1].start()

        def arrive(self):
            for copy in self.copies:
                copy.wait_recv()

        def add(self, first_at):
            p, got = self.p, self.wholes
            place = [None, None, None]
            for q in range(3):
                place[ORDERS[p][q]] = spots[p][q][ME]
            place[ORDERS[p][0]] = first_at
            ref = sums[p].at[tuple(place)]
            total = ref[...].astype(F32)
            for n in range(3):
                total = total + got[n, first_at].astype(F32)
            ref[...] = total.astype(BF16)

    third, middle, last = [], [], []
    for p in parts:
        at = 24 * p
        own = [spots[p][k][ME] for k in range(3)]
        third.append(
            [Back(p, 2, at + 4 * u, [None, spots[p][1][u], None], u) for u in range(4)]
        )
        middle.append(Straight(p, 1, at + 16, [None, None, own[2]]))
        last.append(Straight(p, 0, at + 20, own))
    order = (FAR, LEFT, RIGHT, ME)
    for send in sends:
        send.wait()
    for p in parts:
        cols = slice(STARTS[p], STARTS[p] + WIDTHS[p])
        for n in ((0, 1), (2,), (3,))[p]:
            some = slice(256 * n, 256 * n + 256)
            back = dot(act[...], ed[:, some]) + dot(act_other[...], ed_other[:, some])
            result[:, 0:SLOTS, some] = back.astype(BF16).reshape(GROUPS, SLOTS, 256)

        def spread_group(g, carry):
            z, y = g // 2, 2 * lax.rem(g, 2)
            right_side = jnp.concatenate([result[g, :, cols], dd_scaled[:, cols]], axis=0)
            total = dot(left_side[g], right_side).astype(BF16)
            sums[p][z, pl.ds(y, 2)] = total.reshape(2, 4, ROWS, WIDTHS[p])
            return carry

        lax.fori_loop(0, GROUPS, spread_group, 0, unroll=8)
        for u in order:
            third[p][u].start()
    for u in order:
        for p in parts:
            third[p][u].on()
    for u in order:
        for p in parts:
            third[p][u].end()
            if u != ME:
                middle[p].send(u)
    for p in parts:
        middle[p].arrive()
        for u in order:
            middle[p].add(spots[p][0][u])
            if u != ME:
                last[p].send(u)
    for p in parts:
        last[p].arrive()
        got = last[p].wholes
        total = mid[:, pl.ds(pl.multiple_of(own_cols + STARTS[p], 128), WIDTHS[p])]
        total = total + sums[p][here[0], here[1], here[2]].astype(F32)
        for n in range(3):
            total = total + got[n].astype(F32)
        out[:, STARTS[p] : STARTS[p] + WIDTHS[p]] = total.astype(BF16)
    for group in third + [middle, last] + rings:
        for sender in group:
            for copy in sender.copies:
                copy.wait_send()


def run_ffn(carry, partial, eg, eu, ed, dg, du, dd):
    vmem = pl.BlockSpec(memory_space=VMEM)
    hbm = pl.BlockSpec(memory_space=pltpu.HBM)
    blocks = lambda *lead: [VMEM((*lead, WIDTHS[p]), BF16) for p in range(3)]
    sem = pltpu.SemaphoreType.DMA
    return pl.pallas_call(
        ffn_kernel,
        out_shape=jax.ShapeDtypeStruct((ROWS, HALF), BF16),
        in_specs=[hbm] * 8,
        out_specs=vmem,
        scratch_shapes=[
            *[VMEM((4, 4, 4, BLOCK_ROWS[p], WIDTHS[p]), BF16) for p in range(3)],
            *blocks(4, 4, 4, ROWS),
            *blocks(4, 4, 4, ROWS),
            *blocks(4, 2, 2, ROWS),
            *blocks(4, 2, 4, ROWS),
            *blocks(3, ROWS),
            *blocks(3, 4, ROWS),
            VMEM((ROWS, 2 * HALF), BF16),
            VMEM((ROWS, 2 * HALF), BF16),
            VMEM((ROWS, 2 * HALF), F32),
            VMEM((HPAD, 2 * HALF), BF16),
            VMEM((HPAD, 2 * HALF), BF16),
            VMEM((HPAD, HALF), BF16),
            VMEM((HPAD, HALF), BF16),
            VMEM((256, HALF), BF16),
            VMEM((256, HALF), BF16),
            VMEM((DENSE, HALF), BF16),
            VMEM((128, HALF), BF16),
            VMEM((GROUPS * SLOTS, 2 * HALF), BF16),
            VMEM((GROUPS * SLOTS, 128), F32),
            VMEM((GROUPS * SLOTS, HPAD), BF16),
            VMEM((GROUPS * SLOTS, HPAD), BF16),
            VMEM((GROUPS, GROUP_ROWS, 256), BF16),
            VMEM((GROUPS, 128, HALF), BF16),
            sem((6,)),
            sem((252,)),
            sem((252,)),
            sem((39,)),
            sem((39,)),
            sem((72,)),
            sem((72,)),
            sem((6,)),
            sem((6,)),
            VMEM((ROWS + 8, CARRY), F32),
            VMEM((ROWS, 2 * HALF), BF16),
            VMEM((GROUPS * SLOTS, HPAD), F32),
            VMEM((GROUPS * SLOTS, HPAD), F32),
            sem((2,)),
        ],
        compiler_params=pltpu.CompilerParams(
            collective_id=0, has_side_effects=True, vmem_limit_bytes=67043328
        ),
        name="ffn",
    )(carry, partial, eg, eu, ed, dg, du, dd)


def local(
    stream,
    mixer_gain,
    gate_proj,
    input_proj,
    state_maps,
    step_proj,
    step_bias,
    decay_rate,
    input_taps,
    map_taps,
    input_past,
    map_past,
    head_state,
    skip_gain,
    inner_gain,
    mixer_out,
    channel_gain,
    expert_ids,
    expert_weight,
    expert_gate,
    expert_up,
    expert_down,
    dense_gate,
    dense_up,
    dense_down,
    dense_mix,
):
    state_out, carry, partial = run_mixer(
        stream,
        mixer_gain.reshape(1, -1),
        step_proj.T,
        expert_ids.T,
        expert_weight.T,
        step_bias,
        decay_rate,
        skip_gain,
        input_proj,
        input_taps,
        jnp.transpose(input_past, (1, 0, 2)),
        state_maps,
        map_taps,
        jnp.transpose(map_past, (0, 2, 1, 3)).reshape(192, 128),
        inner_gain.reshape(1, -1),
        gate_proj,
        channel_gain.reshape(1, -1),
        dense_mix.reshape(1, -1),
        mixer_out,
        head_state.reshape(256, 4096),
    )
    out = run_ffn(
        carry,
        partial,
        expert_gate.T,
        expert_up.T,
        expert_down,
        dense_gate.T,
        dense_up.T,
        dense_down,
    )
    return out, state_out.reshape(head_state.shape)


def solution(mesh):
    placed = (
        P("ep", None),
        P(),
        P(None, "tp"),
        P(None, "tp"),
        P(None, None, "tp"),
        P(None, "tp"),
        P("tp"),
        P("tp"),
        P(None, "tp"),
        P(None, None, "tp"),
        P("ep", None, "tp"),
        P("ep", None, None, "tp"),
        P("ep", "tp", None),
        P("tp"),
        P("tp"),
        P("tp", None),
        P(),
        P("ep", None),
        P("ep", None),
        P(None, ("ep", "tp")),
        P(None, ("ep", "tp")),
        P(("ep", "tp"), None),
        P("tp", "ep"),
        P("tp", "ep"),
        P("ep", "tp"),
        P("tp"),
    )
    return jax.shard_map(
        local,
        mesh=mesh,
        in_specs=placed,
        out_specs=(P("ep", "tp"), P("ep", "tp", None)),
        check_vma=False,
    )
```

```python
import functools

import jax
import jax.numpy as jnp
from jax import lax
from jax.experimental import pallas as pl
from jax.experimental.pallas import tpu as pltpu
from jax.sharding import PartitionSpec as P

EPS = 1e-06
MESH = pl.DeviceIdType.MESH
F32 = jnp.float32
BF16 = jnp.bfloat16
VMEM = pltpu.VMEM
ANY = pl.ANY

HEADS = 8
ROWS = 32
EXPERTS = 8
CAP = 12
CHUNKS = 8
CHUNK = 512
GROUPS = 8
GROUP_ROWS = 256
SLOTS = 96
HALF = 1024
HIDDEN = 448
HPAD = 512
DENSE = 88
WIDTH = 2048
META = 2048
CARRY = 2304

WIDTHS = (384, 384, 256)
STARTS = (0, 384, 768)
BLOCK_ROWS = (32, 32, 48)
ORDERS = ((2, 1, 0), (1, 0, 2), (0, 2, 1))


def dot(a, b):
    return jnp.dot(a, b, preferred_element_type=F32)


def dot_nt(a, b):
    return lax.dot_general(a, b, (((1,), (1,)), ((), ())), preferred_element_type=F32)


def dot_tn(a, b):
    return lax.dot_general(a, b, (((0,), (0,)), ((), ())), preferred_element_type=F32)


def silu(v):
    return v / (1.0 + jnp.exp(-v))


def rms(v):
    return v * lax.rsqrt(jnp.mean(v * v, axis=-1, keepdims=True) + EPS)


def split(v):
    high = v.astype(BF16)
    return high, (v - high.astype(F32)).astype(BF16)


def mixer_kernel(*refs):
    given, refs = refs[:20], refs[20:]
    state_hbm = given[19]
    state_out, carry_hbm, partial_hbm = refs[:3]
    held, refs = refs[3:22], refs[22:]
    (
        stream,
        mixer_gain,
        step_t,
        ids,
        weights,
        bias,
        decay,
        skip,
        input_w,
        input_taps,
        input_past,
        maps_w,
        map_taps,
        map_past,
        inner_gain,
        gate_w,
        channel_gain,
        mix,
        out_w,
    ) = held
    old, new, dec, write, read, xs, tmp, y, past, carry, partial, in_sems, sems, out_sems = refs
    loads = [
        pltpu.make_async_copy(src, dst, in_sems.at[n])
        for n, (src, dst) in enumerate(zip(given, held))
    ]

    def load_state(t):
        cols = pl.ds(pl.multiple_of(t * CHUNK, CHUNK), CHUNK)
        return pltpu.make_async_copy(state_hbm.at[:, cols], old.at[t], sems.at[t])

    def store_state(t):
        cols = pl.ds(pl.multiple_of(t * CHUNK, CHUNK), CHUNK)
        return pltpu.make_async_copy(
            new.at[t], state_out.at[:, cols], sems.at[CHUNKS + t]
        )

    for load in loads[:15]:
        load.start()
    for t in range(CHUNKS):
        load_state(t).start()
    for load in loads[15:]:
        load.start()

    for load in loads[:8]:
        load.wait()
    normed = (rms(stream[...].astype(F32)) * mixer_gain[...]).astype(BF16)
    steps = dot_nt(normed, step_t[...])

    expert_of = lax.broadcasted_iota(jnp.int32, (EXPERTS, ROWS), 0)
    hit0 = (ids[0:1, :] == expert_of).astype(F32)
    hit1 = (ids[1:2, :] == expert_of).astype(F32)
    member = hit0 + hit1
    upper = (
        lax.broadcasted_iota(jnp.int32, (ROWS, ROWS), 0)
        <= lax.broadcasted_iota(jnp.int32, (ROWS, ROWS), 1)
    ).astype(BF16)
    rank = dot(member.astype(BF16), upper) * member
    weight = hit0 * weights[0:1, :] + hit1 * weights[1:2, :]
    w_high = weight.astype(BF16).astype(F32)
    w_low = weight - w_high
    table = jnp.concatenate(
        [rank, w_high, w_low, jnp.zeros((104, ROWS), F32)], axis=0
    ).astype(BF16)
    eye = (
        lax.broadcasted_iota(jnp.int32, (ROWS, ROWS), 0)
        == lax.broadcasted_iota(jnp.int32, (ROWS, ROWS), 1)
    ).astype(BF16)
    by_row = dot_nt(eye, table)
    carry[0:16, META : META + 256] = jnp.concatenate([by_row[0:16], by_row[16:32]], axis=1)
    carry[0:ROWS, 0:WIDTH] = stream[...].astype(F32)

    for load in loads[8:11]:
        load.wait()
    newest = dot(normed, input_w[...]).astype(BF16).astype(F32)
    conv = newest * input_taps[3:4, :]
    for t in range(3):
        conv = conv + input_past[t].astype(F32) * input_taps[t : t + 1, :]
    conv = silu(conv)

    for load in loads[11:14]:
        load.wait()
    past[...] = map_past[...].astype(F32)
    conv_maps = []
    for m in range(2):
        new_map = dot(normed, maps_w[m]).astype(BF16).astype(F32)
        acc = new_map * map_taps[m, 3:4, :]
        for t in range(3):
            acc = acc + past[pl.ds(2 * t + m, ROWS, stride=6), :] * map_taps[m, t : t + 1, :]
        conv_maps.append(silu(acc))

    lane = lax.broadcasted_iota(jnp.int32, (ROWS, 128), 1)
    low_half = lane < 64

    def both_halves(v):
        turned = pltpu.roll(v, 64, 1)
        return jnp.where(low_half, v, turned), jnp.where(low_half, turned, v)

    write_by_group = both_halves(conv_maps[0])
    read_by_group = both_halves(conv_maps[1])
    for h in range(HEADS):
        rows = pl.ds(h, ROWS, stride=HEADS)
        v = jnp.broadcast_to(steps[:, h : h + 1], (ROWS, 128)) + bias[h]
        step = jnp.maximum(v, 0.0) + jnp.log1p(jnp.exp(-jnp.abs(v)))
        dec[rows, :] = jnp.exp(-decay[h] * step)
        pair = conv[:, 128 * (h // 2) : 128 * (h // 2) + 128]
        mine = low_half if h % 2 == 0 else jnp.logical_not(low_half)
        tmp[rows, :] = jnp.where(mine, step * pair, 0.0)
        write[rows, :] = write_by_group[h // 4]
        read[rows, :] = read_by_group[h // 4]
    high, low = split(tmp[...])
    xs[:, 0:128] = high
    xs[:, 128:256] = low
    y[...] = jnp.zeros_like(y)

    slot = lax.broadcasted_iota(jnp.int32, (256, CHUNK), 0) % 64
    place = lax.broadcasted_iota(jnp.int32, (256, CHUNK), 1) // 64

    def chunk_step(t, carry):
        spread = (slot == place + 8 * t).astype(F32).astype(BF16)
        load_state(t).wait()
        values = dot(xs[...], spread)
        wide = lambda ref: jnp.concatenate([ref[...]] * (CHUNK // 128), axis=1)
        fresh = wide(dec) * old[t] + values * wide(write)
        new[t] = fresh
        store_state(t).start()
        both = dot_nt(jnp.concatenate(split(fresh * wide(read)), axis=0), spread[0:128])
        y[...] += both[0:256] + both[256:512]
        return carry

    lax.fori_loop(0, CHUNKS, chunk_step, 0, unroll=4)

    for load in loads[14:18]:
        load.wait()
    carry[ROWS : ROWS + 1, 0:WIDTH] = channel_gain[...]
    carry[ROWS + 1 : ROWS + 2, 0:HALF] = mix[...]
    out_parts = []
    for n, (first, size) in enumerate(((0, WIDTH), (META, 256))):
        where = (pl.ds(0, ROWS + 8), pl.ds(first, size))
        out_parts.append(
            pltpu.make_async_copy(carry.at[where], carry_hbm.at[where], out_sems.at[n])
        )
    out_parts[0].start()
    out_parts[1].start()
    gate = silu(dot(normed, gate_w[...]).astype(BF16).astype(F32))
    pieces = []
    for j in range(HEADS // 2):
        even = y[pl.ds(2 * j, ROWS, stride=HEADS), :]
        odd = y[pl.ds(2 * j + 1, ROWS, stride=HEADS), :]
        gain = jnp.where(low_half, skip[2 * j], skip[2 * j + 1])
        cols = slice(128 * j, 128 * j + 128)
        pieces.append(
            (jnp.where(low_half, even, odd) + gain * conv[:, cols]) * gate[:, cols]
        )
    groups = [jnp.concatenate(pieces[2 * g : 2 * g + 2], axis=1) for g in range(2)]
    inner = jnp.concatenate([rms(g) for g in groups], axis=1) * inner_gain[...]
    loads[18].wait()
    partial[...] = dot(inner.astype(BF16), out_w[...]).astype(BF16)
    out_parts.append(pltpu.make_async_copy(partial, partial_hbm, out_sems.at[2]))
    out_parts[2].start()
    for part in out_parts:
        part.wait()
    for t in range(CHUNKS):
        store_state(t).wait()


def run_mixer(*given):
    hbm = pl.BlockSpec(memory_space=pltpu.HBM)
    lanes = lambda: VMEM((256, 128), F32)
    held = [
        (pltpu.SMEM if 5 <= n < 8 else VMEM)(v.shape, v.dtype)
        for n, v in enumerate(given[:19])
    ]
    return pl.pallas_call(
        mixer_kernel,
        out_shape=(
            jax.ShapeDtypeStruct((256, 4096), F32),
            jax.ShapeDtypeStruct((ROWS + 8, CARRY), F32),
            jax.ShapeDtypeStruct((ROWS, 2 * HALF), BF16),
        ),
        in_specs=[hbm] * 20,
        out_specs=(hbm, hbm, hbm),
        scratch_shapes=[
            *held,
            VMEM((CHUNKS, 256, CHUNK), F32),
            VMEM((CHUNKS, 256, CHUNK), F32),
            lanes(),
            lanes(),
            lanes(),
            VMEM((256, 256), BF16),
            lanes(),
            lanes(),
            VMEM((192, 128), F32),
            VMEM((ROWS + 8, CARRY), F32),
            VMEM((ROWS, 2 * HALF), BF16),
            pltpu.SemaphoreType.DMA((19,)),
            pltpu.SemaphoreType.DMA((2 * CHUNKS,)),
            pltpu.SemaphoreType.DMA((3,)),
        ],
        compiler_params=pltpu.CompilerParams(vmem_limit_bytes=67043328),
        name="mixer",
    )(*given)


def ffn_kernel(
    carry_hbm,
    partial_hbm,
    eg_hbm,
    eu_hbm,
    ed_hbm,
    dg_hbm,
    du_hbm,
    dd_hbm,
    out,
    x0,
    x1,
    x2,
    y0,
    y1,
    y2,
    s0,
    s1,
    s2,
    *rest,
):
    landed, rest = rest[:12], rest[12:]
    landing = [landed[3 * k : 3 * k + 3] for k in range(4)]
    (
    other_partial,
    wide,
    mid,
    eg,
    eu,
    ed,
    ed_other,
    dgu,
    dgu_other,
    dd,
    dd_scaled,
    packed,
    slot_weight,
    act,
    act_other,
    left_side,
    result,
    local_sem,
    ag_send,
    ag_recv,
    dd_send,
    dd_recv,
    rs_send,
    rs_recv,
    mi_send,
    mi_recv,
        carry,
        partial,
        gate_own,
        up_own,
        small_sem,
    ) = rest
    ep = lax.axis_index("ep")
    core = lax.axis_index("tp")
    coords = (ep // 16, (ep // 4) % 4, ep % 4)
    other = 1 - core
    own_cols = pl.multiple_of(core * HALF, HALF)
    other_cols = pl.multiple_of(other * HALF, HALF)
    expert = ep // 8
    mine = (x0, x1, x2)
    theirs = (y0, y1, y2)
    sums = (s0, s1, s2)

    def neighbour(dim, shift):
        moved = list(coords)
        moved[dim] = lax.rem(coords[dim] + shift, 4)
        return (moved[0] * 16 + moved[1] * 4 + moved[2], core)

    partner = (ep, other)

    small = [
        pltpu.make_async_copy(partial_hbm, partial, small_sem.at[0]),
        pltpu.make_async_copy(carry_hbm, carry, small_sem.at[1]),
    ]
    for load in small:
        load.start()
    barrier = pltpu.get_barrier_semaphore()
    for dim in range(3):
        for shift in (1, 2, 3):
            pl.semaphore_signal(
                barrier, inc=1, device_id=neighbour(dim, shift), device_id_type=MESH
            )
    pl.semaphore_signal(barrier, inc=1, device_id=partner, device_id_type=MESH)
    small[0].wait()
    pl.semaphore_wait(barrier, 10)

    def to_partner(src, dst, n):
        return pltpu.make_async_remote_copy(
            src_ref=src,
            dst_ref=dst,
            send_sem=mi_send.at[n],
            recv_sem=mi_recv.at[n],
            device_id=partner,
            device_id_type=MESH,
        )

    swap_partial = to_partner(partial, other_partial, 0)
    swap_partial.start()
    loads = [
        pltpu.make_async_copy(eg_hbm, eg.at[pl.ds(0, HIDDEN)], local_sem.at[0]),
        pltpu.make_async_copy(eu_hbm, eu.at[pl.ds(0, HIDDEN)], local_sem.at[1]),
        pltpu.make_async_copy(
            ed_hbm.at[:, pl.ds(own_cols, HALF)], ed.at[pl.ds(0, HIDDEN)], local_sem.at[2]
        ),
        pltpu.make_async_copy(dg_hbm, dgu.at[pl.ds(0, DENSE)], local_sem.at[3]),
        pltpu.make_async_copy(du_hbm, dgu.at[pl.ds(128, DENSE)], local_sem.at[4]),
        pltpu.make_async_copy(dd_hbm, dd, local_sem.at[5]),
    ]
    for load in loads:
        load.start()

    small[1].wait()
    swap_partial.wait()
    mixed = partial[...].astype(F32) + other_partial[...].astype(F32)
    hidden = carry[0:ROWS, 0:WIDTH] + mixed
    mid[...] = hidden
    wide[...] = (rms(hidden) * carry[ROWS : ROWS + 1, 0:WIDTH]).astype(BF16)
    here = coords
    for p in range(3):
        cols = pl.ds(pl.multiple_of(own_cols + STARTS[p], 128), WIDTHS[p])
        mine[p][here[0], here[1], here[2], 0:ROWS, :] = wide[:, cols]
    x2[here[0], here[1], here[2], ROWS : ROWS + 16, :] = carry[0:16, META : META + 256].astype(
        BF16
    )

    def cut(buf, p, where, half=None, rows=None):
        index = [None, None, None]
        for q in range(3):
            index[ORDERS[p][q]] = pl.ds(0, 4) if where[q] is None else where[q]
        if half is not None:
            free = sorted(ORDERS[p][q] for q in range(3) if where[q] is None)
            if free:
                index[free[0]] = pl.ds(2 * half, 2)
            else:
                rows = pl.ds(0, 16) if half == 0 else pl.ds(16, rows - 16)
        elif rows is not None:
            rows = pl.ds(0, rows)
        if rows is not None and not (half is not None and free):
            index.append(rows)
        return buf.at[tuple(index)]

    def turn(p, k, shift):
        return lax.rem(coords[ORDERS[p][k]] + shift, 4)

    ME, RIGHT, FAR, LEFT = 0, 1, 2, 3
    spots = [[[turn(p, k, shift) for shift in range(4)] for k in range(3)] for p in range(3)]

    class Ring:
        def __init__(self, p, k, at, place, direct=False):
            self.p, self.k, self.place, self.direct = p, k, place, direct
            self.copies = [self.copy(at, ME, None, 1), self.copy(at + 1, ME, None, 3)]
            if direct:
                self.copies.append(self.copy(at + 2, ME, None, 2))
            else:
                self.copies.append(self.copy(at + 2, LEFT, 0, 1))
                self.copies.append(self.copy(at + 3, RIGHT, 1, 3))

        def copy(self, at, shift, half, to):
            p = self.p
            where = list(self.place)
            where[self.k] = spots[p][self.k][shift]
            rows = BLOCK_ROWS[p] if half is not None else None
            ref = cut(mine[p], p, where, half, rows)
            return pltpu.make_async_remote_copy(
                src_ref=ref,
                dst_ref=ref,
                send_sem=ag_send.at[at],
                recv_sem=ag_recv.at[at],
                device_id=neighbour(ORDERS[p][self.k], to),
                device_id_type=MESH,
            )

        def start(self):
            if self.direct:
                self.copies[2].start()
            self.copies[0].start()
            self.copies[1].start()

        def on(self):
            self.copies[0].wait_recv()
            if not self.direct:
                self.copies[2].start()
            self.copies[1].wait_recv()
            if not self.direct:
                self.copies[3].start()

        def end(self):
            for copy in self.copies[2:]:
                copy.wait_recv()

    first, second, third_way = [], [], []
    for p in range(3):
        at = 84 * p
        own = [spots[p][k][ME] for k in range(3)]
        first.append(Ring(p, 0, at, own, True))
        second.append(
            [Ring(p, 1, at + 4 + 4 * u, [spots[p][0][u], None, own[2]], True) for u in range(4)]
        )
        third_way.append(
            [
                [
                    Ring(
                        p,
                        2,
                        at + 20 + 16 * u + 4 * v,
                        [spots[p][0][u], spots[p][1][v], None],
                        FAR in (u, v) and ME not in (u, v),
                    )
                    for v in range(4)
                ]
                for u in range(4)
            ]
        )
    rings = [first] + second + [row for part in third_way for row in part]
    hand_overs = []

    def hand_over(p, n, second_at, third_at):
        where = [None, second_at, third_at]
        copy = pltpu.make_async_remote_copy(
            src_ref=cut(mine[p], p, where, None, ROWS),
            dst_ref=cut(theirs[p], p, where, None, ROWS),
            send_sem=dd_send.at[13 * p + n],
            recv_sem=dd_recv.at[13 * p + n],
            device_id=partner,
            device_id_type=MESH,
        )
        copy.start()
        hand_overs.append(copy)

    parts = range(3)
    def launch(*pairs):
        for p in parts:
            for u, v in pairs:
                third_way[p][u][v].start()

    def pass_on(*pairs):
        for p in parts:
            for u, v in pairs:
                third_way[p][u][v].on()

    for p in parts:
        first[p].start()
    for p in parts:
        second[p][ME].start()
    launch((ME, ME))

    early = [
        to_partner(
            ed_hbm.at[:, pl.ds(other_cols, HALF)], ed_other.at[pl.ds(0, HIDDEN)], 1
        ),
        to_partner(dg_hbm, dgu_other.at[pl.ds(0, DENSE)], 2),
        to_partner(du_hbm, dgu_other.at[pl.ds(128, DENSE)], 3),
    ]
    for copy in early:
        copy.start()

    for p in parts:
        first[p].on()
        for u in (LEFT, RIGHT):
            second[p][u].start()
            third_way[p][u][ME].start()
    for p in parts:
        second[p][ME].on()
    launch((ME, RIGHT), (ME, LEFT))
    for p in parts:
        first[p].end()
        second[p][FAR].start()
        third_way[p][FAR][ME].start()
    for p in parts:
        second[p][ME].end()
    launch((ME, FAR))
    pass_on((ME, ME))
    for ref in (eg, eu, ed, ed_other):
        ref[HIDDEN:HPAD, :] = jnp.zeros((HPAD - HIDDEN, ref.shape[1]), BF16)
    for ref in (dgu, dgu_other):
        ref[DENSE:128, :] = jnp.zeros((128 - DENSE, HALF), BF16)
        ref[128 + DENSE : 256, :] = jnp.zeros((128 - DENSE, HALF), BF16)
    dd_scaled[DENSE:128, :] = jnp.zeros((128 - DENSE, HALF), BF16)
    for g in range(GROUPS):
        result[g, SLOTS:128, :] = jnp.zeros((128 - SLOTS, HALF), BF16)
    for p in parts:
        second[p][LEFT].on()
        second[p][RIGHT].on()
    launch((LEFT, RIGHT), (RIGHT, RIGHT), (LEFT, LEFT), (RIGHT, LEFT))
    pass_on((LEFT, ME), (RIGHT, ME), (ME, RIGHT), (ME, LEFT))
    for p in parts:
        second[p][LEFT].end()
        second[p][RIGHT].end()
    launch((LEFT, FAR), (RIGHT, FAR))
    for p in parts:
        second[p][FAR].on()
    launch((FAR, RIGHT), (FAR, LEFT))
    for p in parts:
        second[p][FAR].end()
    launch((FAR, FAR))
    pass_on((FAR, ME), (ME, FAR))
    for p in parts:
        hand_over(p, 0, None, spots[p][2][ME])
        hand_over(p, 1, spots[p][1][ME], spots[p][2][LEFT])
        hand_over(p, 2, spots[p][1][ME], spots[p][2][RIGHT])

    def finish(v, n):
        for p in parts:
            for u in range(4):
                third_way[p][u][v].end()
            hand_over(p, n, spots[p][1][v], spots[p][2][FAR])

    def sides(v, n):
        for p in parts:
            hand_over(p, n, spots[p][1][v], spots[p][2][LEFT])
            hand_over(p, n + 1, spots[p][1][v], spots[p][2][RIGHT])

    pass_on((LEFT, RIGHT), (RIGHT, RIGHT), (LEFT, LEFT), (RIGHT, LEFT))
    finish(ME, 3)
    pass_on((LEFT, FAR), (RIGHT, FAR), (FAR, RIGHT), (FAR, LEFT))
    sides(RIGHT, 4)
    sides(LEFT, 6)
    pass_on((FAR, FAR))
    sides(FAR, 8)
    finish(RIGHT, 10)
    finish(LEFT, 11)
    finish(FAR, 12)
    pick_row = lax.broadcasted_iota(jnp.int32, (128, 128), 0)
    pick_rank = (pick_row == expert).astype(F32).astype(BF16)
    pick_weight = (
        jnp.logical_or(pick_row == expert + 8, pick_row == expert + 16)
    ).astype(F32).astype(BF16)
    lane = lax.broadcasted_iota(jnp.int32, (GROUP_ROWS, 128), 1)
    source = lax.broadcasted_iota(jnp.int32, (GROUP_ROWS, 128), 0) // ROWS

    def group_of(bufs, g):
        z, y = g // 2, 2 * lax.rem(g, 2)
        return jnp.concatenate(
            [
                bufs[p][z, pl.ds(y, 2), :, 0:ROWS, :].reshape(GROUP_ROWS, WIDTHS[p])
                for p in range(3)
            ],
            axis=1,
        )

    def pack_group(g, carry):
        z, y = g // 2, 2 * lax.rem(g, 2)
        tags = x2[z, pl.ds(y, 2), :, ROWS : ROWS + 16, :].reshape(8, 16, 256)
        tags = jnp.concatenate([tags[:, :, 0:128], tags[:, :, 128:256]], axis=1)
        tags = tags.reshape(GROUP_ROWS, 128)
        rank = dot(tags, pick_rank).astype(jnp.int32)
        hit = jnp.logical_and(rank > 0, rank + (CAP * source - 1) == lane)
        table = hit.astype(F32).astype(BF16)
        left_side[g, :, 0:128] = table
        used = table[:, 0:SLOTS]
        slots = pl.ds(pl.multiple_of(g * SLOTS, SLOTS), SLOTS)
        packed[slots, pl.ds(own_cols, HALF)] = dot_tn(used, group_of(mine, g)).astype(BF16)
        slot_tags = dot_tn(used, tags).astype(BF16)
        slot_weight[slots, :] = dot(slot_tags, pick_weight)
        return carry

    lax.fori_loop(0, GROUPS, pack_group, 0, unroll=8)
    for load in loads:
        load.wait()
    own = pl.ds(own_cols, HALF)
    rest_cols = pl.ds(other_cols, HALF)
    for i in range(2):
        units = pl.ds(256 * i, 256)
        gate_own[:, units] = dot_nt(packed[:, own], eg[units, own])
        up_own[:, units] = dot_nt(packed[:, own], eu[units, own])
    for copy in early:
        copy.wait()
    for copy in hand_overs:
        copy.wait()

    def pack_other(g, carry):
        used = left_side[g, :, 0:SLOTS]
        slots = pl.ds(pl.multiple_of(g * SLOTS, SLOTS), SLOTS)
        packed[slots, pl.ds(other_cols, HALF)] = dot_tn(used, group_of(theirs, g)).astype(
            BF16
        )
        return carry

    lax.fori_loop(0, GROUPS, pack_other, 0, unroll=8)

    sends = []
    for i in range(2):
        units = pl.ds(256 * i, 256)
        gate = gate_own[:, units] + dot_nt(packed[:, rest_cols], eg[units, rest_cols])
        up = up_own[:, units] + dot_nt(packed[:, rest_cols], eu[units, rest_cols])
        act[:, units] = (silu(gate) * up * slot_weight[:, 0:1]).astype(BF16)
        copy = to_partner(act.at[:, units], act_other.at[:, units], 4 + i)
        copy.start()
        sends.append(copy)

    def dense_group(g, carry):
        both = dot_nt(group_of(mine, g), dgu[...]) + dot_nt(group_of(theirs, g), dgu_other[...])
        left_side[g, :, 128:256] = (silu(both[:, 0:128]) * both[:, 128:256]).astype(BF16)
        return carry

    lax.fori_loop(0, GROUPS, dense_group, 0, unroll=8)
    share = 1.0 / (1.0 + jnp.exp(-carry[ROWS + 1 : ROWS + 2, 0:HALF]))
    dd_scaled[0:DENSE, :] = (dd[...].astype(F32) * share).astype(BF16)

    class Back:
        def __init__(self, p, k, at, place, slot):
            self.p, self.k, self.place, self.slot = p, k, place, slot
            self.halves, self.wholes = landing[0][p], landing[1][p]
            self.copies = [
                self.copy(at, FAR, 0, 1, self.halves.at[slot, 0]),
                self.copy(at + 1, FAR, 1, 3, self.halves.at[slot, 1]),
                self.copy(at + 2, RIGHT, None, 1, self.wholes.at[slot, 0]),
                self.copy(at + 3, LEFT, None, 3, self.wholes.at[slot, 1]),
            ]

        def spot(self, shift):
            where = list(self.place)
            where[self.k] = spots[self.p][self.k][shift]
            return where

        def copy(self, at, shift, half, to, target):
            p = self.p
            rows = ROWS if half is not None else None
            return pltpu.make_async_remote_copy(
                src_ref=cut(sums[p], p, self.spot(shift), half, rows),
                dst_ref=target,
                send_sem=rs_send.at[at],
                recv_sem=rs_recv.at[at],
                device_id=neighbour(ORDERS[p][self.k], to),
                device_id_type=MESH,
            )

        def start(self):
            self.copies[0].start()
            self.copies[1].start()

        def add_half(self, shift, half):
            p, got = self.p, self.halves
            where = self.spot(shift)
            place = [None, None, None]
            for q in range(3):
                place[ORDERS[p][q]] = where[q]
            free = [d for d in range(3) if place[d] is None]
            for t in range(2):
                place[free[0]] = 2 * half + t
                ref = sums[p].at[tuple(place)]
                ref[...] = ref[...] + got[self.slot, half, t]

        def on(self):
            self.copies[0].wait_recv()
            self.add_half(RIGHT, 0)
            self.copies[2].start()
            self.copies[1].wait_recv()
            self.add_half(LEFT, 1)
            self.copies[3].start()

        def end(self):
            p, got = self.p, self.wholes
            self.copies[2].wait_recv()
            self.copies[3].wait_recv()
            where = self.spot(ME)
            place = [None, None, None]
            for q in range(3):
                place[ORDERS[p][q]] = where[q]
            free = [d for d in range(3) if place[d] is None]
            for t in range(4):
                place[free[0]] = t
                ref = sums[p].at[tuple(place)]
                total = ref[...].astype(F32) + got[self.slot, 0, t].astype(F32)
                ref[...] = (total + got[self.slot, 1, t].astype(F32)).astype(BF16)

    class Straight:
        def __init__(self, p, k, at, place):
            self.p, self.k, self.place, self.wholes = p, k, place, landing[2 + k][p]
            self.copies = [self.copy(at + u - 1, u) for u in (RIGHT, FAR, LEFT)]

        def copy(self, at, u):
            p = self.p
            where = list(self.place)
            where[self.k] = spots[p][self.k][u]
            return pltpu.make_async_remote_copy(
                src_ref=cut(sums[p], p, where),
                dst_ref=self.wholes.at[u - 1],
                send_sem=rs_send.at[at],
                recv_sem=rs_recv.at[at],
                device_id=neighbour(ORDERS[p][self.k], u),
                device_id_type=MESH,
            )

        def send(self, u):
            self.copies[u - 1].start()

        def arrive(self):
            for copy in self.copies:
                copy.wait_recv()

        def add(self, first_at):
            p, got = self.p, self.wholes
            place = [None, None, None]
            for q in range(3):
                place[ORDERS[p][q]] = spots[p][q][ME]
            place[ORDERS[p][0]] = first_at
            ref = sums[p].at[tuple(place)]
            total = ref[...].astype(F32)
            for n in range(3):
                total = total + got[n, first_at].astype(F32)
            ref[...] = total.astype(BF16)

    third, middle, last = [], [], []
    for p in parts:
        at = 24 * p
        own = [spots[p][k][ME] for k in range(3)]
        third.append(
            [Back(p, 2, at + 4 * u, [None, spots[p][1][u], None], u) for u in range(4)]
        )
        middle.append(Straight(p, 1, at + 16, [None, None, own[2]]))
        last.append(Straight(p, 0, at + 20, own))
    order = (FAR, LEFT, RIGHT, ME)
    for send in sends:
        send.wait()
    for p in parts:
        cols = slice(STARTS[p], STARTS[p] + WIDTHS[p])
        for n in ((0, 1), (2,), (3,))[p]:
            some = slice(256 * n, 256 * n + 256)
            back = dot(act[...], ed[:, some]) + dot(act_other[...], ed_other[:, some])
            result[:, 0:SLOTS, some] = back.astype(BF16).reshape(GROUPS, SLOTS, 256)

        def spread_group(g, carry):
            z, y = g // 2, 2 * lax.rem(g, 2)
            right_side = jnp.concatenate([result[g, :, cols], dd_scaled[:, cols]], axis=0)
            total = dot(left_side[g], right_side).astype(BF16)
            sums[p][z, pl.ds(y, 2)] = total.reshape(2, 4, ROWS, WIDTHS[p])
            return carry

        lax.fori_loop(0, GROUPS, spread_group, 0, unroll=8)
        for u in order:
            third[p][u].start()
    for u in order:
        for p in parts:
            third[p][u].on()
    for u in order:
        for p in parts:
            third[p][u].end()
            if u != ME:
                middle[p].send(u)
    for p in parts:
        middle[p].arrive()
        for u in order:
            middle[p].add(spots[p][0][u])
            if u != ME:
                last[p].send(u)
    for p in parts:
        last[p].arrive()
        got = last[p].wholes
        total = mid[:, pl.ds(pl.multiple_of(own_cols + STARTS[p], 128), WIDTHS[p])]
        total = total + sums[p][here[0], here[1], here[2]].astype(F32)
        for n in range(3):
            total = total + got[n].astype(F32)
        out[:, STARTS[p] : STARTS[p] + WIDTHS[p]] = total.astype(BF16)
    for group in third + [middle, last] + rings:
        for sender in group:
            for copy in sender.copies:
                copy.wait_send()


def run_ffn(carry, partial, eg, eu, ed, dg, du, dd):
    vmem = pl.BlockSpec(memory_space=VMEM)
    hbm = pl.BlockSpec(memory_space=pltpu.HBM)
    blocks = lambda *lead: [VMEM((*lead, WIDTHS[p]), BF16) for p in range(3)]
    sem = pltpu.SemaphoreType.DMA
    return pl.pallas_call(
        ffn_kernel,
        out_shape=jax.ShapeDtypeStruct((ROWS, HALF), BF16),
        in_specs=[hbm] * 8,
        out_specs=vmem,
        scratch_shapes=[
            *[VMEM((4, 4, 4, BLOCK_ROWS[p], WIDTHS[p]), BF16) for p in range(3)],
            *blocks(4, 4, 4, ROWS),
            *blocks(4, 4, 4, ROWS),
            *blocks(4, 2, 2, ROWS),
            *blocks(4, 2, 4, ROWS),
            *blocks(3, ROWS),
            *blocks(3, 4, ROWS),
            VMEM((ROWS, 2 * HALF), BF16),
            VMEM((ROWS, 2 * HALF), BF16),
            VMEM((ROWS, 2 * HALF), F32),
            VMEM((HPAD, 2 * HALF), BF16),
            VMEM((HPAD, 2 * HALF), BF16),
            VMEM((HPAD, HALF), BF16),
            VMEM((HPAD, HALF), BF16),
            VMEM((256, HALF), BF16),
            VMEM((256, HALF), BF16),
            VMEM((DENSE, HALF), BF16),
            VMEM((128, HALF), BF16),
            VMEM((GROUPS * SLOTS, 2 * HALF), BF16),
            VMEM((GROUPS * SLOTS, 128), F32),
            VMEM((GROUPS * SLOTS, HPAD), BF16),
            VMEM((GROUPS * SLOTS, HPAD), BF16),
            VMEM((GROUPS, GROUP_ROWS, 256), BF16),
            VMEM((GROUPS, 128, HALF), BF16),
            sem((6,)),
            sem((252,)),
            sem((252,)),
            sem((39,)),
            sem((39,)),
            sem((72,)),
            sem((72,)),
            sem((6,)),
            sem((6,)),
            VMEM((ROWS + 8, CARRY), F32),
            VMEM((ROWS, 2 * HALF), BF16),
            VMEM((GROUPS * SLOTS, HPAD), F32),
            VMEM((GROUPS * SLOTS, HPAD), F32),
            sem((2,)),
        ],
        compiler_params=pltpu.CompilerParams(
            collective_id=0, has_side_effects=True, vmem_limit_bytes=67043328
        ),
        name="ffn",
    )(carry, partial, eg, eu, ed, dg, du, dd)


def local(
    stream,
    mixer_gain,
    gate_proj,
    input_proj,
    state_maps,
    step_proj,
    step_bias,
    decay_rate,
    input_taps,
    map_taps,
    input_past,
    map_past,
    head_state,
    skip_gain,
    inner_gain,
    mixer_out,
    channel_gain,
    expert_ids,
    expert_weight,
    expert_gate,
    expert_up,
    expert_down,
    dense_gate,
    dense_up,
    dense_down,
    dense_mix,
):
    state_out, carry, partial = run_mixer(
        stream,
        mixer_gain.reshape(1, -1),
        step_proj.T,
        expert_ids.T,
        expert_weight.T,
        step_bias,
        decay_rate,
        skip_gain,
        input_proj,
        input_taps,
        jnp.transpose(input_past, (1, 0, 2)),
        state_maps,
        map_taps,
        jnp.transpose(map_past, (0, 2, 1, 3)).reshape(192, 128),
        inner_gain.reshape(1, -1),
        gate_proj,
        channel_gain.reshape(1, -1),
        dense_mix.reshape(1, -1),
        mixer_out,
        head_state.reshape(256, 4096),
    )
    out = run_ffn(
        carry,
        partial,
        expert_gate.T,
        expert_up.T,
        expert_down,
        dense_gate.T,
        dense_up.T,
        dense_down,
    )
    return out, state_out.reshape(head_state.shape)


def solution(mesh):
    placed = (
        P("ep", None),
        P(),
        P(None, "tp"),
        P(None, "tp"),
        P(None, None, "tp"),
        P(None, "tp"),
        P("tp"),
        P("tp"),
        P(None, "tp"),
        P(None, None, "tp"),
        P("ep", None, "tp"),
        P("ep", None, None, "tp"),
        P("ep", "tp", None),
        P("tp"),
        P("tp"),
        P("tp", None),
        P(),
        P("ep", None),
        P("ep", None),
        P(None, ("ep", "tp")),
        P(None, ("ep", "tp")),
        P(("ep", "tp"), None),
        P("tp", "ep"),
        P("tp", "ep"),
        P("ep", "tp"),
        P("tp"),
    )
    return jax.shard_map(
        local,
        mesh=mesh,
        in_specs=placed,
        out_specs=(P("ep", "tp"), P("ep", "tp", None)),
        check_vma=False,
    )
```

```python
import functools

import jax
import jax.numpy as jnp
from jax import lax
from jax.experimental import pallas as pl
from jax.experimental.pallas import tpu as pltpu
from jax.sharding import PartitionSpec as P

EPS = 1e-06
MESH = pl.DeviceIdType.MESH
F32 = jnp.float32
BF16 = jnp.bfloat16
VMEM = pltpu.VMEM
ANY = pl.ANY

HEADS = 8
ROWS = 32
EXPERTS = 8
CAP = 12
CHUNKS = 8
CHUNK = 512
GROUPS = 8
GROUP_ROWS = 256
SLOTS = 96
HALF = 1024
HIDDEN = 448
HPAD = 512
DENSE = 88
WIDTH = 2048
META = 2048
CARRY = 2304

WIDTHS = (384, 384, 256)
STARTS = (0, 384, 768)
BLOCK_ROWS = (32, 32, 48)
ORDERS = ((2, 1, 0), (1, 0, 2), (0, 2, 1))


def dot(a, b):
    return jnp.dot(a, b, preferred_element_type=F32)


def dot_nt(a, b):
    return lax.dot_general(a, b, (((1,), (1,)), ((), ())), preferred_element_type=F32)


def dot_tn(a, b):
    return lax.dot_general(a, b, (((0,), (0,)), ((), ())), preferred_element_type=F32)


def silu(v):
    return v / (1.0 + jnp.exp(-v))


def rms(v):
    return v * lax.rsqrt(jnp.mean(v * v, axis=-1, keepdims=True) + EPS)


def split(v):
    high = v.astype(BF16)
    return high, (v - high.astype(F32)).astype(BF16)


def mixer_kernel(*refs):
    given, refs = refs[:20], refs[20:]
    state_hbm = given[19]
    state_out, carry_hbm, partial_hbm = refs[:3]
    held, refs = refs[3:22], refs[22:]
    (
        stream,
        mixer_gain,
        step_t,
        ids,
        weights,
        bias,
        decay,
        skip,
        input_w,
        input_taps,
        input_past,
        maps_w,
        map_taps,
        map_past,
        inner_gain,
        gate_w,
        channel_gain,
        mix,
        out_w,
    ) = held
    old, new, dec, write, read, xs, tmp, y, past, carry, partial, in_sems, sems, out_sems = refs
    loads = [
        pltpu.make_async_copy(src, dst, in_sems.at[n])
        for n, (src, dst) in enumerate(zip(given, held))
    ]

    def load_state(t):
        cols = pl.ds(pl.multiple_of(t * CHUNK, CHUNK), CHUNK)
        return pltpu.make_async_copy(state_hbm.at[:, cols], old.at[t], sems.at[t])

    def store_state(t):
        cols = pl.ds(pl.multiple_of(t * CHUNK, CHUNK), CHUNK)
        return pltpu.make_async_copy(
            new.at[t], state_out.at[:, cols], sems.at[CHUNKS + t]
        )

    for load in loads[:15]:
        load.start()
    for t in range(CHUNKS):
        load_state(t).start()
    for load in loads[15:]:
        load.start()

    for load in loads[:8]:
        load.wait()
    normed = (rms(stream[...].astype(F32)) * mixer_gain[...]).astype(BF16)
    steps = dot_nt(normed, step_t[...])

    expert_of = lax.broadcasted_iota(jnp.int32, (EXPERTS, ROWS), 0)
    hit0 = (ids[0:1, :] == expert_of).astype(F32)
    hit1 = (ids[1:2, :] == expert_of).astype(F32)
    member = hit0 + hit1
    upper = (
        lax.broadcasted_iota(jnp.int32, (ROWS, ROWS), 0)
        <= lax.broadcasted_iota(jnp.int32, (ROWS, ROWS), 1)
    ).astype(BF16)
    rank = dot(member.astype(BF16), upper) * member
    weight = hit0 * weights[0:1, :] + hit1 * weights[1:2, :]
    w_high = weight.astype(BF16).astype(F32)
    w_low = weight - w_high
    table = jnp.concatenate(
        [rank, w_high, w_low, jnp.zeros((104, ROWS), F32)], axis=0
    ).astype(BF16)
    eye = (
        lax.broadcasted_iota(jnp.int32, (ROWS, ROWS), 0)
        == lax.broadcasted_iota(jnp.int32, (ROWS, ROWS), 1)
    ).astype(BF16)
    by_row = dot_nt(eye, table)
    carry[0:16, META : META + 256] = jnp.concatenate([by_row[0:16], by_row[16:32]], axis=1)
    carry[0:ROWS, 0:WIDTH] = stream[...].astype(F32)

    for load in loads[8:11]:
        load.wait()
    newest = dot(normed, input_w[...]).astype(BF16).astype(F32)
    conv = newest * input_taps[3:4, :]
    for t in range(3):
        conv = conv + input_past[t].astype(F32) * input_taps[t : t + 1, :]
    conv = silu(conv)

    for load in loads[11:14]:
        load.wait()
    past[...] = map_past[...].astype(F32)
    conv_maps = []
    for m in range(2):
        new_map = dot(normed, maps_w[m]).astype(BF16).astype(F32)
        acc = new_map * map_taps[m, 3:4, :]
        for t in range(3):
            acc = acc + past[pl.ds(2 * t + m, ROWS, stride=6), :] * map_taps[m, t : t + 1, :]
        conv_maps.append(silu(acc))

    lane = lax.broadcasted_iota(jnp.int32, (ROWS, 128), 1)
    low_half = lane < 64

    def both_halves(v):
        turned = pltpu.roll(v, 64, 1)
        return jnp.where(low_half, v, turned), jnp.where(low_half, turned, v)

    write_by_group = both_halves(conv_maps[0])
    read_by_group = both_halves(conv_maps[1])
    for h in range(HEADS):
        rows = pl.ds(h, ROWS, stride=HEADS)
        v = jnp.broadcast_to(steps[:, h : h + 1], (ROWS, 128)) + bias[h]
        step = jnp.maximum(v, 0.0) + jnp.log1p(jnp.exp(-jnp.abs(v)))
        dec[rows, :] = jnp.exp(-decay[h] * step)
        pair = conv[:, 128 * (h // 2) : 128 * (h // 2) + 128]
        mine = low_half if h % 2 == 0 else jnp.logical_not(low_half)
        tmp[rows, :] = jnp.where(mine, step * pair, 0.0)
        write[rows, :] = write_by_group[h // 4]
        read[rows, :] = read_by_group[h // 4]
    high, low = split(tmp[...])
    xs[:, 0:128] = high
    xs[:, 128:256] = low
    y[...] = jnp.zeros_like(y)

    slot = lax.broadcasted_iota(jnp.int32, (256, CHUNK), 0) % 64
    place = lax.broadcasted_iota(jnp.int32, (256, CHUNK), 1) // 64

    def chunk_step(t, carry):
        spread = (slot == place + 8 * t).astype(F32).astype(BF16)
        load_state(t).wait()
        values = dot(xs[...], spread)
        wide = lambda ref: jnp.concatenate([ref[...]] * (CHUNK // 128), axis=1)
        fresh = wide(dec) * old[t] + values * wide(write)
        new[t] = fresh
        store_state(t).start()
        both = dot_nt(jnp.concatenate(split(fresh * wide(read)), axis=0), spread[0:128])
        y[...] += both[0:256] + both[256:512]
        return carry

    lax.fori_loop(0, CHUNKS, chunk_step, 0, unroll=4)

    for load in loads[14:18]:
        load.wait()
    carry[ROWS : ROWS + 1, 0:WIDTH] = channel_gain[...]
    carry[ROWS + 1 : ROWS + 2, 0:HALF] = mix[...]
    out_parts = []
    for n, (first, size) in enumerate(((0, WIDTH), (META, 256))):
        where = (pl.ds(0, ROWS + 8), pl.ds(first, size))
        out_parts.append(
            pltpu.make_async_copy(carry.at[where], carry_hbm.at[where], out_sems.at[n])
        )
    out_parts[0].start()
    out_parts[1].start()
    gate = silu(dot(normed, gate_w[...]).astype(BF16).astype(F32))
    pieces = []
    for j in range(HEADS // 2):
        even = y[pl.ds(2 * j, ROWS, stride=HEADS), :]
        odd = y[pl.ds(2 * j + 1, ROWS, stride=HEADS), :]
        gain = jnp.where(low_half, skip[2 * j], skip[2 * j + 1])
        cols = slice(128 * j, 128 * j + 128)
        pieces.append(
            (jnp.where(low_half, even, odd) + gain * conv[:, cols]) * gate[:, cols]
        )
    groups = [jnp.concatenate(pieces[2 * g : 2 * g + 2], axis=1) for g in range(2)]
    inner = jnp.concatenate([rms(g) for g in groups], axis=1) * inner_gain[...]
    loads[18].wait()
    partial[...] = dot(inner.astype(BF16), out_w[...]).astype(BF16)
    out_parts.append(pltpu.make_async_copy(partial, partial_hbm, out_sems.at[2]))
    out_parts[2].start()
    for part in out_parts:
        part.wait()
    for t in range(CHUNKS):
        store_state(t).wait()


def run_mixer(*given):
    hbm = pl.BlockSpec(memory_space=pltpu.HBM)
    lanes = lambda: VMEM((256, 128), F32)
    held = [
        (pltpu.SMEM if 5 <= n < 8 else VMEM)(v.shape, v.dtype)
        for n, v in enumerate(given[:19])
    ]
    return pl.pallas_call(
        mixer_kernel,
        out_shape=(
            jax.ShapeDtypeStruct((256, 4096), F32),
            jax.ShapeDtypeStruct((ROWS + 8, CARRY), F32),
            jax.ShapeDtypeStruct((ROWS, 2 * HALF), BF16),
        ),
        in_specs=[hbm] * 20,
        out_specs=(hbm, hbm, hbm),
        scratch_shapes=[
            *held,
            VMEM((CHUNKS, 256, CHUNK), F32),
            VMEM((CHUNKS, 256, CHUNK), F32),
            lanes(),
            lanes(),
            lanes(),
            VMEM((256, 256), BF16),
            lanes(),
            lanes(),
            VMEM((192, 128), F32),
            VMEM((ROWS + 8, CARRY), F32),
            VMEM((ROWS, 2 * HALF), BF16),
            pltpu.SemaphoreType.DMA((19,)),
            pltpu.SemaphoreType.DMA((2 * CHUNKS,)),
            pltpu.SemaphoreType.DMA((3,)),
        ],
        compiler_params=pltpu.CompilerParams(vmem_limit_bytes=67043328),
        name="mixer",
    )(*given)


def ffn_kernel(
    carry_hbm,
    partial_hbm,
    eg_hbm,
    eu_hbm,
    ed_hbm,
    dg_hbm,
    du_hbm,
    dd_hbm,
    out,
    x0,
    x1,
    x2,
    y0,
    y1,
    y2,
    s0,
    s1,
    s2,
    *rest,
):
    landed, rest = rest[:12], rest[12:]
    landing = [landed[3 * k : 3 * k + 3] for k in range(4)]
    (
    other_partial,
    wide,
    mid,
    eg,
    eu,
    ed,
    ed_other,
    dgu,
    dgu_other,
    dd,
    dd_scaled,
    packed,
    slot_weight,
    act,
    act_other,
    left_side,
    result,
    local_sem,
    ag_send,
    ag_recv,
    dd_send,
    dd_recv,
    rs_send,
    rs_recv,
    mi_send,
    mi_recv,
        carry,
        partial,
        small_sem,
    ) = rest
    ep = lax.axis_index("ep")
    core = lax.axis_index("tp")
    coords = (ep // 16, (ep // 4) % 4, ep % 4)
    other = 1 - core
    own_cols = pl.multiple_of(core * HALF, HALF)
    other_cols = pl.multiple_of(other * HALF, HALF)
    expert = ep // 8
    mine = (x0, x1, x2)
    theirs = (y0, y1, y2)
    sums = (s0, s1, s2)

    def neighbour(dim, shift):
        moved = list(coords)
        moved[dim] = lax.rem(coords[dim] + shift, 4)
        return (moved[0] * 16 + moved[1] * 4 + moved[2], core)

    partner = (ep, other)

    small = [
        pltpu.make_async_copy(partial_hbm, partial, small_sem.at[0]),
        pltpu.make_async_copy(carry_hbm, carry, small_sem.at[1]),
    ]
    for load in small:
        load.start()
    barrier = pltpu.get_barrier_semaphore()
    for dim in range(3):
        for shift in (1, 2, 3):
            pl.semaphore_signal(
                barrier, inc=1, device_id=neighbour(dim, shift), device_id_type=MESH
            )
    pl.semaphore_signal(barrier, inc=1, device_id=partner, device_id_type=MESH)
    small[0].wait()
    pl.semaphore_wait(barrier, 10)

    def to_partner(src, dst, n):
        return pltpu.make_async_remote_copy(
            src_ref=src,
            dst_ref=dst,
            send_sem=mi_send.at[n],
            recv_sem=mi_recv.at[n],
            device_id=partner,
            device_id_type=MESH,
        )

    swap_partial = to_partner(partial, other_partial, 0)
    swap_partial.start()
    loads = [
        pltpu.make_async_copy(eg_hbm, eg.at[pl.ds(0, HIDDEN)], local_sem.at[0]),
        pltpu.make_async_copy(eu_hbm, eu.at[pl.ds(0, HIDDEN)], local_sem.at[1]),
        pltpu.make_async_copy(
            ed_hbm.at[:, pl.ds(own_cols, HALF)], ed.at[pl.ds(0, HIDDEN)], local_sem.at[2]
        ),
        pltpu.make_async_copy(dg_hbm, dgu.at[pl.ds(0, DENSE)], local_sem.at[3]),
        pltpu.make_async_copy(du_hbm, dgu.at[pl.ds(128, DENSE)], local_sem.at[4]),
        pltpu.make_async_copy(dd_hbm, dd, local_sem.at[5]),
    ]
    for load in loads:
        load.start()

    small[1].wait()
    swap_partial.wait()
    mixed = partial[...].astype(F32) + other_partial[...].astype(F32)
    hidden = carry[0:ROWS, 0:WIDTH] + mixed
    mid[...] = hidden
    wide[...] = (rms(hidden) * carry[ROWS : ROWS + 1, 0:WIDTH]).astype(BF16)
    here = coords
    for p in range(3):
        cols = pl.ds(pl.multiple_of(own_cols + STARTS[p], 128), WIDTHS[p])
        mine[p][here[0], here[1], here[2], 0:ROWS, :] = wide[:, cols]
    x2[here[0], here[1], here[2], ROWS : ROWS + 16, :] = carry[0:16, META : META + 256].astype(
        BF16
    )

    def cut(buf, p, where, half=None, rows=None):
        index = [None, None, None]
        for q in range(3):
            index[ORDERS[p][q]] = pl.ds(0, 4) if where[q] is None else where[q]
        if half is not None:
            free = sorted(ORDERS[p][q] for q in range(3) if where[q] is None)
            if free:
                index[free[0]] = pl.ds(2 * half, 2)
            else:
                rows = pl.ds(0, 16) if half == 0 else pl.ds(16, rows - 16)
        elif rows is not None:
            rows = pl.ds(0, rows)
        if rows is not None and not (half is not None and free):
            index.append(rows)
        return buf.at[tuple(index)]

    def turn(p, k, shift):
        return lax.rem(coords[ORDERS[p][k]] + shift, 4)

    ME, RIGHT, FAR, LEFT = 0, 1, 2, 3
    spots = [[[turn(p, k, shift) for shift in range(4)] for k in range(3)] for p in range(3)]

    class Ring:
        def __init__(self, p, k, at, place, direct=False):
            self.p, self.k, self.place, self.direct = p, k, place, direct
            self.copies = [self.copy(at, ME, None, 1), self.copy(at + 1, ME, None, 3)]
            if direct:
                self.copies.append(self.copy(at + 2, ME, None, 2))
            else:
                self.copies.append(self.copy(at + 2, LEFT, 0, 1))
                self.copies.append(self.copy(at + 3, RIGHT, 1, 3))

        def copy(self, at, shift, half, to):
            p = self.p
            where = list(self.place)
            where[self.k] = spots[p][self.k][shift]
            rows = BLOCK_ROWS[p] if half is not None else None
            ref = cut(mine[p], p, where, half, rows)
            return pltpu.make_async_remote_copy(
                src_ref=ref,
                dst_ref=ref,
                send_sem=ag_send.at[at],
                recv_sem=ag_recv.at[at],
                device_id=neighbour(ORDERS[p][self.k], to),
                device_id_type=MESH,
            )

        def start(self):
            if self.direct:
                self.copies[2].start()
            self.copies[0].start()
            self.copies[1].start()

        def on(self):
            self.copies[0].wait_recv()
            if not self.direct:
                self.copies[2].start()
            self.copies[1].wait_recv()
            if not self.direct:
                self.copies[3].start()

        def end(self):
            for copy in self.copies[2:]:
                copy.wait_recv()

    first, second, third_way = [], [], []
    for p in range(3):
        at = 84 * p
        own = [spots[p][k][ME] for k in range(3)]
        first.append(Ring(p, 0, at, own, True))
        second.append(
            [Ring(p, 1, at + 4 + 4 * u, [spots[p][0][u], None, own[2]], u != ME) for u in range(4)]
        )
        third_way.append(
            [
                [
                    Ring(
                        p,
                        2,
                        at + 20 + 16 * u + 4 * v,
                        [spots[p][0][u], spots[p][1][v], None],
                        FAR in (u, v) and ME not in (u, v),
                    )
                    for v in range(4)
                ]
                for u in range(4)
            ]
        )
    rings = [first] + second + [row for part in third_way for row in part]
    hand_overs = []

    def hand_over(p, n, second_at, third_at):
        where = [None, second_at, third_at]
        copy = pltpu.make_async_remote_copy(
            src_ref=cut(mine[p], p, where, None, ROWS),
            dst_ref=cut(theirs[p], p, where, None, ROWS),
            send_sem=dd_send.at[13 * p + n],
            recv_sem=dd_recv.at[13 * p + n],
            device_id=partner,
            device_id_type=MESH,
        )
        copy.start()
        hand_overs.append(copy)

    parts = range(3)
    def launch(*pairs):
        for p in parts:
            for u, v in pairs:
                third_way[p][u][v].start()

    def pass_on(*pairs):
        for p in parts:
            for u, v in pairs:
                third_way[p][u][v].on()

    for p in parts:
        first[p].start()
    for p in parts:
        second[p][ME].start()
    launch((ME, ME))

    early = [
        to_partner(
            ed_hbm.at[:, pl.ds(other_cols, HALF)], ed_other.at[pl.ds(0, HIDDEN)], 1
        ),
        to_partner(dg_hbm, dgu_other.at[pl.ds(0, DENSE)], 2),
        to_partner(du_hbm, dgu_other.at[pl.ds(128, DENSE)], 3),
    ]
    for copy in early:
        copy.start()

    for p in parts:
        first[p].on()
        for u in (LEFT, RIGHT):
            second[p][u].start()
            third_way[p][u][ME].start()
    for p in parts:
        second[p][ME].on()
    launch((ME, RIGHT), (ME, LEFT))
    for p in parts:
        first[p].end()
        second[p][FAR].start()
        third_way[p][FAR][ME].start()
    for p in parts:
        second[p][ME].end()
    launch((ME, FAR))
    pass_on((ME, ME))
    for ref in (eg, eu, ed, ed_other):
        ref[HIDDEN:HPAD, :] = jnp.zeros((HPAD - HIDDEN, ref.shape[1]), BF16)
    for ref in (dgu, dgu_other):
        ref[DENSE:128, :] = jnp.zeros((128 - DENSE, HALF), BF16)
        ref[128 + DENSE : 256, :] = jnp.zeros((128 - DENSE, HALF), BF16)
    dd_scaled[DENSE:128, :] = jnp.zeros((128 - DENSE, HALF), BF16)
    for g in range(GROUPS):
        result[g, SLOTS:128, :] = jnp.zeros((128 - SLOTS, HALF), BF16)
    for p in parts:
        second[p][LEFT].on()
        second[p][RIGHT].on()
    launch((LEFT, RIGHT), (RIGHT, RIGHT), (LEFT, LEFT), (RIGHT, LEFT))
    pass_on((LEFT, ME), (RIGHT, ME), (ME, RIGHT), (ME, LEFT))
    for p in parts:
        second[p][LEFT].end()
        second[p][RIGHT].end()
    launch((LEFT, FAR), (RIGHT, FAR))
    for p in parts:
        second[p][FAR].on()
    launch((FAR, RIGHT), (FAR, LEFT))
    for p in parts:
        second[p][FAR].end()
    launch((FAR, FAR))
    pass_on((FAR, ME), (ME, FAR))
    for p in parts:
        hand_over(p, 0, None, spots[p][2][ME])
        hand_over(p, 1, spots[p][1][ME], spots[p][2][LEFT])
        hand_over(p, 2, spots[p][1][ME], spots[p][2][RIGHT])

    def finish(v, n):
        for p in parts:
            for u in range(4):
                third_way[p][u][v].end()
            hand_over(p, n, spots[p][1][v], spots[p][2][FAR])

    def sides(v, n):
        for p in parts:
            hand_over(p, n, spots[p][1][v], spots[p][2][LEFT])
            hand_over(p, n + 1, spots[p][1][v], spots[p][2][RIGHT])

    pass_on((LEFT, RIGHT), (RIGHT, RIGHT), (LEFT, LEFT), (RIGHT, LEFT))
    finish(ME, 3)
    pass_on((LEFT, FAR), (RIGHT, FAR), (FAR, RIGHT), (FAR, LEFT))
    sides(RIGHT, 4)
    sides(LEFT, 6)
    pass_on((FAR, FAR))
    sides(FAR, 8)
    finish(RIGHT, 10)
    finish(LEFT, 11)
    finish(FAR, 12)
    pick_row = lax.broadcasted_iota(jnp.int32, (128, 128), 0)
    pick_rank = (pick_row == expert).astype(F32).astype(BF16)
    pick_weight = (
        jnp.logical_or(pick_row == expert + 8, pick_row == expert + 16)
    ).astype(F32).astype(BF16)
    lane = lax.broadcasted_iota(jnp.int32, (GROUP_ROWS, 128), 1)
    source = lax.broadcasted_iota(jnp.int32, (GROUP_ROWS, 128), 0) // ROWS

    def group_of(bufs, g):
        z, y = g // 2, 2 * lax.rem(g, 2)
        return jnp.concatenate(
            [
                bufs[p][z, pl.ds(y, 2), :, 0:ROWS, :].reshape(GROUP_ROWS, WIDTHS[p])
                for p in range(3)
            ],
            axis=1,
        )

    def pack_group(g, carry):
        z, y = g // 2, 2 * lax.rem(g, 2)
        tags = x2[z, pl.ds(y, 2), :, ROWS : ROWS + 16, :].reshape(8, 16, 256)
        tags = jnp.concatenate([tags[:, :, 0:128], tags[:, :, 128:256]], axis=1)
        tags = tags.reshape(GROUP_ROWS, 128)
        rank = dot(tags, pick_rank).astype(jnp.int32)
        hit = jnp.logical_and(rank > 0, rank + (CAP * source - 1) == lane)
        table = hit.astype(F32).astype(BF16)
        left_side[g, :, 0:128] = table
        used = table[:, 0:SLOTS]
        slots = pl.ds(pl.multiple_of(g * SLOTS, SLOTS), SLOTS)
        packed[slots, pl.ds(own_cols, HALF)] = dot_tn(used, group_of(mine, g)).astype(BF16)
        slot_tags = dot_tn(used, tags).astype(BF16)
        slot_weight[slots, :] = dot(slot_tags, pick_weight)
        return carry

    lax.fori_loop(0, GROUPS, pack_group, 0, unroll=8)
    for load in loads:
        load.wait()
    for copy in early:
        copy.wait()
    for copy in hand_overs:
        copy.wait()

    def pack_other(g, carry):
        used = left_side[g, :, 0:SLOTS]
        slots = pl.ds(pl.multiple_of(g * SLOTS, SLOTS), SLOTS)
        packed[slots, pl.ds(other_cols, HALF)] = dot_tn(used, group_of(theirs, g)).astype(
            BF16
        )
        return carry

    lax.fori_loop(0, GROUPS, pack_other, 0, unroll=8)

    sends = []
    for i in range(2):
        units = pl.ds(256 * i, 256)
        gate = dot_nt(packed[...], eg[units, :])
        up = dot_nt(packed[...], eu[units, :])
        act[:, units] = (silu(gate) * up * slot_weight[:, 0:1]).astype(BF16)
        copy = to_partner(act.at[:, units], act_other.at[:, units], 4 + i)
        copy.start()
        sends.append(copy)

    def dense_group(g, carry):
        both = dot_nt(group_of(mine, g), dgu[...]) + dot_nt(group_of(theirs, g), dgu_other[...])
        left_side[g, :, 128:256] = (silu(both[:, 0:128]) * both[:, 128:256]).astype(BF16)
        return carry

    lax.fori_loop(0, GROUPS, dense_group, 0, unroll=8)
    share = 1.0 / (1.0 + jnp.exp(-carry[ROWS + 1 : ROWS + 2, 0:HALF]))
    dd_scaled[0:DENSE, :] = (dd[...].astype(F32) * share).astype(BF16)

    class Back:
        def __init__(self, p, k, at, place, slot):
            self.p, self.k, self.place, self.slot = p, k, place, slot
            self.halves, self.wholes = landing[0][p], landing[1][p]
            self.copies = [
                self.copy(at, FAR, 0, 1, self.halves.at[slot, 0]),
                self.copy(at + 1, FAR, 1, 3, self.halves.at[slot, 1]),
                self.copy(at + 2, RIGHT, None, 1, self.wholes.at[slot, 0]),
                self.copy(at + 3, LEFT, None, 3, self.wholes.at[slot, 1]),
            ]

        def spot(self, shift):
            where = list(self.place)
            where[self.k] = spots[self.p][self.k][shift]
            return where

        def copy(self, at, shift, half, to, target):
            p = self.p
            rows = ROWS if half is not None else None
            return pltpu.make_async_remote_copy(
                src_ref=cut(sums[p], p, self.spot(shift), half, rows),
                dst_ref=target,
                send_sem=rs_send.at[at],
                recv_sem=rs_recv.at[at],
                device_id=neighbour(ORDERS[p][self.k], to),
                device_id_type=MESH,
            )

        def start(self):
            self.copies[0].start()
            self.copies[1].start()

        def add_half(self, shift, half):
            p, got = self.p, self.halves
            where = self.spot(shift)
            place = [None, None, None]
            for q in range(3):
                place[ORDERS[p][q]] = where[q]
            free = [d for d in range(3) if place[d] is None]
            for t in range(2):
                place[free[0]] = 2 * half + t
                ref = sums[p].at[tuple(place)]
                ref[...] = ref[...] + got[self.slot, half, t]

        def on(self):
            self.copies[0].wait_recv()
            self.add_half(RIGHT, 0)
            self.copies[2].start()
            self.copies[1].wait_recv()
            self.add_half(LEFT, 1)
            self.copies[3].start()

        def end(self):
            p, got = self.p, self.wholes
            self.copies[2].wait_recv()
            self.copies[3].wait_recv()
            where = self.spot(ME)
            place = [None, None, None]
            for q in range(3):
                place[ORDERS[p][q]] = where[q]
            free = [d for d in range(3) if place[d] is None]
            for t in range(4):
                place[free[0]] = t
                ref = sums[p].at[tuple(place)]
                total = ref[...].astype(F32) + got[self.slot, 0, t].astype(F32)
                ref[...] = (total + got[self.slot, 1, t].astype(F32)).astype(BF16)

    class Straight:
        def __init__(self, p, k, at, place):
            self.p, self.k, self.place, self.wholes = p, k, place, landing[2 + k][p]
            self.copies = [self.copy(at + u - 1, u) for u in (RIGHT, FAR, LEFT)]

        def copy(self, at, u):
            p = self.p
            where = list(self.place)
            where[self.k] = spots[p][self.k][u]
            return pltpu.make_async_remote_copy(
                src_ref=cut(sums[p], p, where),
                dst_ref=self.wholes.at[u - 1],
                send_sem=rs_send.at[at],
                recv_sem=rs_recv.at[at],
                device_id=neighbour(ORDERS[p][self.k], u),
                device_id_type=MESH,
            )

        def send(self, u):
            self.copies[u - 1].start()

        def arrive(self):
            for copy in self.copies:
                copy.wait_recv()

        def add(self, first_at):
            p, got = self.p, self.wholes
            place = [None, None, None]
            for q in range(3):
                place[ORDERS[p][q]] = spots[p][q][ME]
            place[ORDERS[p][0]] = first_at
            ref = sums[p].at[tuple(place)]
            total = ref[...].astype(F32)
            for n in range(3):
                total = total + got[n, first_at].astype(F32)
            ref[...] = total.astype(BF16)

    third, middle, last = [], [], []
    for p in parts:
        at = 24 * p
        own = [spots[p][k][ME] for k in range(3)]
        third.append(
            [Back(p, 2, at + 4 * u, [None, spots[p][1][u], None], u) for u in range(4)]
        )
        middle.append(Straight(p, 1, at + 16, [None, None, own[2]]))
        last.append(Straight(p, 0, at + 20, own))
    order = (FAR, LEFT, RIGHT, ME)
    for send in sends:
        send.wait()
    for p in parts:
        cols = slice(STARTS[p], STARTS[p] + WIDTHS[p])
        for n in ((0, 1), (2,), (3,))[p]:
            some = slice(256 * n, 256 * n + 256)
            back = dot(act[...], ed[:, some]) + dot(act_other[...], ed_other[:, some])
            result[:, 0:SLOTS, some] = back.astype(BF16).reshape(GROUPS, SLOTS, 256)

        def spread_group(g, carry):
            z, y = g // 2, 2 * lax.rem(g, 2)
            right_side = jnp.concatenate([result[g, :, cols], dd_scaled[:, cols]], axis=0)
            total = dot(left_side[g], right_side).astype(BF16)
            sums[p][z, pl.ds(y, 2)] = total.reshape(2, 4, ROWS, WIDTHS[p])
            return carry

        lax.fori_loop(0, GROUPS, spread_group, 0, unroll=8)
        for u in order:
            third[p][u].start()
    for u in order:
        for p in parts:
            third[p][u].on()
    for u in order:
        for p in parts:
            third[p][u].end()
            if u != ME:
                middle[p].send(u)
    for p in parts:
        middle[p].arrive()
        for u in order:
            middle[p].add(spots[p][0][u])
            if u != ME:
                last[p].send(u)
    for p in parts:
        last[p].arrive()
        got = last[p].wholes
        total = mid[:, pl.ds(pl.multiple_of(own_cols + STARTS[p], 128), WIDTHS[p])]
        total = total + sums[p][here[0], here[1], here[2]].astype(F32)
        for n in range(3):
            total = total + got[n].astype(F32)
        out[:, STARTS[p] : STARTS[p] + WIDTHS[p]] = total.astype(BF16)
    for group in third + [middle, last] + rings:
        for sender in group:
            for copy in sender.copies:
                copy.wait_send()


def run_ffn(carry, partial, eg, eu, ed, dg, du, dd):
    vmem = pl.BlockSpec(memory_space=VMEM)
    hbm = pl.BlockSpec(memory_space=pltpu.HBM)
    blocks = lambda *lead: [VMEM((*lead, WIDTHS[p]), BF16) for p in range(3)]
    sem = pltpu.SemaphoreType.DMA
    return pl.pallas_call(
        ffn_kernel,
        out_shape=jax.ShapeDtypeStruct((ROWS, HALF), BF16),
        in_specs=[hbm] * 8,
        out_specs=vmem,
        scratch_shapes=[
            *[VMEM((4, 4, 4, BLOCK_ROWS[p], WIDTHS[p]), BF16) for p in range(3)],
            *blocks(4, 4, 4, ROWS),
            *blocks(4, 4, 4, ROWS),
            *blocks(4, 2, 2, ROWS),
            *blocks(4, 2, 4, ROWS),
            *blocks(3, ROWS),
            *blocks(3, 4, ROWS),
            VMEM((ROWS, 2 * HALF), BF16),
            VMEM((ROWS, 2 * HALF), BF16),
            VMEM((ROWS, 2 * HALF), F32),
            VMEM((HPAD, 2 * HALF), BF16),
            VMEM((HPAD, 2 * HALF), BF16),
            VMEM((HPAD, HALF), BF16),
            VMEM((HPAD, HALF), BF16),
            VMEM((256, HALF), BF16),
            VMEM((256, HALF), BF16),
            VMEM((DENSE, HALF), BF16),
            VMEM((128, HALF), BF16),
            VMEM((GROUPS * SLOTS, 2 * HALF), BF16),
            VMEM((GROUPS * SLOTS, 128), F32),
            VMEM((GROUPS * SLOTS, HPAD), BF16),
            VMEM((GROUPS * SLOTS, HPAD), BF16),
            VMEM((GROUPS, GROUP_ROWS, 256), BF16),
            VMEM((GROUPS, 128, HALF), BF16),
            sem((6,)),
            sem((252,)),
            sem((252,)),
            sem((39,)),
            sem((39,)),
            sem((72,)),
            sem((72,)),
            sem((6,)),
            sem((6,)),
            VMEM((ROWS + 8, CARRY), F32),
            VMEM((ROWS, 2 * HALF), BF16),
            sem((2,)),
        ],
        compiler_params=pltpu.CompilerParams(
            collective_id=0, has_side_effects=True, vmem_limit_bytes=67043328
        ),
        name="ffn",
    )(carry, partial, eg, eu, ed, dg, du, dd)


def local(
    stream,
    mixer_gain,
    gate_proj,
    input_proj,
    state_maps,
    step_proj,
    step_bias,
    decay_rate,
    input_taps,
    map_taps,
    input_past,
    map_past,
    head_state,
    skip_gain,
    inner_gain,
    mixer_out,
    channel_gain,
    expert_ids,
    expert_weight,
    expert_gate,
    expert_up,
    expert_down,
    dense_gate,
    dense_up,
    dense_down,
    dense_mix,
):
    state_out, carry, partial = run_mixer(
        stream,
        mixer_gain.reshape(1, -1),
        step_proj.T,
        expert_ids.T,
        expert_weight.T,
        step_bias,
        decay_rate,
        skip_gain,
        input_proj,
        input_taps,
        jnp.transpose(input_past, (1, 0, 2)),
        state_maps,
        map_taps,
        jnp.transpose(map_past, (0, 2, 1, 3)).reshape(192, 128),
        inner_gain.reshape(1, -1),
        gate_proj,
        channel_gain.reshape(1, -1),
        dense_mix.reshape(1, -1),
        mixer_out,
        head_state.reshape(256, 4096),
    )
    out = run_ffn(
        carry,
        partial,
        expert_gate.T,
        expert_up.T,
        expert_down,
        dense_gate.T,
        dense_up.T,
        dense_down,
    )
    return out, state_out.reshape(head_state.shape)


def solution(mesh):
    placed = (
        P("ep", None),
        P(),
        P(None, "tp"),
        P(None, "tp"),
        P(None, None, "tp"),
        P(None, "tp"),
        P("tp"),
        P("tp"),
        P(None, "tp"),
        P(None, None, "tp"),
        P("ep", None, "tp"),
        P("ep", None, None, "tp"),
        P("ep", "tp", None),
        P("tp"),
        P("tp"),
        P("tp", None),
        P(),
        P("ep", None),
        P("ep", None),
        P(None, ("ep", "tp")),
        P(None, ("ep", "tp")),
        P(("ep", "tp"), None),
        P("tp", "ep"),
        P("tp", "ep"),
        P("ep", "tp"),
        P("tp"),
    )
    return jax.shard_map(
        local,
        mesh=mesh,
        in_specs=placed,
        out_specs=(P("ep", "tp"), P("ep", "tp", None)),
        check_vma=False,
    )
```
